32 devices in a mesh: kv: 8 (over z, x), tp: 4 (over y, core).
Axes of the slice: x: 2, y: 2, z: 4, core: 2. Of those that a mesh axis runs over, the one named last changes fastest.
Arguments:
- tokens: bfloat16 [384, 2048], P(None, 'kv'), may hold values from -40 to 40
- norm_gain: float32 [2048], P('kv'), may hold values from 0.1 to 1.9
- w_query: bfloat16 [2048, 1024], P('kv', 'tp'), may hold values from -0.088388348 to 0.088388348
- w_key: bfloat16 [2048, 1024], P('kv', 'tp'), may hold values from -0.125 to 0.125
- w_value: bfloat16 [2048, 1024], P('kv', 'tp'), may hold values from -0.125 to 0.125
- w_gate: bfloat16 [2048, 16], replicated, may hold values from -0.125 to 0.125
- gate_bias: float32 [16], replicated, may hold values from -1 to 3
- w_out: bfloat16 [1024, 2048], P('tp', 'kv'), may hold values from -0.1875 to 0.1875
- keys_cache: bfloat16 [24, 4096, 1024], P(None, 'kv', 'tp'), may hold values from -512 to 512
- values_cache: bfloat16 [24, 4096, 1024], P(None, 'kv', 'tp'), may hold values from -6 to 6
- cum_gates: float32 [24, 16, 4096], P(None, 'tp', 'kv'), may hold values from -4496 to 0, as said below
- prior_len: int32 [24], replicated, may hold values from 2048 to 4074, as said below
- accepted: int32 [24], replicated, may hold values from 0 to 6
- parents: int32 [24, 16], replicated, may hold values from -1 to 14, as said below
Outputs:
- mixed_rows: bfloat16 [384, 2048], P('tp', 'kv')
- keys_out: bfloat16 [24, 4096, 1024], P(None, 'kv', 'tp')
- values_out: bfloat16 [24, 4096, 1024], P(None, 'kv', 'tp')
The draws below stay inside these ranges and needn't reach their ends.
Inputs may be any that keep to these rules, and one draw needn't show every extreme that they name: parents[b, 0] = -1 and 0 <= parents[b, j] < j for later j. prior_len is at least half of 4096, and prior_len + accepted + 16 <= 4096. `cum_gates`: non-increasing along positions.
All inputs are finite; a program needn't handle non-finite values.
Results may differ from the reference program's by a relative error of at most 0.04.
Values may be sent and summed in bfloat16 or wider, within the bound.
A program may use at most 64 MiB of HBM per device.

```python
import jax
import jax.numpy as jnp
from jax import lax

D = 2048
H = 16
HEAD = 64
PROPS = 16
MOST_ACCEPTED = 6
SEQUENCE_TOTAL = 24
LEN_DEV = 512
CACHE_POSITIONS = 4096
ROWS = 384
N_KV = 8
N_TP = 4


def token_floats(token_key):
    random_keys = jax.random.split(token_key, 3)
    normal_part = jax.random.normal(random_keys[0], (ROWS, D), jnp.float32)
    row_scale = jnp.exp(jax.random.uniform(random_keys[1], (ROWS, 1), jnp.float32, jnp.log(0.3), jnp.log(3.0)))
    column_rise = jnp.exp(jnp.log(3.0) * jnp.arange(D, dtype=jnp.float32)[None, :] / D)
    column_spread = jnp.exp(jax.random.uniform(random_keys[2], (1, D), jnp.float32, jnp.log(0.5), jnp.log(2.0)))
    return jnp.clip(normal_part * row_scale * column_rise * column_spread, -40.0, 40.0)


def query_floats(weight_key):
    drawn = jax.random.truncated_normal(weight_key, -4.0, 4.0, (D, H * HEAD), jnp.float32)
    return drawn * D ** (-0.5)


def draw_tokens(key, part):
    return token_floats(jax.random.fold_in(key, 101)).astype(jnp.bfloat16)


def draw_w_query(key, part):
    return query_floats(jax.random.fold_in(key, 202)).astype(jnp.bfloat16)


def draw_keys_cache(key, part):
    random_keys = jax.random.split(jax.random.fold_in(key, 303), 1)
    result = jax.random.normal(random_keys[0], (SEQUENCE_TOTAL, CACHE_POSITIONS, H * HEAD), jnp.float32)
    result = jnp.clip(result, -6.0, 6.0)
    return jnp.clip(result, -512.0, 512.0).astype(jnp.bfloat16)


def draw_cum_gates(key, part):
    random_keys = jax.random.split(key, 8)
    ranking = jax.random.permutation(random_keys[0], H)
    quick_count = H // 2
    fast_decay_heads = (ranking < quick_count)[None, :, None]
    quick_rate = jnp.exp(jax.random.uniform(random_keys[1], (SEQUENCE_TOTAL, H, 1), jnp.float32, jnp.log(1.0 / 100.0), jnp.log(1.0 / 30.0)))
    slow_rate = jnp.exp(jax.random.uniform(random_keys[2], (SEQUENCE_TOTAL, H, 1), jnp.float32, jnp.log(0.1), jnp.log(0.4))) / CACHE_POSITIONS
    decay_rates = jnp.where(fast_decay_heads, quick_rate, slow_rate)
    block_count = CACHE_POSITIONS // LEN_DEV
    block_multiplier = jnp.exp(jax.random.uniform(random_keys[3], (SEQUENCE_TOTAL, 1, block_count, 1), jnp.float32, 0.0, jnp.log(4.0)))
    block_multiplier = jnp.broadcast_to(block_multiplier, (SEQUENCE_TOTAL, 1, block_count, LEN_DEV)).reshape(SEQUENCE_TOTAL, 1, CACHE_POSITIONS)
    jitter_level = jax.random.uniform(random_keys[4], (SEQUENCE_TOTAL, H, CACHE_POSITIONS), jnp.float32, 0.4, 1.6)
    spike_position = jax.random.randint(random_keys[5], (SEQUENCE_TOTAL, 1, CACHE_POSITIONS), 0, CACHE_POSITIONS) < 2
    dropped_fraction = jax.random.uniform(random_keys[6], (SEQUENCE_TOTAL, H, CACHE_POSITIONS), jnp.float32, 0.2, 0.5)
    spike_events = jnp.where(spike_position & jnp.logical_not(fast_decay_heads), jnp.log(1.0 - dropped_fraction), 0.0)
    gate_increments = spike_events - decay_rates * block_multiplier * jitter_level
    head_offset = jax.random.uniform(random_keys[7], (SEQUENCE_TOTAL, H, 1), jnp.float32, 0.0, 320.0)
    return (jnp.cumsum(gate_increments, axis=2) - head_offset).astype(jnp.float32)


def draw_prior_len(key, part):
    return jax.random.randint(key, (SEQUENCE_TOTAL,), CACHE_POSITIONS // 2, CACHE_POSITIONS - PROPS - MOST_ACCEPTED + 1, dtype=jnp.int32)


def draw_parents(key, part):
    columns = jnp.arange(PROPS, dtype=jnp.int32)
    random_bits = jax.random.randint(key, (SEQUENCE_TOTAL, PROPS), 0, 1 << 20, dtype=jnp.int32)
    picked = random_bits % jnp.maximum(columns, 1)[None, :]
    return jnp.where(columns[None, :] == 0, -1, picked).astype(jnp.int32)


def set_ends(values, own_key, smallest, largest):
    place = [jax.random.randint(jax.random.fold_in(own_key, axis), (), 0, length) for axis, length in enumerate(values.shape)]
    longest = values.shape.index(max(values.shape))
    next_to = place[:longest] + [(place[longest] + 1) % values.shape[longest]] + place[longest + 1:]
    return values.at[tuple(place)].set(smallest).at[tuple(next_to)].set(largest)


def steps_of(key, shape, pieces, least, high):
    loudness = 1.0
    for axis_at, parts in pieces:
        heights = jax.random.uniform(jax.random.fold_in(jax.random.fold_in(key, 6), axis_at), (parts,), jnp.float32, least / len(pieces), high / len(pieces))
        loudness = loudness * jnp.repeat(jnp.exp(heights), shape[axis_at] // parts).reshape((-1,) + (1,) * (len(shape) - 1 - axis_at))
    return loudness


def centred(stream_key, extent, spread, limit, cuts=(), held_as=jnp.bfloat16):
    values = jax.random.normal(stream_key, extent, jnp.float32) * spread
    if len(cuts) > 0:
        values = steps_of(stream_key, extent, cuts, -0.22, 0.18) * values
    return jnp.clip(values, min=-limit, max=limit).astype(held_as)


def setup_inputs(seed: int = 0) -> dict:
    streams_of = jax.random.split(jax.random.key(seed), 15)
    tokens = draw_tokens(jax.random.fold_in(streams_of[14], 71), 0)
    norm_gain = jnp.clip(1.0 + 0.18 * jax.random.normal(streams_of[1], (D,), jnp.float32), 0.1, 1.9)
    w_query = draw_w_query(jax.random.fold_in(streams_of[14], 71), 0)
    w_key = centred(streams_of[3], (D, H * HEAD), D ** -0.5, 0.125, ((0, 8), (1, 4)))
    w_value = centred(streams_of[4], (D, H * HEAD), D ** -0.5, 0.125, ((0, 8), (1, 4)))
    w_gate = centred(streams_of[5], (D, H), D ** -0.5, 0.125)
    gate_bias = jnp.clip(jax.random.uniform(streams_of[6], (H,), jnp.float32, -1.0, 3.0), -1.0, 3.0)
    w_out = centred(streams_of[7], (H * HEAD, D), (H * HEAD) ** -0.5, 0.1875, ((0, 4), (1, 8)))
    keys_cache = draw_keys_cache(jax.random.fold_in(streams_of[14], 71), 0)
    values_cache = centred(streams_of[9], (SEQUENCE_TOTAL, CACHE_POSITIONS, H * HEAD), 1.0, 6.0, ((1, 8), (2, 4)))
    cum_gates = draw_cum_gates(jax.random.fold_in(streams_of[14], 71), 0)
    prior_len = draw_prior_len(jax.random.fold_in(streams_of[14], 71), 0)
    accepted = set_ends(jax.random.randint(streams_of[12], (SEQUENCE_TOTAL,), 0, MOST_ACCEPTED + 1), jax.random.fold_in(streams_of[12], 1), 0, MOST_ACCEPTED).astype(jnp.int32)
    parents = draw_parents(jax.random.fold_in(streams_of[14], 71), 0)
    return {"tokens": tokens, "norm_gain": norm_gain, "w_query": w_query, "w_key": w_key, "w_value": w_value, "w_gate": w_gate, "gate_bias": gate_bias, "w_out": w_out, "keys_cache": keys_cache, "values_cache": values_cache, "cum_gates": cum_gates, "prior_len": prior_len, "accepted": accepted, "parents": parents}


masked_score = -1e+30
norm_eps = 1e-06

def ancestry(parents):
    columns = jnp.arange(PROPS, dtype=jnp.int32)
    parent_link = (parents[:, :, None] == columns[None, None, :]).astype(jnp.float32)
    reached = jnp.eye(PROPS, dtype=jnp.float32)[None] + parent_link
    for squaring in range(PROPS.bit_length()):
        reached = jnp.minimum(jnp.einsum('bij,bjk->bik', reached, reached, precision=lax.Precision.HIGHEST), 1.0)
    return reached

def reference(tokens, norm_gain, w_query, w_key, w_value, w_gate, gate_bias, w_out, keys_cache, values_cache, cum_gates, prior_len, accepted, parents):
    floats = tokens.astype(jnp.float32)
    inv_rms = lax.rsqrt(lax.optimization_barrier(jnp.sum(floats * floats, axis=1)) / D + norm_eps)
    scaled = (floats * norm_gain).astype(jnp.bfloat16)

    def project(weight):
        return inv_rms[:, None] * jnp.dot(scaled, weight, preferred_element_type=jnp.float32)
    queries = project(w_query).astype(jnp.bfloat16)
    new_keys = project(w_key).astype(jnp.bfloat16)
    new_values = project(w_value).astype(jnp.bfloat16)
    log_gates = jax.nn.log_sigmoid(project(w_gate) + gate_bias).reshape(SEQUENCE_TOTAL, PROPS, H)
    reached = ancestry(parents)
    tree_gates = jnp.einsum('bij,bjh->bih', reached, log_gates, precision=lax.Precision.HIGHEST)
    filled = prior_len + accepted
    last_pos = filled - 1
    index_last = jnp.broadcast_to(last_pos[:, None, None], (SEQUENCE_TOTAL, H, 1))
    last_gate = jnp.take_along_axis(cum_gates, index_last, axis=2)[:, :, 0]
    prop_cum = last_gate[:, None, :] + tree_gates
    owners = (last_pos // LEN_DEV).astype(jnp.int32)
    scale = HEAD ** (-0.5)

    def attend(packed):
        seq_query, seq_keys, seq_values, seq_cum, seq_newk, seq_newv, seq_prop, seq_reach, seq_fill, seq_owner = packed
        query_f = seq_query.reshape(PROPS, H, HEAD).astype(jnp.float32)
        keys_f = seq_keys.reshape(CACHE_POSITIONS, H, HEAD).astype(jnp.float32)
        scores = jnp.einsum('ihd,phd->hip', query_f, keys_f) * scale - seq_cum[:, None, :]
        positions = jnp.arange(CACHE_POSITIONS, dtype=jnp.int32)
        valid_keys = positions < seq_fill
        scores = jnp.where(valid_keys[None, None, :], scores, masked_score)
        blocked = scores.reshape(H, PROPS, N_KV, LEN_DEV)
        newk_f = seq_newk.reshape(PROPS, H, HEAD).astype(jnp.float32)
        tree_scores = jnp.einsum('ihd,jhd->hij', query_f, newk_f) * scale - jnp.transpose(seq_prop)[:, None, :]
        tree_live = (seq_reach > 0.5)[None]
        tree_scores = jnp.where(tree_live, tree_scores, masked_score)
        is_owner = jnp.arange(N_KV, dtype=jnp.int32) == seq_owner
        block_max = lax.optimization_barrier(jnp.max(blocked, axis=3))
        tree_max = lax.optimization_barrier(jnp.max(tree_scores, axis=2))
        block_max = jnp.where(is_owner[None, None, :], jnp.maximum(block_max, tree_max[:, :, None]), block_max)
        owner_max = lax.optimization_barrier(jnp.max(jnp.where(is_owner[None, None, :], block_max, masked_score), axis=2))
        valid_blocks = valid_keys.reshape(N_KV, LEN_DEV)[None, None]
        weights = jnp.where(valid_blocks, jnp.exp(blocked - block_max[..., None]), 0.0)
        tree_weights = jnp.where(tree_live, jnp.exp(tree_scores - owner_max[:, :, None]), 0.0)
        block_sums = lax.optimization_barrier(jnp.sum(weights, axis=3)) + jnp.where(is_owner[None, None, :], lax.optimization_barrier(jnp.sum(tree_weights, axis=2))[:, :, None], 0.0)
        values_f = seq_values.reshape(N_KV, LEN_DEV, H, HEAD).astype(jnp.float32)
        newv_f = seq_newv.reshape(PROPS, H, HEAD).astype(jnp.float32)
        rounded = lax.optimization_barrier(weights.astype(jnp.bfloat16)).astype(jnp.float32)
        tree_rounded = lax.optimization_barrier(tree_weights.astype(jnp.bfloat16)).astype(jnp.float32)
        block_values = jnp.einsum('hinp,nphd->hind', rounded, values_f)
        tree_values = jnp.einsum('hij,jhd->hid', tree_rounded, newv_f)
        block_values = block_values + jnp.where(is_owner[None, None, :, None], tree_values[:, :, None, :], 0.0)
        block_values = lax.optimization_barrier(block_values.astype(jnp.bfloat16)).astype(jnp.float32)
        top_score = lax.optimization_barrier(jnp.max(block_max, axis=2))
        rescale = jnp.exp(block_max - top_score[..., None])
        grand_total = lax.optimization_barrier(jnp.sum(rescale * block_sums, axis=2))
        result = lax.optimization_barrier(jnp.sum(rescale[..., None] * block_values, axis=2)) / grand_total[..., None]
        return jnp.transpose(result, (1, 0, 2)).astype(jnp.bfloat16)
    packed = (queries.reshape(SEQUENCE_TOTAL, PROPS, H * HEAD), keys_cache, values_cache, cum_gates, new_keys.reshape(SEQUENCE_TOTAL, PROPS, H * HEAD), new_values.reshape(SEQUENCE_TOTAL, PROPS, H * HEAD), prop_cum, reached, filled, owners)
    attended = lax.map(attend, packed).reshape(ROWS, H * HEAD)
    group = H // N_TP * HEAD
    parted = attended.reshape(ROWS, N_TP, group).astype(jnp.float32)
    weight_groups = w_out.reshape(N_TP, group, D).astype(jnp.float32)
    head_parts = jnp.einsum('rgc,gcd->grd', parted, weight_groups)
    head_parts = lax.optimization_barrier(head_parts.astype(jnp.bfloat16)).astype(jnp.float32)
    mixed_rows = lax.optimization_barrier(jnp.sum(head_parts, axis=0)).astype(jnp.bfloat16)

    def write(cache, new_rows, start):
        return lax.dynamic_update_slice(cache, new_rows, (start.astype(jnp.int32), jnp.zeros((), jnp.int32)))
    keys_out = jax.vmap(write)(keys_cache, new_keys.reshape(SEQUENCE_TOTAL, PROPS, H * HEAD), filled)
    values_out = jax.vmap(write)(values_cache, new_values.reshape(SEQUENCE_TOTAL, PROPS, H * HEAD), filled)
    return (mixed_rows, keys_out, values_out)
```

```python
import functools

import jax
import jax.numpy as jnp
from jax import lax
from jax.experimental import pallas as pl
from jax.experimental.pallas import tpu as pltpu
from jax.sharding import PartitionSpec as P

HEAD = 64
PROPS = 16
LANES = 128
SQUARE_ROW = 7
SUM_ROW = 4
masked_score = -1e30
norm_eps = 1e-06
MESH = pl.DeviceIdType.MESH
f32, bf16, i32 = jnp.float32, jnp.bfloat16, jnp.int32


def iota(shape, axis):
    return lax.broadcasted_iota(i32, shape, axis)


def ones_where(mask, dtype=f32):
    return jnp.where(mask, 1.0, 0.0).astype(dtype)


def split2(x):
    hi = x.astype(bf16)
    return hi, (x - hi.astype(f32)).astype(bf16)


def split3(x):
    hi = x.astype(bf16).astype(f32)
    mid = (x - hi).astype(bf16).astype(f32)
    return hi, mid, x - hi - mid


def contract_last(a, b):
    return lax.dot_general(a, b, (((1,), (1,)), ((), ())), preferred_element_type=f32)


def matmul(a, b):
    return jnp.dot(a, b, preferred_element_type=f32)


def step_kernel(
    n_kv,
    n_tp,
    heads,
    per,
    prior_s,
    accepted_s,
    tokens_ref,
    gain_ref,
    wq_ref,
    wk_ref,
    wv_ref,
    wg_ref,
    bias_ref,
    wout_ref,
    parents_ref,
    k_hbm,
    v_hbm,
    cum_hbm,
    mixed_ref,
    newk_ref,
    newv_ref,
    kbuf,
    vbuf,
    cumbuf,
    part,
    gpart,
    arr1,
    garr1,
    half,
    ghalf,
    arr2,
    garr2,
    full,
    gfull,
    wall,
    parts_v,
    parts_s,
    got_v,
    got_s,
    mine,
    att,
    load_sems,
    s1_send,
    s1_recv,
    s2_send,
    s2_recv,
    s3_send,
    s3_recv,
    w_send,
    w_recv,
    cv_send,
    cv_recv,
    cs_send,
    cs_recv,
    ag_send,
    ag_recv,
):
    me = lax.axis_index("kv")
    tp = lax.axis_index("tp")
    n_chunks, rc, depth = tokens_ref.shape
    length = kbuf.shape[1]
    width = heads * HEAD
    lines = heads * PROPS
    cq = n_chunks // 4
    n_groups = n_kv // 4
    cpt = n_chunks // n_tp
    corner, group = lax.rem(me, 4), me // 4
    quarter = pl.ds(corner * cq, cq)

    barrier = pltpu.get_barrier_semaphore()
    for d in range(1, n_kv * n_tp):
        other = lax.rem(me * n_tp + tp + d, n_kv * n_tp)
        pl.semaphore_signal(
            barrier,
            inc=1,
            device_id={"kv": other // n_tp, "tp": lax.rem(other, n_tp)},
            device_id_type=MESH,
        )
    loads = []
    for c in range(n_chunks):
        span = pl.ds(c * per, per)
        for at, (source, target) in enumerate(((k_hbm, kbuf), (v_hbm, vbuf), (cum_hbm, cumbuf))):
            copy = pltpu.make_async_copy(source.at[span], target.at[span], load_sems.at[at, c])
            copy.start()
            loads.append(copy)

    def send(source, target, sems, at, kv=None, to_tp=None):
        where = {}
        if kv is not None:
            where["kv"] = kv
        if to_tp is not None:
            where["tp"] = to_tp
        copy = pltpu.make_async_remote_copy(
            src_ref=source,
            dst_ref=target,
            send_sem=sems[0].at[at],
            recv_sem=sems[1].at[at],
            device_id=where,
            device_id_type=MESH,
        )
        copy.start()
        return copy

    total_heads = bias_ref.shape[1]
    pick = (iota((8, total_heads), 1) == tp * heads + iota((8, total_heads), 0)) & (
        iota((8, total_heads), 0) < heads
    )
    if depth % LANES == 0:
        gate_w = wg_ref[:, pl.ds(pl.multiple_of(me * depth, depth), depth)]
        gate_w = matmul(ones_where(pick, bf16), gate_w).astype(bf16)
    else:
        gate_w = wg_ref[pl.ds(pl.multiple_of(me * depth, depth), depth), :]
        gate_w = contract_last(ones_where(pick, bf16), gate_w).astype(bf16)
    square_w = ones_where(iota((8, depth), 0) == SQUARE_ROW, bf16)
    floats = tokens_ref[...].reshape(n_chunks * rc, depth).astype(f32)
    scaled = (floats * gain_ref[...]).astype(bf16)

    def product(piece, w_ref):
        value = matmul(scaled, w_ref[...]).astype(bf16)
        part[piece] = value.reshape(n_chunks, rc, width)

    product(0, wq_ref)
    sq_hi, sq_lo = split2(floats * floats)
    gpart[...] = jnp.zeros_like(gpart)
    for c in range(n_chunks):
        rows = slice(c * rc, (c + 1) * rc)
        gpart[c, :, :rc] = (
            contract_last(gate_w, scaled[rows])
            + contract_last(square_w, sq_hi[rows])
            + contract_last(square_w, sq_lo[rows])
        )

    pl.semaphore_wait(barrier, n_kv * n_tp - 1)
    started = []

    def corner_sends(sources, targets, sems, piece):
        out = []
        for d in range(1, 4):
            there = lax.rem(corner + d, 4)
            out.append(
                send(
                    sources(there), targets(d), sems, piece * 3 + d - 1, kv=group * 4 + there
                )
            )
        started.extend(out)
        return out

    def first_stage(piece):
        return corner_sends(
            lambda there: part.at[piece, pl.ds(there * cq, cq)],
            lambda d: arr1.at[piece, d - 1],
            (s1_send, s1_recv),
            piece,
        )

    def group_sends(source, target, piece):
        out = []
        for d in range(1, n_groups):
            there = lax.rem(group + d, n_groups) * 4 + corner
            out.append(
                send(
                    source,
                    target(d),
                    (s2_send, s2_recv),
                    piece * (n_groups - 1) + d - 1,
                    kv=there,
                )
            )
        started.extend(out)
        return out

    def second_stage(piece, stage):
        for copy in stage:
            copy.wait_recv()
        total = part[piece, quarter].astype(f32)
        for d in range(3):
            total = total + arr1[piece, d].astype(f32)
        half[piece] = total.astype(bf16)
        return group_sends(half.at[piece], lambda d: arr2.at[piece, d - 1], piece)

    def third_stage(piece, stage, columns):
        for copy in stage:
            copy.wait_recv()
        total = half[piece].astype(f32)
        for d in range(n_groups - 1):
            total = total + arr2[piece, d].astype(f32)
        for j in range(cq):
            full[piece, corner * cq + j] = (total[j] * columns[j]).astype(bf16)
        return corner_sends(
            lambda there: full.at[piece, quarter],
            lambda d: full.at[piece, quarter],
            (s3_send, s3_recv),
            piece,
        )

    q1 = first_stage(0)
    g1 = corner_sends(
        lambda there: gpart.at[pl.ds(there * cq, cq)],
        lambda d: garr1.at[d - 1],
        (s1_send, s1_recv),
        3,
    )
    product(1, wk_ref)
    k1 = first_stage(1)
    product(2, wv_ref)

    slot = lax.rem(me, n_tp) * cpt + me // n_tp
    own = jnp.minimum(slot, n_chunks - 1)
    every = parents_ref[...]
    parent = jnp.concatenate(
        [
            jnp.sum(
                jnp.where(iota(every.shape, 1) == own * per + k, every, 0).astype(f32),
                axis=1,
                keepdims=True,
            ).astype(i32)
            for k in range(per)
        ],
        axis=0,
    )
    row, column = iota((rc, rc), 0), iota((rc, rc), 1)
    link = (parent + (row // PROPS) * PROPS == column) & (parent >= 0)
    reached = ones_where(link | (row == column))
    for squaring in range((PROPS - 1).bit_length()):
        reached = jnp.minimum(matmul(reached.astype(bf16), reached.astype(bf16)), 1.0)

    q2 = second_stage(0, q1)
    for copy in g1:
        copy.wait_recv()
    ghalf[...] = gpart[quarter] + garr1[0] + garr1[1] + garr1[2]
    g2 = group_sends(ghalf, lambda d: garr2.at[d - 1], 3)
    v1 = first_stage(2)
    w_copies = []
    for d in range(1, n_tp):
        w_copies.append(
            send(
                wout_ref, wall.at[tp], (w_send, w_recv), d - 1, to_tp=lax.rem(tp + d, n_tp)
            )
        )
    started.extend(w_copies)
    wall[tp] = wout_ref[...]

    for copy in g2:
        copy.wait_recv()
    gates = ghalf[...]
    for d in range(n_groups - 1):
        gates = gates + garr2[d]
    bias = jnp.sum(
        jnp.where(pick, jnp.broadcast_to(bias_ref[...], (8, total_heads)), 0.0),
        axis=1,
        keepdims=True,
    )
    inv_columns = []
    eye = iota((rc, LANES), 0) == iota((rc, LANES), 1)
    for j in range(cq):
        inv_row = lax.rsqrt(
            gates[j, SQUARE_ROW : SQUARE_ROW + 1, :] / (n_kv * depth) + norm_eps
        )
        pre = inv_row * gates[j] + bias
        gfull[corner * cq + j] = jnp.minimum(pre, 0.0) - jnp.log1p(jnp.exp(-jnp.abs(pre)))
        inv_columns.append(
            jnp.sum(
                jnp.where(eye, jnp.broadcast_to(inv_row, (rc, LANES)), 0.0),
                axis=1,
                keepdims=True,
            )
        )
    q3 = third_stage(0, q2, [c * HEAD ** (-0.5) for c in inv_columns])
    g3 = corner_sends(
        lambda there: gfull.at[quarter], lambda d: gfull.at[quarter], (s3_send, s3_recv), 3
    )
    k2 = second_stage(1, k1)
    v2 = second_stage(2, v1)

    lane_head = iota((PROPS, width), 1) // HEAD
    head_rows = [ones_where(lane_head == h) for h in range(heads)]
    head_mask = jnp.concatenate(head_rows, axis=0).astype(bf16)
    position = iota((lines, length), 1)
    short_position = iota((heads, length), 1)
    line_eye = iota((lines, LANES), 0) == iota((lines, LANES), 1)
    last_lane = iota((heads, LANES), 1) - LANES // 2
    last_mask = (last_lane >= 0) & (last_lane // PROPS == iota((heads, LANES), 0))
    tile_row = iota((8, LANES), 0)
    offset = me * length

    def as_row(value):
        return jnp.sum(jnp.where(line_eye, value, 0.0), axis=0, keepdims=True)

    def attend(owner):
        chunk = jnp.minimum(lax.rem(owner, n_tp) * cpt + owner // n_tp, n_chunks - 1)
        limits, scores = [], []
        for k in range(per):
            seq = chunk * per + k
            limits.append(prior_s[seq] + accepted_s[seq] - offset)
            query = full[0, chunk, k * PROPS : (k + 1) * PROPS, :]
            query = jnp.concatenate([query] * heads, axis=0) * head_mask
            scores.append(contract_last(query, kbuf[seq]))
        tile = jnp.zeros((8, LANES), f32)
        weights = []
        for k in range(per):
            seq = chunk * per + k
            cum = jnp.concatenate(
                [
                    jnp.broadcast_to(cumbuf[seq, h : h + 1, :], (PROPS, length))
                    for h in range(heads)
                ],
                axis=0,
            )
            value = jnp.where(position < limits[k], scores[k] - cum, masked_score)
            top = jnp.max(value, axis=1, keepdims=True)
            weight = jnp.exp(value - top)
            total = jnp.sum(weight, axis=1, keepdims=True)
            weights.append(weight.astype(bf16))
            last = jnp.sum(
                jnp.where(short_position == limits[k] - 1, cumbuf[seq], 0.0),
                axis=1,
                keepdims=True,
            )
            last_row = jnp.sum(jnp.where(last_mask, last, 0.0), axis=0, keepdims=True)
            tile = jnp.where(tile_row == k, as_row(top) + last_row, tile)
            tile = jnp.where(tile_row == SUM_ROW + k, as_row(total), tile)
        for k in range(per):
            values = matmul(weights[k], vbuf[chunk * per + k])
            picked = values[:PROPS] * head_rows[0]
            for h in range(1, heads):
                picked = picked + values[h * PROPS : (h + 1) * PROPS] * head_rows[h]
            parts_v[owner, k * PROPS : (k + 1) * PROPS, :] = picked.astype(bf16)
        parts_s[owner] = tile

    def part_copies(d):
        owner = lax.rem(me + d, n_kv)
        return [
            pltpu.make_async_remote_copy(
                src_ref=source.at[owner],
                dst_ref=target.at[d - 1],
                send_sem=send_sem.at[d - 1],
                recv_sem=recv_sem.at[d - 1],
                device_id={"kv": owner},
                device_id_type=MESH,
            )
            for source, target, send_sem, recv_sem in (
                (parts_v, got_v, cv_send, cv_recv),
                (parts_s, got_s, cs_send, cs_recv),
            )
        ]

    def attend_and_send(d):
        attend(lax.rem(me + d, n_kv))
        for copy in part_copies(d):
            copy.start()

    for copy in loads:
        copy.wait()
    for copy in q3:
        copy.wait_recv()
    attend_and_send(1)
    k3 = third_stage(1, k2, inv_columns)
    attend_and_send(2)
    v3 = third_stage(2, v2, inv_columns)

    def one(d, carry):
        attend_and_send(d)
        return carry

    lax.fori_loop(3, n_kv, one, 0)
    attend(me)

    for copy in g3 + k3:
        copy.wait_recv()
    gate_parts = jnp.concatenate(split3(gfull[own]), axis=0)[:, :rc].astype(bf16)
    tree_gates = contract_last(gate_parts, reached.astype(bf16))
    tree_gates = tree_gates[0:8] + tree_gates[8:16] + tree_gates[16:24]
    wide_rows = [ones_where(iota((rc, width), 1) // HEAD == h) for h in range(heads)]
    wide_mask = jnp.concatenate(wide_rows, axis=0).astype(bf16)
    tree_query = jnp.concatenate([full[0, own]] * heads, axis=0) * wide_mask
    tree = contract_last(tree_query, full[1, own])
    tree = tree - jnp.concatenate(
        [jnp.broadcast_to(tree_gates[h : h + 1, :], (rc, rc)) for h in range(heads)], axis=0
    )
    live = jnp.concatenate([reached] * heads, axis=0) > 0.5
    tree = jnp.where(live, tree, masked_score)
    tree_top = jnp.max(tree, axis=1, keepdims=True)
    tree_weights = jnp.where(live, jnp.exp(tree - tree_top), 0.0)
    tree_sum = jnp.sum(tree_weights, axis=1, keepdims=True)
    for copy in v3:
        copy.wait_recv()
    tree_values = matmul(tree_weights.astype(bf16), full[2, own])
    tree_picked = tree_values[:rc] * wide_rows[0]
    for h in range(1, heads):
        tree_picked = tree_picked + tree_values[h * rc : (h + 1) * rc] * wide_rows[h]
    newk_ref[...] = full[1]
    newv_ref[...] = full[2]

    def tile_of(value):
        rows = [
            as_row(
                jnp.concatenate(
                    [
                        value[h * rc + k * PROPS : h * rc + (k + 1) * PROPS]
                        for h in range(heads)
                    ],
                    axis=0,
                )
            )
            for k in range(per)
        ]
        rows = rows + [jnp.zeros((1, LANES), f32)] * (4 - per)
        return jnp.concatenate(rows, axis=0)

    tree_top_tile, tree_sum_tile = tile_of(tree_top), tile_of(tree_sum)

    landing = [part_copies(d) for d in range(1, n_kv)]
    for pair in landing:
        pair[1].wait_recv()
    tiles = [parts_s[me]] + [got_s[d] for d in range(n_kv - 1)]
    last = tiles[0][:4]
    for tile in tiles[1:]:
        last = last + tile[:4]
    last = pltpu.roll(last, LANES // 2, axis=1)
    lane_ok = iota((4, LANES), 1) < lines
    tops = [jnp.where(lane_ok, tile[:4], 0.0) for tile in tiles]
    tops.append(jnp.where(lane_ok, tree_top_tile - last, 0.0))
    sums = [jnp.where(lane_ok, tile[4:], 1.0) for tile in tiles] + [
        jnp.where(lane_ok, tree_sum_tile, 1.0)
    ]
    top = functools.reduce(jnp.maximum, tops)
    scales = [jnp.exp(t - top) for t in tops]
    total = functools.reduce(lambda a, b: a + b, [a * b for a, b in zip(scales, sums)])
    spread = ones_where(
        (iota((LANES, width), 0) // PROPS == iota((LANES, width), 1) // HEAD)
        & (iota((LANES, width), 0) < lines),
        bf16,
    )
    fits = (iota((PROPS, LANES), 1) % PROPS == iota((PROPS, LANES), 0)) & (
        iota((PROPS, LANES), 1) < lines
    )

    def expand(scale):
        scale = scale / total
        rows = jnp.concatenate(
            [
                jnp.where(fits, jnp.broadcast_to(scale[k : k + 1], (PROPS, LANES)), 0.0)
                for k in range(per)
            ],
            axis=0,
        )
        hi, lo = split2(rows)
        return matmul(hi, spread) + matmul(lo, spread)

    result = expand(scales[-1]) * tree_picked
    result = result + expand(scales[0]) * parts_v[me].astype(f32)
    for d in range(n_kv - 1):
        landing[d][0].wait_recv()
        result = result + expand(scales[d + 1]) * got_v[d].astype(f32)
    mine[...] = result.astype(bf16)

    target, early = lax.rem(me, n_tp), me // n_tp
    spreads = [
        pltpu.make_async_remote_copy(
            src_ref=mine,
            dst_ref=att.at[jnp.minimum(early, cpt - 1), tp],
            send_sem=ag_send.at[d],
            recv_sem=ag_recv.at[jnp.minimum(early, cpt - 1) * n_tp + tp],
            device_id={"kv": lax.rem(me + d, n_kv), "tp": target},
            device_id_type=MESH,
        )
        for d in range(n_kv)
    ]
    sends = early < cpt
    for d in range(1, n_kv):

        @pl.when(sends)
        def _(d=d):
            spreads[d].start()

    @pl.when(sends & (target != tp))
    def _():
        spreads[0].start()

    @pl.when(sends & (target == tp))
    def _():
        att[jnp.minimum(early, cpt - 1), tp] = mine[...]

    for copy in w_copies:
        copy.wait_recv()
    for at in range(cpt * n_tp):
        e, t = at // n_tp, at % n_tp

        @pl.when((me != e * n_tp + tp) | (tp != t))
        def _(at=at, e=e, t=t):
            pltpu.make_async_remote_copy(
                src_ref=mine,
                dst_ref=att.at[e, t],
                send_sem=ag_send.at[0],
                recv_sem=ag_recv.at[at],
                device_id={"kv": me, "tp": lax.rem(tp + 1, n_tp)},
                device_id_type=MESH,
            ).wait_recv()

    mixed = None
    for t in range(n_tp):
        rows = jnp.concatenate([att[e, t] for e in range(cpt)], axis=0)
        piece = matmul(rows, wall[t]).astype(bf16).astype(f32)
        mixed = piece if mixed is None else mixed + piece
    mixed_ref[...] = mixed.astype(bf16)

    for d in range(1, n_kv):

        @pl.when(sends)
        def _(d=d):
            spreads[d].wait_send()

    @pl.when(sends & (target != tp))
    def _():
        spreads[0].wait_send()

    for copy in started:
        copy.wait_send()
    for pair in landing:
        for copy in pair:
            copy.wait_send()


def write_kernel(
    prior_s,
    accepted_s,
    newk_ref,
    newv_ref,
    mixed_in,
    k_ref,
    v_ref,
    mixed_ref,
    ko_ref,
    vo_ref,
    windows,
    bulk_sems,
    window_sems,
):
    seq_count, length, width = k_ref.shape
    window = 2 * PROPS
    offset = lax.axis_index("kv") * length
    bulk = []
    for b in range(seq_count):
        for at, (source, target) in enumerate(((k_ref, ko_ref), (v_ref, vo_ref))):
            copy = pltpu.make_async_copy(source.at[b], target.at[b], bulk_sems.at[at, b])
            copy.start()
            bulk.append(copy)
    mixed_ref[...] = mixed_in[...]
    placed = []
    for b in range(seq_count):
        limit = prior_s[b] + accepted_s[b] - offset
        start = pl.multiple_of(jnp.clip(limit, 0, length - window) // PROPS * PROPS, PROPS)
        select = start + iota((window, PROPS), 0) - limit == iota((window, PROPS), 1)
        select = ones_where(select, bf16)
        slot = start + iota((window, width), 0) - limit
        inside = (slot >= 0) & (slot < PROPS)
        for at, (source, fresh, target) in enumerate(
            ((k_ref, newk_ref, ko_ref), (v_ref, newv_ref, vo_ref))
        ):
            rows = matmul(select, fresh[b * PROPS : (b + 1) * PROPS])
            old = source[b, pl.ds(start, window), :].astype(f32)
            windows[at, b] = jnp.where(inside, rows, old).astype(bf16)
            placed.append(
                pltpu.make_async_copy(
                    windows.at[at, b],
                    target.at[b, pl.ds(start, window), :],
                    window_sems.at[at, b],
                )
            )
    for first, second in zip(bulk, placed):
        first.wait()
        second.start()
    for copy in placed:
        copy.wait()


def shards(
    n_kv,
    n_tp,
    tokens,
    norm_gain,
    w_query,
    w_key,
    w_value,
    w_gate,
    gate_bias,
    w_out,
    keys_cache,
    values_cache,
    cum_gates,
    prior_len,
    accepted,
    parents,
):
    row_count, depth = tokens.shape
    seq_count, length, width = keys_cache.shape
    heads = width // HEAD
    per = next(p for p in range(1, 5) if seq_count % p == 0 and seq_count // p <= n_kv)
    n_chunks = seq_count // per
    rc = per * PROPS
    cq = n_chunks // 4
    n_groups = n_kv // 4
    cpt = n_chunks // n_tp
    columns = w_out.shape[1]
    vmem = pl.BlockSpec(memory_space=pltpu.VMEM)
    smem = pl.BlockSpec(memory_space=pltpu.SMEM)
    hbm = pl.BlockSpec(memory_space=pltpu.HBM)
    dma = pltpu.SemaphoreType.DMA

    mixed, new_keys, new_values = pl.pallas_call(
        functools.partial(step_kernel, n_kv, n_tp, heads, per),
        out_shape=(
            jax.ShapeDtypeStruct((cpt * rc, columns), bf16),
            jax.ShapeDtypeStruct((n_chunks, rc, width), bf16),
            jax.ShapeDtypeStruct((n_chunks, rc, width), bf16),
        ),
        in_specs=[smem] * 2 + [vmem] * 9 + [hbm] * 3,
        out_specs=[vmem] * 3,
        scratch_shapes=[
            pltpu.VMEM((seq_count, length, width), bf16),
            pltpu.VMEM((seq_count, length, width), bf16),
            pltpu.VMEM((seq_count, heads, length), f32),
            pltpu.VMEM((3, n_chunks, rc, width), bf16),
            pltpu.VMEM((n_chunks, 8, LANES), f32),
            pltpu.VMEM((3, 3, cq, rc, width), bf16),
            pltpu.VMEM((3, cq, 8, LANES), f32),
            pltpu.VMEM((3, cq, rc, width), bf16),
            pltpu.VMEM((cq, 8, LANES), f32),
            pltpu.VMEM((3, n_groups - 1, cq, rc, width), bf16),
            pltpu.VMEM((n_groups - 1, cq, 8, LANES), f32),
            pltpu.VMEM((3, n_chunks, rc, width), bf16),
            pltpu.VMEM((n_chunks, 8, LANES), f32),
            pltpu.VMEM((n_tp, width, columns), bf16),
            pltpu.VMEM((n_kv, rc, width), bf16),
            pltpu.VMEM((n_kv, 8, LANES), f32),
            pltpu.VMEM((n_kv - 1, rc, width), bf16),
            pltpu.VMEM((n_kv - 1, 8, LANES), f32),
            pltpu.VMEM((rc, width), bf16),
            pltpu.VMEM((cpt, n_tp, rc, width), bf16),
            dma((3, n_chunks)),
            dma((12,)),
            dma((12,)),
            dma((4 * (n_groups - 1),)),
            dma((4 * (n_groups - 1),)),
            dma((12,)),
            dma((12,)),
            dma((n_tp - 1,)),
            dma((n_tp - 1,)),
            dma((n_kv - 1,)),
            dma((n_kv - 1,)),
            dma((n_kv - 1,)),
            dma((n_kv - 1,)),
            dma((n_kv,)),
            dma((cpt * n_tp,)),
        ],
        compiler_params=pltpu.CompilerParams(
            collective_id=0, has_side_effects=True, vmem_limit_bytes=28 * 1024 * 1024
        ),
        name="step",
    )(
        prior_len,
        accepted,
        tokens.reshape(n_chunks, rc, depth),
        norm_gain.reshape(1, depth),
        w_query,
        w_key,
        w_value,
        w_gate.T if depth % LANES == 0 else w_gate,
        gate_bias.reshape(1, -1),
        w_out,
        parents.T,
        keys_cache,
        values_cache,
        cum_gates,
    )

    return pl.pallas_call(
        write_kernel,
        out_shape=(
            jax.ShapeDtypeStruct((cpt * rc, columns), bf16),
            jax.ShapeDtypeStruct(keys_cache.shape, bf16),
            jax.ShapeDtypeStruct(values_cache.shape, bf16),
        ),
        in_specs=[smem] * 2 + [vmem] * 5,
        out_specs=[vmem, hbm, hbm],
        scratch_shapes=[
            pltpu.VMEM((2, seq_count, 2 * PROPS, width), bf16),
            dma((2, seq_count)),
            dma((2, seq_count)),
        ],
        name="write",
    )(
        prior_len,
        accepted,
        new_keys.reshape(row_count, width),
        new_values.reshape(row_count, width),
        mixed,
        keys_cache,
        values_cache,
    )


def solution(mesh):
    placed = (
        P(None, "kv"),
        P("kv"),
        P("kv", "tp"),
        P("kv", "tp"),
        P("kv", "tp"),
        P(),
        P(),
        P("tp", "kv"),
        P(None, "kv", "tp"),
        P(None, "kv", "tp"),
        P(None, "tp", "kv"),
        P(),
        P(),
        P(),
    )
    return jax.shard_map(
        functools.partial(shards, mesh.shape["kv"], mesh.shape["tp"]),
        mesh=mesh,
        in_specs=placed,
        out_specs=(P("tp", "kv"), P(None, "kv", "tp"), P(None, "kv", "tp")),
        check_vma=False,
    )
```

```python
import functools

import jax
import jax.numpy as jnp
from jax import lax
from jax.experimental import pallas as pl
from jax.experimental.pallas import tpu as pltpu
from jax.sharding import PartitionSpec as P

HEAD = 64
PROPS = 16
LANES = 128
SQUARE_ROW = 7
SUM_ROW = 4
masked_score = -1e30
norm_eps = 1e-06
MESH = pl.DeviceIdType.MESH
f32, bf16, i32 = jnp.float32, jnp.bfloat16, jnp.int32


def iota(shape, axis):
    return lax.broadcasted_iota(i32, shape, axis)


def ones_where(mask, dtype=f32):
    return jnp.where(mask, 1.0, 0.0).astype(dtype)


def split2(x):
    hi = x.astype(bf16)
    return hi, (x - hi.astype(f32)).astype(bf16)


def split3(x):
    hi = x.astype(bf16).astype(f32)
    mid = (x - hi).astype(bf16).astype(f32)
    return hi, mid, x - hi - mid


def contract_last(a, b):
    return lax.dot_general(a, b, (((1,), (1,)), ((), ())), preferred_element_type=f32)


def matmul(a, b):
    return jnp.dot(a, b, preferred_element_type=f32)


def step_kernel(
    n_kv,
    n_tp,
    heads,
    per,
    prior_s,
    accepted_s,
    tokens_ref,
    gain_ref,
    wq_ref,
    wk_ref,
    wv_ref,
    wg_ref,
    bias_ref,
    wout_ref,
    parents_ref,
    k_hbm,
    v_hbm,
    cum_hbm,
    mixed_ref,
    newk_ref,
    newv_ref,
    kbuf,
    vbuf,
    cumbuf,
    part,
    gpart,
    arr1,
    garr1,
    half,
    ghalf,
    arr2,
    garr2,
    full,
    gfull,
    wall,
    parts_v,
    parts_s,
    got_v,
    got_s,
    mine,
    att,
    load_sems,
    s1_send,
    s1_recv,
    s2_send,
    s2_recv,
    s3_send,
    s3_recv,
    w_send,
    w_recv,
    cv_send,
    cv_recv,
    cs_send,
    cs_recv,
    ag_send,
    ag_recv,
):
    me = lax.axis_index("kv")
    tp = lax.axis_index("tp")
    n_chunks, rc, depth = tokens_ref.shape
    length = kbuf.shape[1]
    width = heads * HEAD
    lines = heads * PROPS
    cq = n_chunks // 4
    n_groups = n_kv // 4
    cpt = n_chunks // n_tp
    corner, group = lax.rem(me, 4), me // 4
    quarter = pl.ds(corner * cq, cq)

    barrier = pltpu.get_barrier_semaphore()
    for d in range(1, n_kv * n_tp):
        other = lax.rem(me * n_tp + tp + d, n_kv * n_tp)
        pl.semaphore_signal(
            barrier,
            inc=1,
            device_id={"kv": other // n_tp, "tp": lax.rem(other, n_tp)},
            device_id_type=MESH,
        )
    loads = []
    for c in range(n_chunks):
        span = pl.ds(c * per, per)
        for at, (source, target) in enumerate(((k_hbm, kbuf), (v_hbm, vbuf), (cum_hbm, cumbuf))):
            copy = pltpu.make_async_copy(source.at[span], target.at[span], load_sems.at[at, c])
            copy.start()
            loads.append(copy)

    def send(source, target, sems, at, kv=None, to_tp=None):
        where = {}
        if kv is not None:
            where["kv"] = kv
        if to_tp is not None:
            where["tp"] = to_tp
        copy = pltpu.make_async_remote_copy(
            src_ref=source,
            dst_ref=target,
            send_sem=sems[0].at[at],
            recv_sem=sems[1].at[at],
            device_id=where,
            device_id_type=MESH,
        )
        copy.start()
        return copy

    total_heads = bias_ref.shape[1]
    pick = (iota((8, total_heads), 1) == tp * heads + iota((8, total_heads), 0)) & (
        iota((8, total_heads), 0) < heads
    )
    if depth % LANES == 0:
        gate_w = wg_ref[:, pl.ds(pl.multiple_of(me * depth, depth), depth)]
        gate_w = matmul(ones_where(pick, bf16), gate_w).astype(bf16)
    else:
        gate_w = wg_ref[pl.ds(pl.multiple_of(me * depth, depth), depth), :]
        gate_w = contract_last(ones_where(pick, bf16), gate_w).astype(bf16)
    square_w = ones_where(iota((8, depth), 0) == SQUARE_ROW, bf16)
    floats = tokens_ref[...].reshape(n_chunks * rc, depth).astype(f32)
    scaled = (floats * gain_ref[...]).astype(bf16)

    def product(piece, w_ref):
        value = matmul(scaled, w_ref[...]).astype(bf16)
        part[piece] = value.reshape(n_chunks, rc, width)

    product(0, wq_ref)
    sq_hi, sq_lo = split2(floats * floats)
    gpart[...] = jnp.zeros_like(gpart)
    for c in range(n_chunks):
        rows = slice(c * rc, (c + 1) * rc)
        gpart[c, :, :rc] = (
            contract_last(gate_w, scaled[rows])
            + contract_last(square_w, sq_hi[rows])
            + contract_last(square_w, sq_lo[rows])
        )

    pl.semaphore_wait(barrier, n_kv * n_tp - 1)
    started = []

    def corner_sends(sources, targets, sems, piece):
        out = []
        for d in range(1, 4):
            there = lax.rem(corner + d, 4)
            out.append(
                send(
                    sources(there), targets(d), sems, piece * 3 + d - 1, kv=group * 4 + there
                )
            )
        started.extend(out)
        return out

    def first_stage(piece):
        return corner_sends(
            lambda there: part.at[piece, pl.ds(there * cq, cq)],
            lambda d: arr1.at[piece, d - 1],
            (s1_send, s1_recv),
            piece,
        )

    def group_sends(source, target, piece):
        out = []
        for d in range(1, n_groups):
            there = lax.rem(group + d, n_groups) * 4 + corner
            out.append(
                send(
                    source,
                    target(d),
                    (s2_send, s2_recv),
                    piece * (n_groups - 1) + d - 1,
                    kv=there,
                )
            )
        started.extend(out)
        return out

    def second_stage(piece, stage):
        for copy in stage:
            copy.wait_recv()
        total = part[piece, quarter].astype(f32)
        for d in range(3):
            total = total + arr1[piece, d].astype(f32)
        half[piece] = total.astype(bf16)
        return group_sends(half.at[piece], lambda d: arr2.at[piece, d - 1], piece)

    def third_stage(piece, stage, columns):
        for copy in stage:
            copy.wait_recv()
        total = half[piece].astype(f32)
        for d in range(n_groups - 1):
            total = total + arr2[piece, d].astype(f32)
        for j in range(cq):
            full[piece, corner * cq + j] = (total[j] * columns[j]).astype(bf16)
        return corner_sends(
            lambda there: full.at[piece, quarter],
            lambda d: full.at[piece, quarter],
            (s3_send, s3_recv),
            piece,
        )

    q1 = first_stage(0)
    g1 = corner_sends(
        lambda there: gpart.at[pl.ds(there * cq, cq)],
        lambda d: garr1.at[d - 1],
        (s1_send, s1_recv),
        3,
    )
    product(1, wk_ref)
    k1 = first_stage(1)
    product(2, wv_ref)

    slot = lax.rem(me, n_tp) * cpt + me // n_tp
    own = jnp.minimum(slot, n_chunks - 1)
    every = parents_ref[...]
    parent = jnp.concatenate(
        [
            jnp.sum(
                jnp.where(iota(every.shape, 1) == own * per + k, every, 0).astype(f32),
                axis=1,
                keepdims=True,
            ).astype(i32)
            for k in range(per)
        ],
        axis=0,
    )
    row, column = iota((rc, rc), 0), iota((rc, rc), 1)
    link = (parent + (row // PROPS) * PROPS == column) & (parent >= 0)
    reached = ones_where(link | (row == column))
    for squaring in range((PROPS - 1).bit_length()):
        reached = jnp.minimum(matmul(reached.astype(bf16), reached.astype(bf16)), 1.0)

    q2 = second_stage(0, q1)
    for copy in g1:
        copy.wait_recv()
    ghalf[...] = gpart[quarter] + garr1[0] + garr1[1] + garr1[2]
    g2 = group_sends(ghalf, lambda d: garr2.at[d - 1], 3)
    v1 = first_stage(2)
    w_copies = []
    for d in range(1, n_tp):
        w_copies.append(
            send(
                wout_ref, wall.at[tp], (w_send, w_recv), d - 1, to_tp=lax.rem(tp + d, n_tp)
            )
        )
    started.extend(w_copies)
    wall[tp] = wout_ref[...]

    for copy in g2:
        copy.wait_recv()
    gates = ghalf[...]
    for d in range(n_groups - 1):
        gates = gates + garr2[d]
    bias = jnp.sum(
        jnp.where(pick, jnp.broadcast_to(bias_ref[...], (8, total_heads)), 0.0),
        axis=1,
        keepdims=True,
    )
    inv_columns = []
    eye = iota((rc, LANES), 0) == iota((rc, LANES), 1)
    for j in range(cq):
        inv_row = lax.rsqrt(
            gates[j, SQUARE_ROW : SQUARE_ROW + 1, :] / (n_kv * depth) + norm_eps
        )
        pre = inv_row * gates[j] + bias
        gfull[corner * cq + j] = jnp.minimum(pre, 0.0) - jnp.log1p(jnp.exp(-jnp.abs(pre)))
        inv_columns.append(
            jnp.sum(
                jnp.where(eye, jnp.broadcast_to(inv_row, (rc, LANES)), 0.0),
                axis=1,
                keepdims=True,
            )
        )
    q3 = third_stage(0, q2, [c * HEAD ** (-0.5) for c in inv_columns])
    g3 = corner_sends(
        lambda there: gfull.at[quarter], lambda d: gfull.at[quarter], (s3_send, s3_recv), 3
    )
    k2 = second_stage(1, k1)
    v2 = second_stage(2, v1)

    lane_head = iota((PROPS, width), 1) // HEAD
    head_rows = [ones_where(lane_head == h) for h in range(heads)]
    head_mask = jnp.concatenate(head_rows, axis=0).astype(bf16)
    position = iota((lines, length), 1)
    short_position = iota((heads, length), 1)
    line_eye = iota((lines, LANES), 0) == iota((lines, LANES), 1)
    last_lane = iota((heads, LANES), 1) - LANES // 2
    last_mask = (last_lane >= 0) & (last_lane // PROPS == iota((heads, LANES), 0))
    tile_row = iota((8, LANES), 0)
    offset = me * length

    def as_row(value):
        return jnp.sum(jnp.where(line_eye, value, 0.0), axis=0, keepdims=True)

    def attend(owner):
        chunk = jnp.minimum(lax.rem(owner, n_tp) * cpt + owner // n_tp, n_chunks - 1)
        limits, scores = [], []
        for k in range(per):
            seq = chunk * per + k
            limits.append(prior_s[seq] + accepted_s[seq] - offset)
            query = full[0, chunk, k * PROPS : (k + 1) * PROPS, :]
            query = jnp.concatenate([query] * heads, axis=0) * head_mask
            scores.append(contract_last(query, kbuf[seq]))
        tile = jnp.zeros((8, LANES), f32)
        weights = []
        for k in range(per):
            seq = chunk * per + k
            cum = jnp.concatenate(
                [
                    jnp.broadcast_to(cumbuf[seq, h : h + 1, :], (PROPS, length))
                    for h in range(heads)
                ],
                axis=0,
            )
            value = jnp.where(position < limits[k], scores[k] - cum, masked_score)
            top = jnp.max(value, axis=1, keepdims=True)
            weight = jnp.exp(value - top)
            total = jnp.sum(weight, axis=1, keepdims=True)
            weights.append(weight.astype(bf16))
            last = jnp.sum(
                jnp.where(short_position == limits[k] - 1, cumbuf[seq], 0.0),
                axis=1,
                keepdims=True,
            )
            last_row = jnp.sum(jnp.where(last_mask, last, 0.0), axis=0, keepdims=True)
            tile = jnp.where(tile_row == k, as_row(top) + last_row, tile)
            tile = jnp.where(tile_row == SUM_ROW + k, as_row(total), tile)
        for k in range(per):
            values = matmul(weights[k], vbuf[chunk * per + k])
            picked = values[:PROPS] * head_rows[0]
            for h in range(1, heads):
                picked = picked + values[h * PROPS : (h + 1) * PROPS] * head_rows[h]
            parts_v[owner, k * PROPS : (k + 1) * PROPS, :] = picked.astype(bf16)
        parts_s[owner] = tile

    def part_copies(d):
        owner = lax.rem(me + d, n_kv)
        return [
            pltpu.make_async_remote_copy(
                src_ref=source.at[owner],
                dst_ref=target.at[d - 1],
                send_sem=send_sem.at[d - 1],
                recv_sem=recv_sem.at[d - 1],
                device_id={"kv": owner},
                device_id_type=MESH,
            )
            for source, target, send_sem, recv_sem in (
                (parts_v, got_v, cv_send, cv_recv),
                (parts_s, got_s, cs_send, cs_recv),
            )
        ]

    def attend_and_send(d):
        attend(lax.rem(me + d, n_kv))
        for copy in part_copies(d):
            copy.start()

    for copy in loads:
        copy.wait()
    for copy in q3:
        copy.wait_recv()
    attend_and_send(1)
    k3 = third_stage(1, k2, inv_columns)
    attend_and_send(2)
    v3 = third_stage(2, v2, inv_columns)

    def one(d, carry):
        attend_and_send(d)
        return carry

    lax.fori_loop(3, n_kv, one, 0)
    attend(me)

    for copy in g3 + k3:
        copy.wait_recv()
    gate_parts = jnp.concatenate(split3(gfull[own]), axis=0)[:, :rc].astype(bf16)
    tree_gates = contract_last(gate_parts, reached.astype(bf16))
    tree_gates = tree_gates[0:8] + tree_gates[8:16] + tree_gates[16:24]
    wide_rows = [ones_where(iota((rc, width), 1) // HEAD == h) for h in range(heads)]
    wide_mask = jnp.concatenate(wide_rows, axis=0).astype(bf16)
    tree_query = jnp.concatenate([full[0, own]] * heads, axis=0) * wide_mask
    tree = contract_last(tree_query, full[1, own])
    tree = tree - jnp.concatenate(
        [jnp.broadcast_to(tree_gates[h : h + 1, :], (rc, rc)) for h in range(heads)], axis=0
    )
    live = jnp.concatenate([reached] * heads, axis=0) > 0.5
    tree = jnp.where(live, tree, masked_score)
    tree_top = jnp.max(tree, axis=1, keepdims=True)
    tree_weights = jnp.where(live, jnp.exp(tree - tree_top), 0.0)
    tree_sum = jnp.sum(tree_weights, axis=1, keepdims=True)
    for copy in v3:
        copy.wait_recv()
    tree_values = matmul(tree_weights.astype(bf16), full[2, own])
    tree_picked = tree_values[:rc] * wide_rows[0]
    for h in range(1, heads):
        tree_picked = tree_picked + tree_values[h * rc : (h + 1) * rc] * wide_rows[h]
    newk_ref[...] = full[1]
    newv_ref[...] = full[2]

    def tile_of(value):
        rows = [
            as_row(
                jnp.concatenate(
                    [
                        value[h * rc + k * PROPS : h * rc + (k + 1) * PROPS]
                        for h in range(heads)
                    ],
                    axis=0,
                )
            )
            for k in range(per)
        ]
        rows = rows + [jnp.zeros((1, LANES), f32)] * (4 - per)
        return jnp.concatenate(rows, axis=0)

    tree_top_tile, tree_sum_tile = tile_of(tree_top), tile_of(tree_sum)

    landing = [part_copies(d) for d in range(1, n_kv)]
    for pair in landing:
        pair[1].wait_recv()
    tiles = [parts_s[me]] + [got_s[d] for d in range(n_kv - 1)]
    last = tiles[0][:4]
    for tile in tiles[1:]:
        last = last + tile[:4]
    last = pltpu.roll(last, LANES // 2, axis=1)
    lane_ok = iota((4, LANES), 1) < lines
    tops = [jnp.where(lane_ok, tile[:4], 0.0) for tile in tiles]
    tops.append(jnp.where(lane_ok, tree_top_tile - last, 0.0))
    sums = [jnp.where(lane_ok, tile[4:], 1.0) for tile in tiles] + [
        jnp.where(lane_ok, tree_sum_tile, 1.0)
    ]
    top = functools.reduce(jnp.maximum, tops)
    scales = [jnp.exp(t - top) for t in tops]
    total = functools.reduce(lambda a, b: a + b, [a * b for a, b in zip(scales, sums)])
    spread = ones_where(
        (iota((LANES, width), 0) // PROPS == iota((LANES, width), 1) // HEAD)
        & (iota((LANES, width), 0) < lines),
        bf16,
    )
    fits = (iota((PROPS, LANES), 1) % PROPS == iota((PROPS, LANES), 0)) & (
        iota((PROPS, LANES), 1) < lines
    )

    def expand(scale):
        scale = scale / total
        rows = jnp.concatenate(
            [
                jnp.where(fits, jnp.broadcast_to(scale[k : k + 1], (PROPS, LANES)), 0.0)
                for k in range(per)
            ],
            axis=0,
        )
        hi, lo = split2(rows)
        return matmul(hi, spread) + matmul(lo, spread)

    result = expand(scales[-1]) * tree_picked
    result = result + expand(scales[0]) * parts_v[me].astype(f32)
    for d in range(n_kv - 1):
        landing[d][0].wait_recv()
        result = result + expand(scales[d + 1]) * got_v[d].astype(f32)
    mine[...] = result.astype(bf16)

    target, early = lax.rem(me, n_tp), me // n_tp
    spreads = [
        pltpu.make_async_remote_copy(
            src_ref=mine,
            dst_ref=att.at[jnp.minimum(early, cpt - 1), tp],
            send_sem=ag_send.at[d],
            recv_sem=ag_recv.at[jnp.minimum(early, cpt - 1) * n_tp + tp],
            device_id={"kv": lax.rem(me + d, n_kv), "tp": target},
            device_id_type=MESH,
        )
        for d in range(n_kv)
    ]
    sends = early < cpt
    for d in range(1, n_kv):

        @pl.when(sends)
        def _(d=d):
            spreads[d].start()

    @pl.when(sends & (target != tp))
    def _():
        spreads[0].start()

    @pl.when(sends & (target == tp))
    def _():
        att[jnp.minimum(early, cpt - 1), tp] = mine[...]

    for copy in w_copies:
        copy.wait_recv()
    for at in range(cpt * n_tp):
        e, t = at // n_tp, at % n_tp

        @pl.when((me != e * n_tp + tp) | (tp != t))
        def _(at=at, e=e, t=t):
            pltpu.make_async_remote_copy(
                src_ref=mine,
                dst_ref=att.at[e, t],
                send_sem=ag_send.at[0],
                recv_sem=ag_recv.at[at],
                device_id={"kv": me, "tp": lax.rem(tp + 1, n_tp)},
                device_id_type=MESH,
            ).wait_recv()

    mixed = None
    for t in range(n_tp):
        rows = jnp.concatenate([att[e, t] for e in range(cpt)], axis=0)
        piece = matmul(rows, wall[t]).astype(bf16).astype(f32)
        mixed = piece if mixed is None else mixed + piece
    mixed_ref[...] = mixed.astype(bf16)

    for d in range(1, n_kv):

        @pl.when(sends)
        def _(d=d):
            spreads[d].wait_send()

    @pl.when(sends & (target != tp))
    def _():
        spreads[0].wait_send()

    for copy in started:
        copy.wait_send()
    for pair in landing:
        for copy in pair:
            copy.wait_send()


def write_kernel(
    prior_s,
    accepted_s,
    newk_ref,
    newv_ref,
    mixed_in,
    k_ref,
    v_ref,
    mixed_ref,
    ko_ref,
    vo_ref,
    windows,
    bulk_sems,
    window_sems,
):
    seq_count, length, width = k_ref.shape
    window = 2 * PROPS
    offset = lax.axis_index("kv") * length
    bulk = []
    for b in range(seq_count):
        for at, (source, target) in enumerate(((k_ref, ko_ref), (v_ref, vo_ref))):
            copy = pltpu.make_async_copy(source.at[b], target.at[b], bulk_sems.at[at, b])
            copy.start()
            bulk.append(copy)
    mixed_ref[...] = mixed_in[...]
    placed = []
    for b in range(seq_count):
        limit = prior_s[b] + accepted_s[b] - offset
        start = pl.multiple_of(jnp.clip(limit, 0, length - window) // PROPS * PROPS, PROPS)
        select = start + iota((window, PROPS), 0) - limit == iota((window, PROPS), 1)
        select = ones_where(select, bf16)
        slot = start + iota((window, width), 0) - limit
        inside = (slot >= 0) & (slot < PROPS)
        for at, (source, fresh, target) in enumerate(
            ((k_ref, newk_ref, ko_ref), (v_ref, newv_ref, vo_ref))
        ):
            rows = matmul(select, fresh[b * PROPS : (b + 1) * PROPS])
            old = source[b, pl.ds(start, window), :].astype(f32)
            windows[at, b] = jnp.where(inside, rows, old).astype(bf16)
            placed.append(
                pltpu.make_async_copy(
                    windows.at[at, b],
                    target.at[b, pl.ds(start, window), :],
                    window_sems.at[at, b],
                )
            )
    for first, second in zip(bulk, placed):
        first.wait()
        second.start()
    for copy in placed:
        copy.wait()


def shards(
    n_kv,
    n_tp,
    tokens,
    norm_gain,
    w_query,
    w_key,
    w_value,
    w_gate,
    gate_bias,
    w_out,
    keys_cache,
    values_cache,
    cum_gates,
    prior_len,
    accepted,
    parents,
):
    row_count, depth = tokens.shape
    seq_count, length, width = keys_cache.shape
    heads = width // HEAD
    per = next(p for p in range(1, 5) if seq_count % p == 0 and seq_count // p <= n_kv)
    n_chunks = seq_count // per
    rc = per * PROPS
    cq = n_chunks // 4
    n_groups = n_kv // 4
    cpt = n_chunks // n_tp
    columns = w_out.shape[1]
    vmem = pl.BlockSpec(memory_space=pltpu.VMEM)
    smem = pl.BlockSpec(memory_space=pltpu.SMEM)
    hbm = pl.BlockSpec(memory_space=pltpu.HBM)
    dma = pltpu.SemaphoreType.DMA

    mixed, new_keys, new_values = pl.pallas_call(
        functools.partial(step_kernel, n_kv, n_tp, heads, per),
        out_shape=(
            jax.ShapeDtypeStruct((cpt * rc, columns), bf16),
            jax.ShapeDtypeStruct((n_chunks, rc, width), bf16),
            jax.ShapeDtypeStruct((n_chunks, rc, width), bf16),
        ),
        in_specs=[smem] * 2 + [vmem] * 9 + [hbm] * 3,
        out_specs=[vmem] * 3,
        scratch_shapes=[
            pltpu.VMEM((seq_count, length, width), bf16),
            pltpu.VMEM((seq_count, length, width), bf16),
            pltpu.VMEM((seq_count, heads, length), f32),
            pltpu.VMEM((3, n_chunks, rc, width), bf16),
            pltpu.VMEM((n_chunks, 8, LANES), f32),
            pltpu.VMEM((3, 3, cq, rc, width), bf16),
            pltpu.VMEM((3, cq, 8, LANES), f32),
            pltpu.VMEM((3, cq, rc, width), bf16),
            pltpu.VMEM((cq, 8, LANES), f32),
            pltpu.VMEM((3, n_groups - 1, cq, rc, width), bf16),
            pltpu.VMEM((n_groups - 1, cq, 8, LANES), f32),
            pltpu.VMEM((3, n_chunks, rc, width), bf16),
            pltpu.VMEM((n_chunks, 8, LANES), f32),
            pltpu.VMEM((n_tp, width, columns), bf16),
            pltpu.VMEM((n_kv, rc, width), bf16),
            pltpu.VMEM((n_kv, 8, LANES), f32),
            pltpu.VMEM((n_kv - 1, rc, width), bf16),
            pltpu.VMEM((n_kv - 1, 8, LANES), f32),
            pltpu.VMEM((rc, width), bf16),
            pltpu.VMEM((cpt, n_tp, rc, width), bf16),
            dma((3, n_chunks)),
            dma((12,)),
            dma((12,)),
            dma((4 * (n_groups - 1),)),
            dma((4 * (n_groups - 1),)),
            dma((12,)),
            dma((12,)),
            dma((n_tp - 1,)),
            dma((n_tp - 1,)),
            dma((n_kv - 1,)),
            dma((n_kv - 1,)),
            dma((n_kv - 1,)),
            dma((n_kv - 1,)),
            dma((n_kv,)),
            dma((cpt * n_tp,)),
        ],
        compiler_params=pltpu.CompilerParams(
            collective_id=0, has_side_effects=True, vmem_limit_bytes=28 * 1024 * 1024
        ),
        name="step",
    )(
        *(
            pltpu.with_memory_space_constraint(value, pltpu.HBM)
            for value in (
                prior_len,
                accepted,
                tokens.reshape(n_chunks, rc, depth),
                norm_gain.reshape(1, depth),
                w_query,
                w_key,
                w_value,
                w_gate.T if depth % LANES == 0 else w_gate,
                gate_bias.reshape(1, -1),
                w_out,
                parents.T,
                keys_cache,
                values_cache,
                cum_gates,
            )
        ),
    )

    return pl.pallas_call(
        write_kernel,
        out_shape=(
            jax.ShapeDtypeStruct((cpt * rc, columns), bf16),
            jax.ShapeDtypeStruct(keys_cache.shape, bf16),
            jax.ShapeDtypeStruct(values_cache.shape, bf16),
        ),
        in_specs=[smem] * 2 + [vmem] * 5,
        out_specs=[vmem, hbm, hbm],
        scratch_shapes=[
            pltpu.VMEM((2, seq_count, 2 * PROPS, width), bf16),
            dma((2, seq_count)),
            dma((2, seq_count)),
        ],
        compiler_params=pltpu.CompilerParams(vmem_limit_bytes=8 * 1024 * 1024),
        name="write",
    )(
        pltpu.with_memory_space_constraint(prior_len, pltpu.HBM),
        pltpu.with_memory_space_constraint(accepted, pltpu.HBM),
        new_keys.reshape(row_count, width),
        new_values.reshape(row_count, width),
        mixed,
        keys_cache,
        values_cache,
    )


def solution(mesh):
    placed = (
        P(None, "kv"),
        P("kv"),
        P("kv", "tp"),
        P("kv", "tp"),
        P("kv", "tp"),
        P(),
        P(),
        P("tp", "kv"),
        P(None, "kv", "tp"),
        P(None, "kv", "tp"),
        P(None, "tp", "kv"),
        P(),
        P(),
        P(),
    )
    return jax.shard_map(
        functools.partial(shards, mesh.shape["kv"], mesh.shape["tp"]),
        mesh=mesh,
        in_specs=placed,
        out_specs=(P("tp", "kv"), P(None, "kv", "tp"), P(None, "kv", "tp")),
        check_vma=False,
    )
```

```python
import functools

import jax
import jax.numpy as jnp
from jax import lax
from jax.experimental import pallas as pl
from jax.experimental.pallas import tpu as pltpu
from jax.sharding import PartitionSpec as P

HEAD = 64
PROPS = 16
LANES = 128
SQUARE_ROW = 7
SUM_ROW = 4
masked_score = -1e30
norm_eps = 1e-06
MESH = pl.DeviceIdType.MESH
f32, bf16, i32 = jnp.float32, jnp.bfloat16, jnp.int32


def iota(shape, axis):
    return lax.broadcasted_iota(i32, shape, axis)


def ones_where(mask, dtype=f32):
    return jnp.where(mask, 1.0, 0.0).astype(dtype)


def split2(x):
    hi = x.astype(bf16)
    return hi, (x - hi.astype(f32)).astype(bf16)


def split3(x):
    hi = x.astype(bf16).astype(f32)
    mid = (x - hi).astype(bf16).astype(f32)
    return hi, mid, x - hi - mid


def contract_last(a, b):
    return lax.dot_general(a, b, (((1,), (1,)), ((), ())), preferred_element_type=f32)


def matmul(a, b):
    return jnp.dot(a, b, preferred_element_type=f32)


def step_kernel(
    n_kv,
    n_tp,
    heads,
    per,
    prior_s,
    accepted_s,
    tokens_hbm,
    gain_hbm,
    wq_hbm,
    wk_hbm,
    wv_hbm,
    wg_hbm,
    bias_hbm,
    wout_hbm,
    parents_hbm,
    k_hbm,
    v_hbm,
    cum_hbm,
    mixed_ref,
    newk_ref,
    newv_ref,
    tokens_ref,
    gain_ref,
    wq_ref,
    wk_ref,
    wv_ref,
    wg_ref,
    bias_ref,
    wout_ref,
    parents_ref,
    kbuf,
    vbuf,
    cumbuf,
    part,
    gpart,
    arr1,
    garr1,
    half,
    ghalf,
    arr2,
    garr2,
    full,
    gfull,
    wall,
    parts_v,
    parts_s,
    got_v,
    got_s,
    mine,
    att,
    input_sems,
    load_sems,
    s1_send,
    s1_recv,
    s2_send,
    s2_recv,
    s3_send,
    s3_recv,
    w_send,
    w_recv,
    cv_send,
    cv_recv,
    cs_send,
    cs_recv,
    ag_send,
    ag_recv,
):
    me = lax.axis_index("kv")
    tp = lax.axis_index("tp")
    n_chunks, rc, depth = tokens_ref.shape
    length = kbuf.shape[1]
    width = heads * HEAD
    lines = heads * PROPS
    cq = n_chunks // 4
    n_groups = n_kv // 4
    cpt = n_chunks // n_tp
    corner, group = lax.rem(me, 4), me // 4
    quarter = pl.ds(corner * cq, cq)

    aligned = n_tp == 4 and cpt == cq and n_kv == n_chunks
    inputs = []
    for at, (source, target) in enumerate(
        (
            (tokens_hbm, tokens_ref),
            (wq_hbm, wq_ref),
            (gain_hbm, gain_ref),
            (wg_hbm, wg_ref),
            (wk_hbm, wk_ref),
            (wv_hbm, wv_ref),
            (parents_hbm, parents_ref),
            (bias_hbm, bias_ref),
            (wout_hbm, wout_ref),
        )
    ):
        copy = pltpu.make_async_copy(source, target, input_sems.at[at])
        copy.start()
        inputs.append(copy)
    barrier = pltpu.get_barrier_semaphore()
    for d in range(1, n_kv * n_tp):
        other = lax.rem(me * n_tp + tp + d, n_kv * n_tp)
        pl.semaphore_signal(
            barrier,
            inc=1,
            device_id={"kv": other // n_tp, "tp": lax.rem(other, n_tp)},
            device_id_type=MESH,
        )

    def send(source, target, sems, at, kv=None, to_tp=None):
        where = {}
        if kv is not None:
            where["kv"] = kv
        if to_tp is not None:
            where["tp"] = to_tp
        copy = pltpu.make_async_remote_copy(
            src_ref=source,
            dst_ref=target,
            send_sem=sems[0].at[at],
            recv_sem=sems[1].at[at],
            device_id=where,
            device_id_type=MESH,
        )
        copy.start()
        return copy

    for copy in inputs[:3]:
        copy.wait()
    floats = tokens_ref[...].reshape(n_chunks * rc, depth).astype(f32)
    scaled = (floats * gain_ref[...]).astype(bf16)

    def product(piece, w_ref):
        value = matmul(scaled, w_ref[...]).astype(bf16)
        part[piece] = value.reshape(n_chunks, rc, width)

    product(0, wq_ref)
    pl.semaphore_wait(barrier, n_kv * n_tp - 1)
    started = []

    def corner_sends(sources, targets, sems, piece, j=0):
        out = []
        for d in range(1, 4):
            there = lax.rem(corner + d, 4)
            at = (piece * 3 + d - 1) * cq + j
            out.append(send(sources(there), targets(d), sems, at, kv=group * 4 + there))
        started.extend(out)
        return out

    def first_stage(piece, j, count):
        return corner_sends(
            lambda there: part.at[piece, pl.ds(there * cq + j, count)],
            lambda d: arr1.at[piece, d - 1, pl.ds(j, count)],
            (s1_send, s1_recv),
            piece,
            j,
        )

    def group_sends(source, target, piece, j=0):
        out = []
        for d in range(1, n_groups):
            there = lax.rem(group + d, n_groups) * 4 + corner
            at = (piece * (n_groups - 1) + d - 1) * cq + j
            out.append(send(source, target(d), (s2_send, s2_recv), at, kv=there))
        started.extend(out)
        return out

    def second_stage(piece, stage, j, count):
        for copy in stage:
            copy.wait_recv()
        span = pl.ds(j, count)
        total = part[piece, pl.ds(corner * cq + j, count)].astype(f32)
        for d in range(3):
            total = total + arr1[piece, d, span].astype(f32)
        half[piece, span] = total.astype(bf16)
        return group_sends(
            half.at[piece, span], lambda d: arr2.at[piece, d - 1, span], piece, j
        )

    def finish(piece, stage, columns, j, count):
        for copy in stage:
            copy.wait_recv()
        for i in range(j, j + count):
            total = half[piece, i].astype(f32)
            for d in range(n_groups - 1):
                total = total + arr2[piece, d, i].astype(f32)
            full[piece, corner * cq + i] = (total * columns[i]).astype(bf16)

    def third_stage(piece, j, count):
        span = pl.ds(corner * cq + j, count)
        return corner_sends(
            lambda there: full.at[piece, span],
            lambda d: full.at[piece, span],
            (s3_send, s3_recv),
            piece,
            j,
        )

    q1 = [first_stage(0, j, 1) for j in range(cq)]
    loads = []
    for c in range(n_chunks):
        span = pl.ds(c * per, per)
        for at, (source, target) in enumerate(((k_hbm, kbuf), (v_hbm, vbuf), (cum_hbm, cumbuf))):
            copy = pltpu.make_async_copy(source.at[span], target.at[span], load_sems.at[at, c])
            copy.start()
            loads.append(copy)
    for copy in inputs[3:]:
        copy.wait()
    total_heads = bias_ref.shape[1]
    pick = (iota((8, total_heads), 1) == tp * heads + iota((8, total_heads), 0)) & (
        iota((8, total_heads), 0) < heads
    )
    if depth % LANES == 0:
        gate_w = wg_ref[:, pl.ds(pl.multiple_of(me * depth, depth), depth)]
        gate_w = matmul(ones_where(pick, bf16), gate_w).astype(bf16)
    else:
        gate_w = wg_ref[pl.ds(pl.multiple_of(me * depth, depth), depth), :]
        gate_w = contract_last(ones_where(pick, bf16), gate_w).astype(bf16)
    square_w = ones_where(iota((8, depth), 0) == SQUARE_ROW, bf16)
    sq_hi, sq_lo = split2(floats * floats)
    gpart[...] = jnp.zeros_like(gpart)
    for c in range(n_chunks):
        rows = slice(c * rc, (c + 1) * rc)
        gpart[c, :, :rc] = (
            contract_last(gate_w, scaled[rows])
            + contract_last(square_w, sq_hi[rows])
            + contract_last(square_w, sq_lo[rows])
        )
    g1 = corner_sends(
        lambda there: gpart.at[pl.ds(there * cq, cq)],
        lambda d: garr1.at[d - 1],
        (s1_send, s1_recv),
        3,
    )
    product(1, wk_ref)
    k1 = first_stage(1, 0, cq)
    product(2, wv_ref)

    slot = lax.rem(me, n_tp) * cpt + me // n_tp
    own = jnp.minimum(slot, n_chunks - 1)
    every = parents_ref[...]
    parent = jnp.concatenate(
        [
            jnp.sum(
                jnp.where(iota(every.shape, 1) == own * per + k, every, 0).astype(f32),
                axis=1,
                keepdims=True,
            ).astype(i32)
            for k in range(per)
        ],
        axis=0,
    )
    row, column = iota((rc, rc), 0), iota((rc, rc), 1)
    link = (parent + (row // PROPS) * PROPS == column) & (parent >= 0)
    reached = ones_where(link | (row == column))
    for squaring in range((PROPS - 1).bit_length()):
        reached = jnp.minimum(matmul(reached.astype(bf16), reached.astype(bf16)), 1.0)

    q2 = [second_stage(0, q1[0], 0, 1)]
    for copy in g1:
        copy.wait_recv()
    ghalf[...] = gpart[quarter] + garr1[0] + garr1[1] + garr1[2]
    g2 = group_sends(ghalf, lambda d: garr2.at[d - 1], 3)
    for j in range(1, cq):
        q2.append(second_stage(0, q1[j], j, 1))
    v1 = first_stage(2, 0, cq)
    w_copies = []
    for d in range(1, n_tp):
        w_copies.append(
            send(
                wout_ref, wall.at[tp], (w_send, w_recv), d - 1, to_tp=lax.rem(tp + d, n_tp)
            )
        )
    started.extend(w_copies)
    wall[tp] = wout_ref[...]

    for copy in g2:
        copy.wait_recv()
    gates = ghalf[...]
    for d in range(n_groups - 1):
        gates = gates + garr2[d]
    bias = jnp.sum(
        jnp.where(pick, jnp.broadcast_to(bias_ref[...], (8, total_heads)), 0.0),
        axis=1,
        keepdims=True,
    )
    inv_columns = []
    eye = iota((rc, LANES), 0) == iota((rc, LANES), 1)
    for j in range(cq):
        inv_row = lax.rsqrt(
            gates[j, SQUARE_ROW : SQUARE_ROW + 1, :] / (n_kv * depth) + norm_eps
        )
        pre = inv_row * gates[j] + bias
        gfull[corner * cq + j] = jnp.minimum(pre, 0.0) - jnp.log1p(jnp.exp(-jnp.abs(pre)))
        inv_columns.append(
            jnp.sum(
                jnp.where(eye, jnp.broadcast_to(inv_row, (rc, LANES)), 0.0),
                axis=1,
                keepdims=True,
            )
        )
    scaled_columns = [c * HEAD ** (-0.5) for c in inv_columns]
    q3 = []
    for j in range(cq):
        finish(0, q2[j], scaled_columns, j, 1)
        q3.append(third_stage(0, j, 1))
    g3 = []
    if not aligned:
        g3 = corner_sends(
            lambda there: gfull.at[quarter],
            lambda d: gfull.at[quarter],
            (s3_send, s3_recv),
            3,
        )
    k2 = second_stage(1, k1, 0, cq)
    lane_head = iota((PROPS, width), 1) // HEAD
    head_rows = [ones_where(lane_head == h) for h in range(heads)]
    head_mask = jnp.concatenate(head_rows, axis=0).astype(bf16)
    position = iota((lines, length), 1)
    short_position = iota((heads, length), 1)
    line_eye = iota((lines, LANES), 0) == iota((lines, LANES), 1)
    last_lane = iota((heads, LANES), 1) - LANES // 2
    last_mask = (last_lane >= 0) & (last_lane // PROPS == iota((heads, LANES), 0))
    tile_row = iota((8, LANES), 0)
    offset = me * length

    def as_row(value):
        return jnp.sum(jnp.where(line_eye, value, 0.0), axis=0, keepdims=True)

    def attend(owner):
        chunk = jnp.minimum(lax.rem(owner, n_tp) * cpt + owner // n_tp, n_chunks - 1)
        limits, scores = [], []
        for k in range(per):
            seq = chunk * per + k
            limits.append(prior_s[seq] + accepted_s[seq] - offset)
            query = full[0, chunk, k * PROPS : (k + 1) * PROPS, :]
            query = jnp.concatenate([query] * heads, axis=0) * head_mask
            scores.append(contract_last(query, kbuf[seq]))
        tile = jnp.zeros((8, LANES), f32)
        weights = []
        for k in range(per):
            seq = chunk * per + k
            cum = jnp.concatenate(
                [
                    jnp.broadcast_to(cumbuf[seq, h : h + 1, :], (PROPS, length))
                    for h in range(heads)
                ],
                axis=0,
            )
            value = jnp.where(position < limits[k], scores[k] - cum, masked_score)
            top = jnp.max(value, axis=1, keepdims=True)
            weight = jnp.exp(value - top)
            total = jnp.sum(weight, axis=1, keepdims=True)
            weights.append(weight.astype(bf16))
            last = jnp.sum(
                jnp.where(short_position == limits[k] - 1, cumbuf[seq], 0.0),
                axis=1,
                keepdims=True,
            )
            last_row = jnp.sum(jnp.where(last_mask, last, 0.0), axis=0, keepdims=True)
            tile = jnp.where(tile_row == k, as_row(top) + last_row, tile)
            tile = jnp.where(tile_row == SUM_ROW + k, as_row(total), tile)
        for k in range(per):
            values = matmul(weights[k], vbuf[chunk * per + k])
            picked = values[:PROPS] * head_rows[0]
            for h in range(1, heads):
                picked = picked + values[h * PROPS : (h + 1) * PROPS] * head_rows[h]
            parts_v[owner, k * PROPS : (k + 1) * PROPS, :] = picked.astype(bf16)
        parts_s[owner] = tile

    def peer(at):
        there = lax.rem(corner + at + jnp.where(at < n_kv - 4, 0, 1), 4)
        return lax.rem(group + at // 4 + 1, n_groups) * 4 + there

    def part_copies(at):
        owner = peer(at)
        return [
            pltpu.make_async_remote_copy(
                src_ref=source.at[owner],
                dst_ref=target.at[at],
                send_sem=send_sem.at[at],
                recv_sem=recv_sem.at[at],
                device_id={"kv": owner},
                device_id_type=MESH,
            )
            for source, target, send_sem, recv_sem in (
                (parts_v, got_v, cv_send, cv_recv),
                (parts_s, got_s, cs_send, cs_recv),
            )
        ]

    def attend_and_send(at):
        attend(peer(at))
        for copy in part_copies(at):
            copy.start()

    for copy in loads:
        copy.wait()
    if aligned:
        attend_and_send(0)
        attend(me)
        v2 = second_stage(2, v1, 0, cq)
        for at in range(1, n_kv - 1):
            if at < 4:
                for stage in q3:
                    stage[3 - at].wait_recv()
            attend_and_send(at)
    else:
        v2 = second_stage(2, v1, 0, cq)
        for stage in q3:
            for copy in stage:
                copy.wait_recv()

        def one(at, carry):
            attend_and_send(at)
            return carry

        lax.fori_loop(0, n_kv - 1, one, 0)
        attend(me)
    finish(1, k2, inv_columns, 0, cq)
    finish(2, v2, inv_columns, 0, cq)
    upper = me >= n_kv // 2
    k3 = v3 = []
    if aligned:
        late = []
        for piece in (1, 2):
            for d in range(1, 4):
                there = lax.rem(corner + d, 4)
                at = (piece * 3 + d - 1) * cq
                late.append(
                    pltpu.make_async_remote_copy(
                        src_ref=full.at[piece, quarter],
                        dst_ref=full.at[piece, quarter],
                        send_sem=s3_send.at[at],
                        recv_sem=s3_recv.at[at],
                        device_id={"kv": group * 4 + there},
                        device_id_type=MESH,
                    )
                )

        @pl.when(upper)
        def _():
            for copy in late:
                copy.start()

    else:
        k3 = third_stage(1, 0, cq)
        v3 = third_stage(2, 0, cq)
        for copy in g3 + k3 + v3:
            copy.wait_recv()
    gate_parts = jnp.concatenate(split3(gfull[own]), axis=0)[:, :rc].astype(bf16)
    tree_gates = contract_last(gate_parts, reached.astype(bf16))
    tree_gates = tree_gates[0:8] + tree_gates[8:16] + tree_gates[16:24]
    wide_rows = [ones_where(iota((rc, width), 1) // HEAD == h) for h in range(heads)]
    wide_mask = jnp.concatenate(wide_rows, axis=0).astype(bf16)
    tree_query = jnp.concatenate([full[0, own]] * heads, axis=0) * wide_mask
    tree = contract_last(tree_query, full[1, own])
    tree = tree - jnp.concatenate(
        [jnp.broadcast_to(tree_gates[h : h + 1, :], (rc, rc)) for h in range(heads)], axis=0
    )
    live = jnp.concatenate([reached] * heads, axis=0) > 0.5
    tree = jnp.where(live, tree, masked_score)
    tree_top = jnp.max(tree, axis=1, keepdims=True)
    tree_weights = jnp.where(live, jnp.exp(tree - tree_top), 0.0)
    tree_sum = jnp.sum(tree_weights, axis=1, keepdims=True)
    tree_values = matmul(tree_weights.astype(bf16), full[2, own])
    tree_picked = tree_values[:rc] * wide_rows[0]
    for h in range(1, heads):
        tree_picked = tree_picked + tree_values[h * rc : (h + 1) * rc] * wide_rows[h]
    def tile_of(value):
        rows = [
            as_row(
                jnp.concatenate(
                    [
                        value[h * rc + k * PROPS : h * rc + (k + 1) * PROPS]
                        for h in range(heads)
                    ],
                    axis=0,
                )
            )
            for k in range(per)
        ]
        rows = rows + [jnp.zeros((1, LANES), f32)] * (4 - per)
        return jnp.concatenate(rows, axis=0)

    tree_top_tile, tree_sum_tile = tile_of(tree_top), tile_of(tree_sum)

    landing = [part_copies(at) for at in range(n_kv - 1)]
    for pair in landing:
        pair[1].wait_recv()
    tiles = [parts_s[me]] + [got_s[d] for d in range(n_kv - 1)]
    last = tiles[0][:4]
    for tile in tiles[1:]:
        last = last + tile[:4]
    last = pltpu.roll(last, LANES // 2, axis=1)
    lane_ok = iota((4, LANES), 1) < lines
    tops = [jnp.where(lane_ok, tile[:4], 0.0) for tile in tiles]
    tops.append(jnp.where(lane_ok, tree_top_tile - last, 0.0))
    sums = [jnp.where(lane_ok, tile[4:], 1.0) for tile in tiles] + [
        jnp.where(lane_ok, tree_sum_tile, 1.0)
    ]
    top = functools.reduce(jnp.maximum, tops)
    scales = [jnp.exp(t - top) for t in tops]
    total = functools.reduce(lambda a, b: a + b, [a * b for a, b in zip(scales, sums)])
    half_lane = iota((LANES, width), 0) % (LANES // 2)
    spread = ones_where(
        (half_lane // PROPS == iota((LANES, width), 1) // HEAD) & (half_lane < lines), bf16
    )
    fits = (iota((PROPS, LANES), 1) % PROPS == iota((PROPS, LANES), 0)) & (
        iota((PROPS, LANES), 1) % (LANES // 2) < lines
    )
    inverse = 1.0 / total
    low_half = iota((4, LANES), 1) < LANES // 2

    def expand(scale):
        hi, lo = split2(jnp.where(low_half, scale * inverse, 0.0))
        both = jnp.where(low_half, hi.astype(f32), pltpu.roll(lo.astype(f32), LANES // 2, axis=1))
        rows = jnp.concatenate(
            [
                jnp.where(fits, jnp.broadcast_to(both[k : k + 1], (PROPS, LANES)), 0.0)
                for k in range(per)
            ],
            axis=0,
        )
        return matmul(rows.astype(bf16), spread)

    expanded = [expand(scale) for scale in scales]
    result = expanded[-1] * tree_picked + expanded[0] * parts_v[me].astype(f32)
    for d in range(n_kv - 1):
        landing[d][0].wait_recv()
        result = result + expanded[d + 1] * got_v[d].astype(f32)
    mine[...] = result.astype(bf16)

    target, early = lax.rem(me, n_tp), me // n_tp
    spreads = [
        pltpu.make_async_remote_copy(
            src_ref=mine,
            dst_ref=att.at[jnp.minimum(early, cpt - 1), tp],
            send_sem=ag_send.at[d],
            recv_sem=ag_recv.at[jnp.minimum(early, cpt - 1) * n_tp + tp],
            device_id={"kv": lax.rem(me + d, n_kv), "tp": target},
            device_id_type=MESH,
        )
        for d in range(n_kv)
    ]
    sends = early < cpt
    for d in range(1, n_kv):

        @pl.when(sends)
        def _(d=d):
            spreads[d].start()

    @pl.when(sends & (target != tp))
    def _():
        spreads[0].start()

    @pl.when(sends & (target == tp))
    def _():
        att[jnp.minimum(early, cpt - 1), tp] = mine[...]

    for copy in w_copies:
        copy.wait_recv()
    for at in range(cpt * n_tp):
        e, t = at // n_tp, at % n_tp

        @pl.when((me != e * n_tp + tp) | (tp != t))
        def _(at=at, e=e, t=t):
            pltpu.make_async_remote_copy(
                src_ref=mine,
                dst_ref=att.at[e, t],
                send_sem=ag_send.at[0],
                recv_sem=ag_recv.at[at],
                device_id={"kv": me, "tp": lax.rem(tp + 1, n_tp)},
                device_id_type=MESH,
            ).wait_recv()

    mixed = None
    for t in range(n_tp):
        rows = jnp.concatenate([att[e, t] for e in range(cpt)], axis=0)
        piece = matmul(rows, wall[t]).astype(bf16).astype(f32)
        mixed = piece if mixed is None else mixed + piece
    mixed_ref[...] = mixed.astype(bf16)
    if aligned:

        @pl.when(upper)
        def _():
            for copy in late:
                copy.wait_recv()
            for copy in late:
                copy.wait_send()

    newk_ref[...] = full[1]
    newv_ref[...] = full[2]
    for d in range(1, n_kv):

        @pl.when(sends)
        def _(d=d):
            spreads[d].wait_send()

    @pl.when(sends & (target != tp))
    def _():
        spreads[0].wait_send()

    for copy in started:
        copy.wait_send()
    for pair in landing:
        for copy in pair:
            copy.wait_send()


def write_kernel(
    prior_s,
    accepted_s,
    newk_ref,
    newv_ref,
    mixed_in,
    k_ref,
    v_ref,
    mixed_ref,
    ko_ref,
    vo_ref,
    windows,
    bulk_sems,
    window_sems,
    mixed_sem,
):
    seq_count, length, width = k_ref.shape
    window = 2 * PROPS
    offset = lax.axis_index("kv") * length
    bulk = []
    for b in range(seq_count):
        for at, (source, target) in enumerate(((k_ref, ko_ref), (v_ref, vo_ref))):
            copy = pltpu.make_async_copy(source.at[b], target.at[b], bulk_sems.at[at, b])
            copy.start()
            bulk.append(copy)
    mixed_copy = pltpu.make_async_copy(mixed_in, mixed_ref, mixed_sem)
    mixed_copy.start()
    placed = []
    for b in range(seq_count):
        limit = prior_s[b] + accepted_s[b] - offset
        start = pl.multiple_of(jnp.clip(limit, 0, length - window) // PROPS * PROPS, PROPS)
        select = start + iota((window, PROPS), 0) - limit == iota((window, PROPS), 1)
        select = ones_where(select, bf16)
        slot = start + iota((window, width), 0) - limit
        inside = (slot >= 0) & (slot < PROPS)
        for at, (source, fresh, target) in enumerate(
            ((k_ref, newk_ref, ko_ref), (v_ref, newv_ref, vo_ref))
        ):
            rows = matmul(select, fresh[b * PROPS : (b + 1) * PROPS])
            old = source[b, pl.ds(start, window), :].astype(f32)
            windows[at, b] = jnp.where(inside, rows, old).astype(bf16)
            placed.append(
                pltpu.make_async_copy(
                    windows.at[at, b],
                    target.at[b, pl.ds(start, window), :],
                    window_sems.at[at, b],
                )
            )
    for first, second in zip(bulk, placed):
        first.wait()
        second.start()
    mixed_copy.wait()
    for copy in placed:
        copy.wait()


def shards(
    n_kv,
    n_tp,
    tokens,
    norm_gain,
    w_query,
    w_key,
    w_value,
    w_gate,
    gate_bias,
    w_out,
    keys_cache,
    values_cache,
    cum_gates,
    prior_len,
    accepted,
    parents,
):
    row_count, depth = tokens.shape
    seq_count, length, width = keys_cache.shape
    heads = width // HEAD
    per = next(p for p in range(1, 5) if seq_count % p == 0 and seq_count // p <= n_kv)
    n_chunks = seq_count // per
    rc = per * PROPS
    cq = n_chunks // 4
    n_groups = n_kv // 4
    cpt = n_chunks // n_tp
    columns = w_out.shape[1]
    vmem = pl.BlockSpec(memory_space=pltpu.VMEM)
    smem = pl.BlockSpec(memory_space=pltpu.SMEM)
    hbm = pl.BlockSpec(memory_space=pltpu.HBM)
    dma = pltpu.SemaphoreType.DMA

    inputs = (
        tokens.reshape(n_chunks, rc, depth),
        norm_gain.reshape(1, depth),
        w_query,
        w_key,
        w_value,
        w_gate.T if depth % LANES == 0 else w_gate,
        gate_bias.reshape(1, -1),
        w_out,
        parents.T,
    )
    mixed, new_keys, new_values = pl.pallas_call(
        functools.partial(step_kernel, n_kv, n_tp, heads, per),
        out_shape=(
            jax.ShapeDtypeStruct((cpt * rc, columns), bf16),
            jax.ShapeDtypeStruct((n_chunks, rc, width), bf16),
            jax.ShapeDtypeStruct((n_chunks, rc, width), bf16),
        ),
        in_specs=[smem] * 2 + [hbm] * 12,
        out_specs=[vmem] * 3,
        scratch_shapes=[pltpu.VMEM(value.shape, value.dtype) for value in inputs]
        + [
            pltpu.VMEM((seq_count, length, width), bf16),
            pltpu.VMEM((seq_count, length, width), bf16),
            pltpu.VMEM((seq_count, heads, length), f32),
            pltpu.VMEM((3, n_chunks, rc, width), bf16),
            pltpu.VMEM((n_chunks, 8, LANES), f32),
            pltpu.VMEM((3, 3, cq, rc, width), bf16),
            pltpu.VMEM((3, cq, 8, LANES), f32),
            pltpu.VMEM((3, cq, rc, width), bf16),
            pltpu.VMEM((cq, 8, LANES), f32),
            pltpu.VMEM((3, n_groups - 1, cq, rc, width), bf16),
            pltpu.VMEM((n_groups - 1, cq, 8, LANES), f32),
            pltpu.VMEM((3, n_chunks, rc, width), bf16),
            pltpu.VMEM((n_chunks, 8, LANES), f32),
            pltpu.VMEM((n_tp, width, columns), bf16),
            pltpu.VMEM((n_kv, rc, width), bf16),
            pltpu.VMEM((n_kv, 8, LANES), f32),
            pltpu.VMEM((n_kv - 1, rc, width), bf16),
            pltpu.VMEM((n_kv - 1, 8, LANES), f32),
            pltpu.VMEM((rc, width), bf16),
            pltpu.VMEM((cpt, n_tp, rc, width), bf16),
            dma((len(inputs),)),
            dma((3, n_chunks)),
            dma((12 * cq,)),
            dma((12 * cq,)),
            dma((4 * (n_groups - 1) * cq,)),
            dma((4 * (n_groups - 1) * cq,)),
            dma((12 * cq,)),
            dma((12 * cq,)),
            dma((n_tp - 1,)),
            dma((n_tp - 1,)),
            dma((n_kv - 1,)),
            dma((n_kv - 1,)),
            dma((n_kv - 1,)),
            dma((n_kv - 1,)),
            dma((n_kv,)),
            dma((cpt * n_tp,)),
        ],
        compiler_params=pltpu.CompilerParams(
            collective_id=0, has_side_effects=True, vmem_limit_bytes=28 * 1024 * 1024
        ),
        name="step",
    )(
        *(
            pltpu.with_memory_space_constraint(value, pltpu.HBM)
            for value in (
                prior_len,
                accepted,
                *inputs,
                keys_cache,
                values_cache,
                cum_gates,
            )
        ),
    )

    return pl.pallas_call(
        write_kernel,
        out_shape=(
            jax.ShapeDtypeStruct((cpt * rc, columns), bf16),
            jax.ShapeDtypeStruct(keys_cache.shape, bf16),
            jax.ShapeDtypeStruct(values_cache.shape, bf16),
        ),
        in_specs=[smem] * 2 + [vmem] * 5,
        out_specs=[hbm, hbm, hbm],
        scratch_shapes=[
            pltpu.VMEM((2, seq_count, 2 * PROPS, width), bf16),
            dma((2, seq_count)),
            dma((2, seq_count)),
            dma(()),
        ],
        compiler_params=pltpu.CompilerParams(vmem_limit_bytes=8 * 1024 * 1024),
        name="write",
    )(
        pltpu.with_memory_space_constraint(prior_len, pltpu.HBM),
        pltpu.with_memory_space_constraint(accepted, pltpu.HBM),
        new_keys.reshape(row_count, width),
        new_values.reshape(row_count, width),
        mixed,
        keys_cache,
        values_cache,
    )


def solution(mesh):
    placed = (
        P(None, "kv"),
        P("kv"),
        P("kv", "tp"),
        P("kv", "tp"),
        P("kv", "tp"),
        P(),
        P(),
        P("tp", "kv"),
        P(None, "kv", "tp"),
        P(None, "kv", "tp"),
        P(None, "tp", "kv"),
        P(),
        P(),
        P(),
    )
    return jax.shard_map(
        functools.partial(shards, mesh.shape["kv"], mesh.shape["tp"]),
        mesh=mesh,
        in_specs=placed,
        out_specs=(P("tp", "kv"), P(None, "kv", "tp"), P(None, "kv", "tp")),
        check_vma=False,
    )
```

```python
import functools

import jax
import jax.numpy as jnp
from jax import lax
from jax.experimental import pallas as pl
from jax.experimental.pallas import tpu as pltpu
from jax.sharding import PartitionSpec as P

HEAD = 64
PROPS = 16
LANES = 128
SQUARE_ROW = 7
SUM_ROW = 4
masked_score = -1e30
norm_eps = 1e-06
MESH = pl.DeviceIdType.MESH
f32, bf16, i32 = jnp.float32, jnp.bfloat16, jnp.int32


def iota(shape, axis):
    return lax.broadcasted_iota(i32, shape, axis)


def ones_where(mask, dtype=f32):
    return jnp.where(mask, 1.0, 0.0).astype(dtype)


def split2(x):
    hi = x.astype(bf16)
    return hi, (x - hi.astype(f32)).astype(bf16)


def split3(x):
    hi = x.astype(bf16).astype(f32)
    mid = (x - hi).astype(bf16).astype(f32)
    return hi, mid, x - hi - mid


def contract_last(a, b):
    return lax.dot_general(a, b, (((1,), (1,)), ((), ())), preferred_element_type=f32)


def matmul(a, b):
    return jnp.dot(a, b, preferred_element_type=f32)


def step_kernel(
    n_kv,
    n_tp,
    heads,
    per,
    prior_hbm,
    accepted_hbm,
    tokens_hbm,
    gain_hbm,
    wq_hbm,
    wk_hbm,
    wv_hbm,
    wg_hbm,
    bias_hbm,
    wout_hbm,
    parents_hbm,
    k_hbm,
    v_hbm,
    cum_hbm,
    mixed_ref,
    newk_ref,
    newv_ref,
    tokens_ref,
    gain_ref,
    wq_ref,
    wk_ref,
    wv_ref,
    wg_ref,
    bias_ref,
    wout_ref,
    parents_ref,
    prior_s,
    accepted_s,
    kbuf,
    vbuf,
    cumbuf,
    part,
    gpart,
    arr1,
    garr1,
    half,
    ghalf,
    arr2,
    garr2,
    full,
    gfull,
    wall,
    parts_v,
    parts_s,
    got_v,
    got_s,
    mine,
    att,
    input_sems,
    load_sems,
    s1_send,
    s1_recv,
    s2_send,
    s2_recv,
    s3_send,
    s3_recv,
    w_send,
    w_recv,
    cv_send,
    cv_recv,
    cs_send,
    cs_recv,
    ag_send,
    ag_recv,
):
    me = lax.axis_index("kv")
    tp = lax.axis_index("tp")
    n_chunks, rc, depth = tokens_ref.shape
    length = kbuf.shape[1]
    width = heads * HEAD
    lines = heads * PROPS
    cq = n_chunks // 4
    n_groups = n_kv // 4
    cpt = n_chunks // n_tp
    corner, group = lax.rem(me, 4), me // 4
    quarter = pl.ds(corner * cq, cq)
    order = [lax.rem(group + 1 + i, cq) for i in range(cq)]

    aligned = n_tp == 4 and cpt == cq and n_kv == n_chunks
    inputs = []
    for at, (source, target) in enumerate(
        (
            (tokens_hbm, tokens_ref),
            (wq_hbm, wq_ref),
            (gain_hbm, gain_ref),
            (wg_hbm, wg_ref),
            (wk_hbm, wk_ref),
            (wv_hbm, wv_ref),
            (parents_hbm, parents_ref),
            (bias_hbm, bias_ref),
            (wout_hbm, wout_ref),
            (prior_hbm, prior_s),
            (accepted_hbm, accepted_s),
        )
    ):
        copy = pltpu.make_async_copy(source, target, input_sems.at[at])
        copy.start()
        inputs.append(copy)
    barrier = pltpu.get_barrier_semaphore()
    for d in range(1, n_kv * n_tp):
        other = lax.rem(me * n_tp + tp + d, n_kv * n_tp)
        pl.semaphore_signal(
            barrier,
            inc=1,
            device_id={"kv": other // n_tp, "tp": lax.rem(other, n_tp)},
            device_id_type=MESH,
        )

    def send(source, target, sems, at, kv=None, to_tp=None):
        where = {}
        if kv is not None:
            where["kv"] = kv
        if to_tp is not None:
            where["tp"] = to_tp
        copy = pltpu.make_async_remote_copy(
            src_ref=source,
            dst_ref=target,
            send_sem=sems[0].at[at],
            recv_sem=sems[1].at[at],
            device_id=where,
            device_id_type=MESH,
        )
        copy.start()
        return copy

    for copy in inputs[:3]:
        copy.wait()
    floats = tokens_ref[...].reshape(n_chunks * rc, depth).astype(f32)
    scaled = (floats * gain_ref[...]).astype(bf16)

    def product(piece, w_ref):
        value = matmul(scaled, w_ref[...]).astype(bf16)
        part[piece] = value.reshape(n_chunks, rc, width)

    product(0, wq_ref)
    pl.semaphore_wait(barrier, n_kv * n_tp - 1)
    started = []

    def corner_sends(sources, targets, sems, piece, j=0):
        out = []
        for d in range(1, 4):
            there = lax.rem(corner + d, 4)
            at = (piece * 3 + d - 1) * cq + j
            out.append(send(sources(there), targets(d), sems, at, kv=group * 4 + there))
        started.extend(out)
        return out

    def first_stage(piece, j, count):
        return corner_sends(
            lambda there: part.at[piece, pl.ds(there * cq + j, count)],
            lambda d: arr1.at[piece, d - 1, pl.ds(j, count)],
            (s1_send, s1_recv),
            piece,
            j,
        )

    def group_sends(source, target, piece, j=0):
        out = []
        for d in range(1, n_groups):
            there = lax.rem(group + d, n_groups) * 4 + corner
            at = (piece * (n_groups - 1) + d - 1) * cq + j
            out.append(send(source, target(d), (s2_send, s2_recv), at, kv=there))
        started.extend(out)
        return out

    def second_stage(piece, stage, j, count):
        for copy in stage:
            copy.wait_recv()
        span = pl.ds(j, count)
        total = part[piece, pl.ds(corner * cq + j, count)].astype(f32)
        for d in range(3):
            total = total + arr1[piece, d, span].astype(f32)
        half[piece, span] = total.astype(bf16)
        return group_sends(
            half.at[piece, span], lambda d: arr2.at[piece, d - 1, span], piece, j
        )

    def finish(piece, stage, columns, spots):
        for copy in stage:
            copy.wait_recv()
        for j, scale in zip(spots, columns):
            total = half[piece, j].astype(f32)
            for d in range(n_groups - 1):
                total = total + arr2[piece, d, j].astype(f32)
            full[piece, corner * cq + j] = (total * scale).astype(bf16)

    def third_stage(piece, j, count):
        span = pl.ds(corner * cq + j, count)
        return corner_sends(
            lambda there: full.at[piece, span],
            lambda d: full.at[piece, span],
            (s3_send, s3_recv),
            piece,
            j,
        )

    q1 = [first_stage(0, j, 1) for j in order]
    loads = []
    for c in range(n_chunks):
        span = pl.ds(c * per, per)
        for at, (source, target) in enumerate(((k_hbm, kbuf), (v_hbm, vbuf), (cum_hbm, cumbuf))):
            copy = pltpu.make_async_copy(source.at[span], target.at[span], load_sems.at[at, c])
            copy.start()
            loads.append(copy)
    for copy in inputs[3:]:
        copy.wait()
    total_heads = bias_ref.shape[1]
    pick = (iota((8, total_heads), 1) == tp * heads + iota((8, total_heads), 0)) & (
        iota((8, total_heads), 0) < heads
    )
    if depth % LANES == 0:
        gate_w = wg_ref[:, pl.ds(pl.multiple_of(me * depth, depth), depth)]
        gate_w = matmul(ones_where(pick, bf16), gate_w).astype(bf16)
    else:
        gate_w = wg_ref[pl.ds(pl.multiple_of(me * depth, depth), depth), :]
        gate_w = contract_last(ones_where(pick, bf16), gate_w).astype(bf16)
    square_w = ones_where(iota((8, depth), 0) == SQUARE_ROW, bf16)
    sq_hi, sq_lo = split2(floats * floats)
    gpart[...] = jnp.zeros_like(gpart)
    for c in range(n_chunks):
        rows = slice(c * rc, (c + 1) * rc)
        gpart[c, :, :rc] = (
            contract_last(gate_w, scaled[rows])
            + contract_last(square_w, sq_hi[rows])
            + contract_last(square_w, sq_lo[rows])
        )
    g1 = corner_sends(
        lambda there: gpart.at[pl.ds(there * cq, cq)],
        lambda d: garr1.at[d - 1],
        (s1_send, s1_recv),
        3,
    )
    product(1, wk_ref)
    k1 = first_stage(1, 0, cq)
    product(2, wv_ref)

    slot = lax.rem(me, n_tp) * cpt + me // n_tp
    own = jnp.minimum(slot, n_chunks - 1)
    every = parents_ref[...]
    parent = jnp.concatenate(
        [
            jnp.sum(
                jnp.where(iota(every.shape, 1) == own * per + k, every, 0).astype(f32),
                axis=1,
                keepdims=True,
            ).astype(i32)
            for k in range(per)
        ],
        axis=0,
    )
    row, column = iota((rc, rc), 0), iota((rc, rc), 1)
    link = (parent + (row // PROPS) * PROPS == column) & (parent >= 0)
    reached = ones_where(link | (row == column))
    for squaring in range((PROPS - 1).bit_length()):
        reached = jnp.minimum(matmul(reached.astype(bf16), reached.astype(bf16)), 1.0)

    q2 = [second_stage(0, q1[0], order[0], 1)]
    for copy in g1:
        copy.wait_recv()
    ghalf[...] = gpart[quarter] + garr1[0] + garr1[1] + garr1[2]
    g2 = group_sends(ghalf, lambda d: garr2.at[d - 1], 3)
    for i in range(1, cq):
        q2.append(second_stage(0, q1[i], order[i], 1))
    v1 = first_stage(2, 0, cq)
    w_copies = []
    for d in range(1, n_tp):
        w_copies.append(
            send(
                wout_ref, wall.at[tp], (w_send, w_recv), d - 1, to_tp=lax.rem(tp + d, n_tp)
            )
        )
    started.extend(w_copies)
    wall[tp] = wout_ref[...]

    for copy in g2:
        copy.wait_recv()
    bias = jnp.sum(
        jnp.where(pick, jnp.broadcast_to(bias_ref[...], (8, total_heads)), 0.0),
        axis=1,
        keepdims=True,
    )
    inv_columns = []
    eye = iota((rc, LANES), 0) == iota((rc, LANES), 1)
    for j in order:
        gates = ghalf[j]
        for d in range(n_groups - 1):
            gates = gates + garr2[d, j]
        inv_row = lax.rsqrt(gates[SQUARE_ROW : SQUARE_ROW + 1, :] / (n_kv * depth) + norm_eps)
        pre = inv_row * gates + bias
        gfull[corner * cq + j] = jnp.minimum(pre, 0.0) - jnp.log1p(jnp.exp(-jnp.abs(pre)))
        inv_columns.append(
            jnp.sum(
                jnp.where(eye, jnp.broadcast_to(inv_row, (rc, LANES)), 0.0),
                axis=1,
                keepdims=True,
            )
        )
    scaled_columns = [c * HEAD ** (-0.5) for c in inv_columns]
    q3 = []
    for i in range(cq):
        finish(0, q2[i], scaled_columns[i : i + 1], order[i : i + 1])
        q3.append(third_stage(0, order[i], 1))
    g3 = []
    if not aligned:
        g3 = corner_sends(
            lambda there: gfull.at[quarter],
            lambda d: gfull.at[quarter],
            (s3_send, s3_recv),
            3,
        )
    k2 = second_stage(1, k1, 0, cq)
    lane_head = iota((PROPS, width), 1) // HEAD
    head_rows = [ones_where(lane_head == h) for h in range(heads)]
    head_mask = jnp.concatenate(head_rows, axis=0).astype(bf16)
    position = iota((lines, length), 1)
    short_position = iota((heads, length), 1)
    line_eye = iota((lines, LANES), 0) == iota((lines, LANES), 1)
    last_lane = iota((heads, LANES), 1) - LANES // 2
    last_mask = (last_lane >= 0) & (last_lane // PROPS == iota((heads, LANES), 0))
    tile_row = iota((8, LANES), 0)
    offset = me * length

    def as_row(value):
        return jnp.sum(jnp.where(line_eye, value, 0.0), axis=0, keepdims=True)

    def attend(owner):
        chunk = jnp.minimum(lax.rem(owner, n_tp) * cpt + owner // n_tp, n_chunks - 1)
        limits, scores = [], []
        for k in range(per):
            seq = chunk * per + k
            limits.append(prior_s[seq] + accepted_s[seq] - offset)
            query = full[0, chunk, k * PROPS : (k + 1) * PROPS, :]
            query = jnp.concatenate([query] * heads, axis=0) * head_mask
            scores.append(contract_last(query, kbuf[seq]))
        tile = jnp.zeros((8, LANES), f32)
        weights = []
        for k in range(per):
            seq = chunk * per + k
            cum = jnp.concatenate(
                [
                    jnp.broadcast_to(cumbuf[seq, h : h + 1, :], (PROPS, length))
                    for h in range(heads)
                ],
                axis=0,
            )
            value = jnp.where(position < limits[k], scores[k] - cum, masked_score)
            top = jnp.max(value, axis=1, keepdims=True)
            weight = jnp.exp(value - top)
            total = jnp.sum(weight, axis=1, keepdims=True)
            weights.append(weight.astype(bf16))
            last = jnp.sum(
                jnp.where(short_position == limits[k] - 1, cumbuf[seq], 0.0),
                axis=1,
                keepdims=True,
            )
            last_row = jnp.sum(jnp.where(last_mask, last, 0.0), axis=0, keepdims=True)
            tile = jnp.where(tile_row == k, as_row(top) + last_row, tile)
            tile = jnp.where(tile_row == SUM_ROW + k, as_row(total), tile)
        for k in range(per):
            values = matmul(weights[k], vbuf[chunk * per + k])
            picked = values[:PROPS] * head_rows[0]
            for h in range(1, heads):
                picked = picked + values[h * PROPS : (h + 1) * PROPS] * head_rows[h]
            parts_v[owner, k * PROPS : (k + 1) * PROPS, :] = picked.astype(bf16)
        parts_s[owner] = tile

    def peer(at):
        there = lax.rem(corner + at + jnp.where(at < n_kv - 4, 0, 1), 4)
        return lax.rem(group + at // 4 + 1, n_groups) * 4 + there

    def part_copies(at):
        owner = peer(at)
        return [
            pltpu.make_async_remote_copy(
                src_ref=source.at[owner],
                dst_ref=target.at[at],
                send_sem=send_sem.at[at],
                recv_sem=recv_sem.at[at],
                device_id={"kv": owner},
                device_id_type=MESH,
            )
            for source, target, send_sem, recv_sem in (
                (parts_v, got_v, cv_send, cv_recv),
                (parts_s, got_s, cs_send, cs_recv),
            )
        ]

    def attend_and_send(at):
        attend(peer(at))
        for copy in part_copies(at):
            copy.start()

    for copy in loads:
        copy.wait()
    if aligned:
        attend_and_send(0)
        attend(me)
        v2 = second_stage(2, v1, 0, cq)
        for at in range(1, n_kv - 1):
            if at < 4:
                q3[0][3 - at].wait_recv()
            else:
                q3[1][2 - at % 4].wait_recv()
            attend_and_send(at)
    else:
        v2 = second_stage(2, v1, 0, cq)
        for stage in q3:
            for copy in stage:
                copy.wait_recv()

        def one(at, carry):
            attend_and_send(at)
            return carry

        lax.fori_loop(0, n_kv - 1, one, 0)
        attend(me)
    finish(1, k2, inv_columns, order)
    finish(2, v2, inv_columns, order)
    upper = me >= n_kv // 2
    k3 = v3 = []
    if aligned:
        late = []
        for piece in (1, 2):
            for d in range(1, 4):
                there = lax.rem(corner + d, 4)
                at = (piece * 3 + d - 1) * cq
                late.append(
                    pltpu.make_async_remote_copy(
                        src_ref=full.at[piece, quarter],
                        dst_ref=full.at[piece, quarter],
                        send_sem=s3_send.at[at],
                        recv_sem=s3_recv.at[at],
                        device_id={"kv": group * 4 + there},
                        device_id_type=MESH,
                    )
                )

        @pl.when(upper)
        def _():
            for copy in late:
                copy.start()

    else:
        k3 = third_stage(1, 0, cq)
        v3 = third_stage(2, 0, cq)
        for copy in g3 + k3 + v3:
            copy.wait_recv()
    gate_parts = jnp.concatenate(split3(gfull[own]), axis=0)[:, :rc].astype(bf16)
    tree_gates = contract_last(gate_parts, reached.astype(bf16))
    tree_gates = tree_gates[0:8] + tree_gates[8:16] + tree_gates[16:24]
    wide_rows = [ones_where(iota((rc, width), 1) // HEAD == h) for h in range(heads)]
    wide_mask = jnp.concatenate(wide_rows, axis=0).astype(bf16)
    tree_query = jnp.concatenate([full[0, own]] * heads, axis=0) * wide_mask
    tree = contract_last(tree_query, full[1, own])
    tree = tree - jnp.concatenate(
        [jnp.broadcast_to(tree_gates[h : h + 1, :], (rc, rc)) for h in range(heads)], axis=0
    )
    live = jnp.concatenate([reached] * heads, axis=0) > 0.5
    tree = jnp.where(live, tree, masked_score)
    tree_top = jnp.max(tree, axis=1, keepdims=True)
    tree_weights = jnp.where(live, jnp.exp(tree - tree_top), 0.0)
    tree_sum = jnp.sum(tree_weights, axis=1, keepdims=True)
    tree_values = matmul(tree_weights.astype(bf16), full[2, own])
    tree_picked = tree_values[:rc] * wide_rows[0]
    for h in range(1, heads):
        tree_picked = tree_picked + tree_values[h * rc : (h + 1) * rc] * wide_rows[h]
    def tile_of(value):
        rows = [
            as_row(
                jnp.concatenate(
                    [
                        value[h * rc + k * PROPS : h * rc + (k + 1) * PROPS]
                        for h in range(heads)
                    ],
                    axis=0,
                )
            )
            for k in range(per)
        ]
        rows = rows + [jnp.zeros((1, LANES), f32)] * (4 - per)
        return jnp.concatenate(rows, axis=0)

    tree_top_tile, tree_sum_tile = tile_of(tree_top), tile_of(tree_sum)

    landing = [part_copies(at) for at in range(n_kv - 1)]
    for pair in landing:
        pair[1].wait_recv()
    tiles = [parts_s[me]] + [got_s[d] for d in range(n_kv - 1)]
    last = tiles[0][:4]
    for tile in tiles[1:]:
        last = last + tile[:4]
    last = pltpu.roll(last, LANES // 2, axis=1)
    lane_ok = iota((4, LANES), 1) < lines
    tops = [jnp.where(lane_ok, tile[:4], 0.0) for tile in tiles]
    tops.append(jnp.where(lane_ok, tree_top_tile - last, 0.0))
    sums = [jnp.where(lane_ok, tile[4:], 1.0) for tile in tiles] + [
        jnp.where(lane_ok, tree_sum_tile, 1.0)
    ]
    top = functools.reduce(jnp.maximum, tops)
    scales = [jnp.exp(t - top) for t in tops]
    total = functools.reduce(lambda a, b: a + b, [a * b for a, b in zip(scales, sums)])
    half_lane = iota((LANES, width), 0) % (LANES // 2)
    spread = ones_where(
        (half_lane // PROPS == iota((LANES, width), 1) // HEAD) & (half_lane < lines), bf16
    )
    fits = (iota((PROPS, LANES), 1) % PROPS == iota((PROPS, LANES), 0)) & (
        iota((PROPS, LANES), 1) % (LANES // 2) < lines
    )
    inverse = 1.0 / total
    low_half = iota((4, LANES), 1) < LANES // 2

    def expand(scale):
        hi, lo = split2(jnp.where(low_half, scale * inverse, 0.0))
        both = jnp.where(low_half, hi.astype(f32), pltpu.roll(lo.astype(f32), LANES // 2, axis=1))
        rows = jnp.concatenate(
            [
                jnp.where(fits, jnp.broadcast_to(both[k : k + 1], (PROPS, LANES)), 0.0)
                for k in range(per)
            ],
            axis=0,
        )
        return matmul(rows.astype(bf16), spread)

    expanded = [expand(scale) for scale in scales]
    result = expanded[-1] * tree_picked + expanded[0] * parts_v[me].astype(f32)
    for d in range(n_kv - 1):
        landing[d][0].wait_recv()
        result = result + expanded[d + 1] * got_v[d].astype(f32)
    mine[...] = result.astype(bf16)

    target, early = lax.rem(me, n_tp), me // n_tp
    spreads = [
        pltpu.make_async_remote_copy(
            src_ref=mine,
            dst_ref=att.at[jnp.minimum(early, cpt - 1), tp],
            send_sem=ag_send.at[d],
            recv_sem=ag_recv.at[jnp.minimum(early, cpt - 1) * n_tp + tp],
            device_id={"kv": peer(d - 1) if d > 0 else me, "tp": target},
            device_id_type=MESH,
        )
        for d in range(n_kv)
    ]
    sends = early < cpt
    for d in range(1, n_kv):

        @pl.when(sends)
        def _(d=d):
            spreads[d].start()

    @pl.when(sends & (target != tp))
    def _():
        spreads[0].start()

    @pl.when(sends & (target == tp))
    def _():
        att[jnp.minimum(early, cpt - 1), tp] = mine[...]

    for copy in w_copies:
        copy.wait_recv()
    for at in range(cpt * n_tp):
        e, t = at // n_tp, at % n_tp

        @pl.when((me != e * n_tp + tp) | (tp != t))
        def _(at=at, e=e, t=t):
            pltpu.make_async_remote_copy(
                src_ref=mine,
                dst_ref=att.at[e, t],
                send_sem=ag_send.at[0],
                recv_sem=ag_recv.at[at],
                device_id={"kv": me, "tp": lax.rem(tp + 1, n_tp)},
                device_id_type=MESH,
            ).wait_recv()

    mixed = None
    for t in range(n_tp):
        rows = jnp.concatenate([att[e, t] for e in range(cpt)], axis=0)
        piece = matmul(rows, wall[t]).astype(bf16).astype(f32)
        mixed = piece if mixed is None else mixed + piece
    mixed_ref[...] = mixed.astype(bf16)
    if aligned:

        @pl.when(upper)
        def _():
            for copy in late:
                copy.wait_recv()
            for copy in late:
                copy.wait_send()

    newk_ref[...] = full[1]
    newv_ref[...] = full[2]
    for d in range(1, n_kv):

        @pl.when(sends)
        def _(d=d):
            spreads[d].wait_send()

    @pl.when(sends & (target != tp))
    def _():
        spreads[0].wait_send()

    for copy in started:
        copy.wait_send()
    for pair in landing:
        for copy in pair:
            copy.wait_send()


def write_kernel(
    prior_hbm,
    accepted_hbm,
    newk_ref,
    newv_ref,
    mixed_in,
    k_ref,
    v_ref,
    mixed_ref,
    ko_ref,
    vo_ref,
    prior_s,
    accepted_s,
    windows,
    scalar_sems,
    bulk_sems,
    window_sems,
    mixed_sem,
):
    seq_count, length, width = k_ref.shape
    window = 2 * PROPS
    offset = lax.axis_index("kv") * length
    scalars = [
        pltpu.make_async_copy(prior_hbm, prior_s, scalar_sems.at[0]),
        pltpu.make_async_copy(accepted_hbm, accepted_s, scalar_sems.at[1]),
    ]
    for copy in scalars:
        copy.start()
    bulk = []
    for b in range(seq_count):
        for at, (source, target) in enumerate(((k_ref, ko_ref), (v_ref, vo_ref))):
            copy = pltpu.make_async_copy(source.at[b], target.at[b], bulk_sems.at[at, b])
            copy.start()
            bulk.append(copy)
    mixed_copy = pltpu.make_async_copy(mixed_in, mixed_ref, mixed_sem)
    mixed_copy.start()
    for copy in scalars:
        copy.wait()
    placed = []
    for b in range(seq_count):
        limit = prior_s[b] + accepted_s[b] - offset
        start = pl.multiple_of(jnp.clip(limit, 0, length - window) // PROPS * PROPS, PROPS)
        select = start + iota((window, PROPS), 0) - limit == iota((window, PROPS), 1)
        select = ones_where(select, bf16)
        slot = start + iota((window, width), 0) - limit
        inside = (slot >= 0) & (slot < PROPS)
        for at, (source, fresh, target) in enumerate(
            ((k_ref, newk_ref, ko_ref), (v_ref, newv_ref, vo_ref))
        ):
            rows = matmul(select, fresh[b * PROPS : (b + 1) * PROPS])
            old = source[b, pl.ds(start, window), :].astype(f32)
            windows[at, b] = jnp.where(inside, rows, old).astype(bf16)
            placed.append(
                pltpu.make_async_copy(
                    windows.at[at, b],
                    target.at[b, pl.ds(start, window), :],
                    window_sems.at[at, b],
                )
            )
    for first, second in zip(bulk, placed):
        first.wait()
        second.start()
    mixed_copy.wait()
    for copy in placed:
        copy.wait()


def shards(
    n_kv,
    n_tp,
    tokens,
    norm_gain,
    w_query,
    w_key,
    w_value,
    w_gate,
    gate_bias,
    w_out,
    keys_cache,
    values_cache,
    cum_gates,
    prior_len,
    accepted,
    parents,
):
    row_count, depth = tokens.shape
    seq_count, length, width = keys_cache.shape
    heads = width // HEAD
    per = next(p for p in range(1, 5) if seq_count % p == 0 and seq_count // p <= n_kv)
    n_chunks = seq_count // per
    rc = per * PROPS
    cq = n_chunks // 4
    n_groups = n_kv // 4
    cpt = n_chunks // n_tp
    columns = w_out.shape[1]
    vmem = pl.BlockSpec(memory_space=pltpu.VMEM)
    hbm = pl.BlockSpec(memory_space=pltpu.HBM)
    dma = pltpu.SemaphoreType.DMA

    inputs = (
        tokens.reshape(n_chunks, rc, depth),
        norm_gain.reshape(1, depth),
        w_query,
        w_key,
        w_value,
        w_gate.T if depth % LANES == 0 else w_gate,
        gate_bias.reshape(1, -1),
        w_out,
        parents.T,
    )
    mixed, new_keys, new_values = pl.pallas_call(
        functools.partial(step_kernel, n_kv, n_tp, heads, per),
        out_shape=(
            jax.ShapeDtypeStruct((cpt * rc, columns), bf16),
            jax.ShapeDtypeStruct((n_chunks, rc, width), bf16),
            jax.ShapeDtypeStruct((n_chunks, rc, width), bf16),
        ),
        in_specs=[hbm] * 14,
        out_specs=[vmem] * 3,
        scratch_shapes=[pltpu.VMEM(value.shape, value.dtype) for value in inputs]
        + [pltpu.SMEM((seq_count,), i32)] * 2
        + [
            pltpu.VMEM((seq_count, length, width), bf16),
            pltpu.VMEM((seq_count, length, width), bf16),
            pltpu.VMEM((seq_count, heads, length), f32),
            pltpu.VMEM((3, n_chunks, rc, width), bf16),
            pltpu.VMEM((n_chunks, 8, LANES), f32),
            pltpu.VMEM((3, 3, cq, rc, width), bf16),
            pltpu.VMEM((3, cq, 8, LANES), f32),
            pltpu.VMEM((3, cq, rc, width), bf16),
            pltpu.VMEM((cq, 8, LANES), f32),
            pltpu.VMEM((3, n_groups - 1, cq, rc, width), bf16),
            pltpu.VMEM((n_groups - 1, cq, 8, LANES), f32),
            pltpu.VMEM((3, n_chunks, rc, width), bf16),
            pltpu.VMEM((n_chunks, 8, LANES), f32),
            pltpu.VMEM((n_tp, width, columns), bf16),
            pltpu.VMEM((n_kv, rc, width), bf16),
            pltpu.VMEM((n_kv, 8, LANES), f32),
            pltpu.VMEM((n_kv - 1, rc, width), bf16),
            pltpu.VMEM((n_kv - 1, 8, LANES), f32),
            pltpu.VMEM((rc, width), bf16),
            pltpu.VMEM((cpt, n_tp, rc, width), bf16),
            dma((len(inputs) + 2,)),
            dma((3, n_chunks)),
            dma((12 * cq,)),
            dma((12 * cq,)),
            dma((4 * (n_groups - 1) * cq,)),
            dma((4 * (n_groups - 1) * cq,)),
            dma((12 * cq,)),
            dma((12 * cq,)),
            dma((n_tp - 1,)),
            dma((n_tp - 1,)),
            dma((n_kv - 1,)),
            dma((n_kv - 1,)),
            dma((n_kv - 1,)),
            dma((n_kv - 1,)),
            dma((n_kv,)),
            dma((cpt * n_tp,)),
        ],
        compiler_params=pltpu.CompilerParams(
            collective_id=0, has_side_effects=True, vmem_limit_bytes=28 * 1024 * 1024
        ),
        name="step",
    )(
        *(
            pltpu.with_memory_space_constraint(value, pltpu.HBM)
            for value in (
                prior_len,
                accepted,
                *inputs,
                keys_cache,
                values_cache,
                cum_gates,
            )
        ),
    )

    return pl.pallas_call(
        write_kernel,
        out_shape=(
            jax.ShapeDtypeStruct((cpt * rc, columns), bf16),
            jax.ShapeDtypeStruct(keys_cache.shape, bf16),
            jax.ShapeDtypeStruct(values_cache.shape, bf16),
        ),
        in_specs=[hbm] * 2 + [vmem] * 5,
        out_specs=[hbm, hbm, hbm],
        scratch_shapes=[
            pltpu.SMEM((seq_count,), i32),
            pltpu.SMEM((seq_count,), i32),
            pltpu.VMEM((2, seq_count, 2 * PROPS, width), bf16),
            dma((2,)),
            dma((2, seq_count)),
            dma((2, seq_count)),
            dma(()),
        ],
        compiler_params=pltpu.CompilerParams(vmem_limit_bytes=8 * 1024 * 1024),
        name="write",
    )(
        pltpu.with_memory_space_constraint(prior_len, pltpu.HBM),
        pltpu.with_memory_space_constraint(accepted, pltpu.HBM),
        new_keys.reshape(row_count, width),
        new_values.reshape(row_count, width),
        mixed,
        keys_cache,
        values_cache,
    )


def solution(mesh):
    placed = (
        P(None, "kv"),
        P("kv"),
        P("kv", "tp"),
        P("kv", "tp"),
        P("kv", "tp"),
        P(),
        P(),
        P("tp", "kv"),
        P(None, "kv", "tp"),
        P(None, "kv", "tp"),
        P(None, "tp", "kv"),
        P(),
        P(),
        P(),
    )
    return jax.shard_map(
        functools.partial(shards, mesh.shape["kv"], mesh.shape["tp"]),
        mesh=mesh,
        in_specs=placed,
        out_specs=(P("tp", "kv"), P(None, "kv", "tp"), P(None, "kv", "tp")),
        check_vma=False,
    )
```

```python
import functools

import jax
import jax.numpy as jnp
from jax import lax
from jax.experimental import pallas as pl
from jax.experimental.pallas import tpu as pltpu
from jax.sharding import PartitionSpec as P

HEAD = 64
PROPS = 16
LANES = 128
SQUARE_ROW = 7
SUM_ROW = 4
masked_score = -1e30
norm_eps = 1e-06
MESH = pl.DeviceIdType.MESH
f32, bf16, i32 = jnp.float32, jnp.bfloat16, jnp.int32


def iota(shape, axis):
    return lax.broadcasted_iota(i32, shape, axis)


def ones_where(mask, dtype=f32):
    return jnp.where(mask, 1.0, 0.0).astype(dtype)


def split2(x):
    hi = x.astype(bf16)
    return hi, (x - hi.astype(f32)).astype(bf16)


def split3(x):
    hi = x.astype(bf16).astype(f32)
    mid = (x - hi).astype(bf16).astype(f32)
    return hi, mid, x - hi - mid


def contract_last(a, b):
    return lax.dot_general(a, b, (((1,), (1,)), ((), ())), preferred_element_type=f32)


def matmul(a, b):
    return jnp.dot(a, b, preferred_element_type=f32)


def step_kernel(
    n_kv,
    n_tp,
    heads,
    per,
    prior_hbm,
    accepted_hbm,
    tokens_hbm,
    gain_hbm,
    wq_hbm,
    wk_hbm,
    wv_hbm,
    wg_hbm,
    bias_hbm,
    wout_hbm,
    parents_hbm,
    k_hbm,
    v_hbm,
    cum_hbm,
    mixed_ref,
    newk_ref,
    newv_ref,
    tokens_ref,
    gain_ref,
    wq_ref,
    wk_ref,
    wv_ref,
    wg_ref,
    bias_ref,
    wout_ref,
    parents_ref,
    prior_s,
    accepted_s,
    kbuf,
    vbuf,
    cumbuf,
    part,
    gpart,
    arr1,
    garr1,
    half,
    ghalf,
    arr2,
    garr2,
    full,
    gfull,
    wall,
    parts_v,
    parts_s,
    got_v,
    got_s,
    mine,
    att,
    input_sems,
    load_sems,
    s1_send,
    s1_recv,
    s2_send,
    s2_recv,
    s3_send,
    s3_recv,
    w_send,
    w_recv,
    cv_send,
    cv_recv,
    cs_send,
    cs_recv,
    ag_send,
    ag_recv,
):
    me = lax.axis_index("kv")
    tp = lax.axis_index("tp")
    n_chunks, rc, depth = tokens_ref.shape
    length = kbuf.shape[1]
    width = heads * HEAD
    lines = heads * PROPS
    cq = n_chunks // 4
    n_groups = n_kv // 4
    cpt = n_chunks // n_tp
    corner, group = lax.rem(me, 4), me // 4
    quarter = pl.ds(corner * cq, cq)
    order = [lax.rem(group + 1 + i, cq) for i in range(cq)]

    aligned = n_tp == 4 and cpt == cq and n_kv == n_chunks
    inputs = []
    for at, (source, target) in enumerate(
        (
            (tokens_hbm, tokens_ref),
            (wq_hbm, wq_ref),
            (gain_hbm, gain_ref),
            (wg_hbm, wg_ref),
            (wk_hbm, wk_ref),
            (wv_hbm, wv_ref),
            (parents_hbm, parents_ref),
            (bias_hbm, bias_ref),
            (wout_hbm, wout_ref),
            (prior_hbm, prior_s),
            (accepted_hbm, accepted_s),
        )
    ):
        copy = pltpu.make_async_copy(source, target, input_sems.at[at])
        copy.start()
        inputs.append(copy)
    barrier = pltpu.get_barrier_semaphore()
    for d in range(1, n_kv * n_tp):
        other = lax.rem(me * n_tp + tp + d, n_kv * n_tp)
        pl.semaphore_signal(
            barrier,
            inc=1,
            device_id={"kv": other // n_tp, "tp": lax.rem(other, n_tp)},
            device_id_type=MESH,
        )

    def send(source, target, sems, at, kv=None, to_tp=None):
        where = {}
        if kv is not None:
            where["kv"] = kv
        if to_tp is not None:
            where["tp"] = to_tp
        copy = pltpu.make_async_remote_copy(
            src_ref=source,
            dst_ref=target,
            send_sem=sems[0].at[at],
            recv_sem=sems[1].at[at],
            device_id=where,
            device_id_type=MESH,
        )
        copy.start()
        return copy

    for copy in inputs[:3]:
        copy.wait()
    floats = tokens_ref[...].reshape(n_chunks * rc, depth).astype(f32)
    scaled = (floats * gain_ref[...]).astype(bf16)

    def product(piece, w_ref):
        value = matmul(scaled, w_ref[...]).astype(bf16)
        part[piece] = value.reshape(n_chunks, rc, width)

    product(0, wq_ref)
    pl.semaphore_wait(barrier, n_kv * n_tp - 1)
    started = []

    def flip(bits):
        low = lax.rem(corner + bits % 2, 2)
        return lax.rem(corner // 2 + bits // 2, 2) * 2 + low

    def corner_sends(sources, targets, sems, piece, j=0):
        out = [None] * 3
        for d in (3, 2, 1):
            there = flip(d)
            at = (piece * 3 + d - 1) * cq + j
            out[d - 1] = send(sources(there), targets(d), sems, at, kv=group * 4 + there)
        started.extend(out)
        return out

    def first_stage(piece, j, count):
        return corner_sends(
            lambda there: part.at[piece, pl.ds(there * cq + j, count)],
            lambda d: arr1.at[piece, d - 1, pl.ds(j, count)],
            (s1_send, s1_recv),
            piece,
            j,
        )

    def group_sends(source, target, piece, j=0):
        out = []
        for d in range(1, n_groups):
            there = lax.rem(group + d, n_groups) * 4 + corner
            at = (piece * (n_groups - 1) + d - 1) * cq + j
            out.append(send(source, target(d), (s2_send, s2_recv), at, kv=there))
        started.extend(out)
        return out

    def second_stage(piece, stage, j, count):
        for copy in stage:
            copy.wait_recv()
        span = pl.ds(j, count)
        total = part[piece, pl.ds(corner * cq + j, count)].astype(f32)
        for d in range(3):
            total = total + arr1[piece, d, span].astype(f32)
        half[piece, span] = total.astype(bf16)
        return group_sends(
            half.at[piece, span], lambda d: arr2.at[piece, d - 1, span], piece, j
        )

    def finish(piece, stage, columns, spots):
        for copy in stage:
            copy.wait_recv()
        for j, scale in zip(spots, columns):
            total = half[piece, j].astype(f32)
            for d in range(n_groups - 1):
                total = total + arr2[piece, d, j].astype(f32)
            full[piece, corner * cq + j] = (total * scale).astype(bf16)

    def third_stage(piece, j, count):
        span = pl.ds(corner * cq + j, count)
        return corner_sends(
            lambda there: full.at[piece, span],
            lambda d: full.at[piece, span],
            (s3_send, s3_recv),
            piece,
            j,
        )

    q1 = [first_stage(0, order[0], 1)]
    inputs[3].wait()
    total_heads = bias_hbm.shape[1]
    pick = (iota((8, total_heads), 1) == tp * heads + iota((8, total_heads), 0)) & (
        iota((8, total_heads), 0) < heads
    )
    if depth % LANES == 0:
        gate_w = wg_ref[:, pl.ds(pl.multiple_of(me * depth, depth), depth)]
        gate_w = matmul(ones_where(pick, bf16), gate_w).astype(bf16)
    else:
        gate_w = wg_ref[pl.ds(pl.multiple_of(me * depth, depth), depth), :]
        gate_w = contract_last(ones_where(pick, bf16), gate_w).astype(bf16)
    square_w = ones_where(iota((8, depth), 0) == SQUARE_ROW, bf16)
    sq_hi, sq_lo = split2(floats * floats)
    gpart[...] = jnp.zeros_like(gpart)
    for c in range(n_chunks):
        rows = slice(c * rc, (c + 1) * rc)
        gpart[c, :, :rc] = (
            contract_last(gate_w, scaled[rows])
            + contract_last(square_w, sq_hi[rows])
            + contract_last(square_w, sq_lo[rows])
        )
    g1 = corner_sends(
        lambda there: gpart.at[pl.ds(there * cq, cq)],
        lambda d: garr1.at[d - 1],
        (s1_send, s1_recv),
        3,
    )
    q1 = q1 + [first_stage(0, j, 1) for j in order[1:]]
    loads = []
    for c in range(n_chunks):
        span = pl.ds(c * per, per)
        for at, (source, target) in enumerate(((k_hbm, kbuf), (v_hbm, vbuf), (cum_hbm, cumbuf))):
            copy = pltpu.make_async_copy(source.at[span], target.at[span], load_sems.at[at, c])
            copy.start()
            loads.append(copy)
    for copy in inputs[4:]:
        copy.wait()
    product(1, wk_ref)
    k1 = first_stage(1, 0, cq)
    product(2, wv_ref)

    slot = lax.rem(me, n_tp) * cpt + me // n_tp
    own = jnp.minimum(slot, n_chunks - 1)
    every = parents_ref[...]
    parent = jnp.concatenate(
        [
            jnp.sum(
                jnp.where(iota(every.shape, 1) == own * per + k, every, 0).astype(f32),
                axis=1,
                keepdims=True,
            ).astype(i32)
            for k in range(per)
        ],
        axis=0,
    )
    row, column = iota((rc, rc), 0), iota((rc, rc), 1)
    link = (parent + (row // PROPS) * PROPS == column) & (parent >= 0)
    reached = ones_where(link | (row == column))
    for squaring in range((PROPS - 1).bit_length()):
        reached = jnp.minimum(matmul(reached.astype(bf16), reached.astype(bf16)), 1.0)

    q2 = [second_stage(0, q1[0], order[0], 1)]
    for copy in g1:
        copy.wait_recv()
    ghalf[...] = gpart[quarter] + garr1[0] + garr1[1] + garr1[2]
    g2 = group_sends(ghalf, lambda d: garr2.at[d - 1], 3)
    for i in range(1, cq):
        q2.append(second_stage(0, q1[i], order[i], 1))
    v1 = first_stage(2, 0, cq)
    w_copies = []
    for d in range(1, n_tp):
        w_copies.append(
            send(
                wout_ref, wall.at[tp], (w_send, w_recv), d - 1, to_tp=lax.rem(tp + d, n_tp)
            )
        )
    started.extend(w_copies)
    wall[tp] = wout_ref[...]

    for copy in g2:
        copy.wait_recv()
    bias = jnp.sum(
        jnp.where(pick, jnp.broadcast_to(bias_ref[...], (8, total_heads)), 0.0),
        axis=1,
        keepdims=True,
    )
    inv_columns = []
    eye = iota((rc, LANES), 0) == iota((rc, LANES), 1)
    for j in order:
        gates = ghalf[j]
        for d in range(n_groups - 1):
            gates = gates + garr2[d, j]
        inv_row = lax.rsqrt(gates[SQUARE_ROW : SQUARE_ROW + 1, :] / (n_kv * depth) + norm_eps)
        pre = inv_row * gates + bias
        gfull[corner * cq + j] = jnp.minimum(pre, 0.0) - jnp.log1p(jnp.exp(-jnp.abs(pre)))
        inv_columns.append(
            jnp.sum(
                jnp.where(eye, jnp.broadcast_to(inv_row, (rc, LANES)), 0.0),
                axis=1,
                keepdims=True,
            )
        )
    scaled_columns = [c * HEAD ** (-0.5) for c in inv_columns]
    q3 = []
    for i in range(cq):
        finish(0, q2[i], scaled_columns[i : i + 1], order[i : i + 1])
        q3.append(third_stage(0, order[i], 1))
    g3 = []
    if not aligned:
        g3 = corner_sends(
            lambda there: gfull.at[quarter],
            lambda d: gfull.at[quarter],
            (s3_send, s3_recv),
            3,
        )
    k2 = second_stage(1, k1, 0, cq)
    lane_head = iota((PROPS, width), 1) // HEAD
    head_rows = [ones_where(lane_head == h) for h in range(heads)]
    head_mask = jnp.concatenate(head_rows, axis=0).astype(bf16)
    position = iota((lines, length), 1)
    short_position = iota((heads, length), 1)
    line_eye = iota((lines, LANES), 0) == iota((lines, LANES), 1)
    last_lane = iota((heads, LANES), 1) - LANES // 2
    last_mask = (last_lane >= 0) & (last_lane // PROPS == iota((heads, LANES), 0))
    tile_row = iota((8, LANES), 0)
    offset = me * length

    def as_row(value):
        return jnp.sum(jnp.where(line_eye, value, 0.0), axis=0, keepdims=True)

    def attend(owner):
        chunk = jnp.minimum(lax.rem(owner, n_tp) * cpt + owner // n_tp, n_chunks - 1)
        limits, scores = [], []
        for k in range(per):
            seq = chunk * per + k
            limits.append(prior_s[seq] + accepted_s[seq] - offset)
            query = full[0, chunk, k * PROPS : (k + 1) * PROPS, :]
            query = jnp.concatenate([query] * heads, axis=0) * head_mask
            scores.append(contract_last(query, kbuf[seq]))
        tile = jnp.zeros((8, LANES), f32)
        weights = []
        for k in range(per):
            seq = chunk * per + k
            cum = jnp.concatenate(
                [
                    jnp.broadcast_to(cumbuf[seq, h : h + 1, :], (PROPS, length))
                    for h in range(heads)
                ],
                axis=0,
            )
            value = jnp.where(position < limits[k], scores[k] - cum, masked_score)
            top = jnp.max(value, axis=1, keepdims=True)
            weight = jnp.exp(value - top)
            total = jnp.sum(weight, axis=1, keepdims=True)
            weights.append(weight.astype(bf16))
            last = jnp.sum(
                jnp.where(short_position == limits[k] - 1, cumbuf[seq], 0.0),
                axis=1,
                keepdims=True,
            )
            last_row = jnp.sum(jnp.where(last_mask, last, 0.0), axis=0, keepdims=True)
            tile = jnp.where(tile_row == k, as_row(top) + last_row, tile)
            tile = jnp.where(tile_row == SUM_ROW + k, as_row(total), tile)
        for k in range(per):
            values = matmul(weights[k], vbuf[chunk * per + k])
            picked = values[:PROPS] * head_rows[0]
            for h in range(1, heads):
                picked = picked + values[h * PROPS : (h + 1) * PROPS] * head_rows[h]
            parts_v[owner, k * PROPS : (k + 1) * PROPS, :] = picked.astype(bf16)
        parts_s[owner] = tile

    def peer(at):
        near = at >= n_kv - 4
        if isinstance(at, int):
            bits = 3 - at % 4 if near else at % 4
        else:
            bits = jnp.where(near, 3 - at % 4, at % 4)
        return lax.rem(group + at // 4 + 1, n_groups) * 4 + flip(bits)

    def part_copies(at):
        owner = peer(at)
        return [
            pltpu.make_async_remote_copy(
                src_ref=source.at[owner],
                dst_ref=target.at[at],
                send_sem=send_sem.at[at],
                recv_sem=recv_sem.at[at],
                device_id={"kv": owner},
                device_id_type=MESH,
            )
            for source, target, send_sem, recv_sem in (
                (parts_v, got_v, cv_send, cv_recv),
                (parts_s, got_s, cs_send, cs_recv),
            )
        ]

    def attend_and_send(at):
        attend(peer(at))
        for copy in part_copies(at):
            copy.start()

    for copy in loads:
        copy.wait()
    if aligned:
        attend_and_send(0)
        attend(me)
        v2 = second_stage(2, v1, 0, cq)
        for at in range(1, n_kv - 1):
            if at < 4:
                q3[0][at - 1].wait_recv()
            else:
                q3[1][2 - at % 4].wait_recv()
            attend_and_send(at)
    else:
        v2 = second_stage(2, v1, 0, cq)
        for stage in q3:
            for copy in stage:
                copy.wait_recv()

        def one(at, carry):
            attend_and_send(at)
            return carry

        lax.fori_loop(0, n_kv - 1, one, 0)
        attend(me)
    finish(1, k2, inv_columns, order)
    finish(2, v2, inv_columns, order)
    upper = me >= n_kv // 2
    k3 = v3 = []
    if aligned:
        late = []
        for piece in (1, 2):
            for d in (3, 2, 1):
                there = flip(d)
                at = (piece * 3 + d - 1) * cq
                late.append(
                    pltpu.make_async_remote_copy(
                        src_ref=full.at[piece, quarter],
                        dst_ref=full.at[piece, quarter],
                        send_sem=s3_send.at[at],
                        recv_sem=s3_recv.at[at],
                        device_id={"kv": group * 4 + there},
                        device_id_type=MESH,
                    )
                )

        @pl.when(upper)
        def _():
            for copy in late:
                copy.start()

    else:
        k3 = third_stage(1, 0, cq)
        v3 = third_stage(2, 0, cq)
        for copy in g3 + k3 + v3:
            copy.wait_recv()
    gate_parts = jnp.concatenate(split3(gfull[own]), axis=0)[:, :rc].astype(bf16)
    tree_gates = contract_last(gate_parts, reached.astype(bf16))
    tree_gates = tree_gates[0:8] + tree_gates[8:16] + tree_gates[16:24]
    wide_rows = [ones_where(iota((rc, width), 1) // HEAD == h) for h in range(heads)]
    wide_mask = jnp.concatenate(wide_rows, axis=0).astype(bf16)
    tree_query = jnp.concatenate([full[0, own]] * heads, axis=0) * wide_mask
    tree = contract_last(tree_query, full[1, own])
    tree = tree - jnp.concatenate(
        [jnp.broadcast_to(tree_gates[h : h + 1, :], (rc, rc)) for h in range(heads)], axis=0
    )
    live = jnp.concatenate([reached] * heads, axis=0) > 0.5
    tree = jnp.where(live, tree, masked_score)
    tree_top = jnp.max(tree, axis=1, keepdims=True)
    tree_weights = jnp.where(live, jnp.exp(tree - tree_top), 0.0)
    tree_sum = jnp.sum(tree_weights, axis=1, keepdims=True)
    tree_values = matmul(tree_weights.astype(bf16), full[2, own])
    tree_picked = tree_values[:rc] * wide_rows[0]
    for h in range(1, heads):
        tree_picked = tree_picked + tree_values[h * rc : (h + 1) * rc] * wide_rows[h]
    def tile_of(value):
        rows = [
            as_row(
                jnp.concatenate(
                    [
                        value[h * rc + k * PROPS : h * rc + (k + 1) * PROPS]
                        for h in range(heads)
                    ],
                    axis=0,
                )
            )
            for k in range(per)
        ]
        rows = rows + [jnp.zeros((1, LANES), f32)] * (4 - per)
        return jnp.concatenate(rows, axis=0)

    tree_top_tile, tree_sum_tile = tile_of(tree_top), tile_of(tree_sum)

    landing = [part_copies(at) for at in range(n_kv - 1)]
    for pair in landing:
        pair[1].wait_recv()
    tiles = [parts_s[me]] + [got_s[d] for d in range(n_kv - 1)]
    last = tiles[0][:4]
    for tile in tiles[1:]:
        last = last + tile[:4]
    last = pltpu.roll(last, LANES // 2, axis=1)
    lane_ok = iota((4, LANES), 1) < lines
    tops = [jnp.where(lane_ok, tile[:4], 0.0) for tile in tiles]
    tops.append(jnp.where(lane_ok, tree_top_tile - last, 0.0))
    sums = [jnp.where(lane_ok, tile[4:], 1.0) for tile in tiles] + [
        jnp.where(lane_ok, tree_sum_tile, 1.0)
    ]
    top = functools.reduce(jnp.maximum, tops)
    scales = [jnp.exp(t - top) for t in tops]
    total = functools.reduce(lambda a, b: a + b, [a * b for a, b in zip(scales, sums)])
    half_lane = iota((LANES, width), 0) % (LANES // 2)
    spread = ones_where(
        (half_lane // PROPS == iota((LANES, width), 1) // HEAD) & (half_lane < lines), bf16
    )
    fits = (iota((PROPS, LANES), 1) % PROPS == iota((PROPS, LANES), 0)) & (
        iota((PROPS, LANES), 1) % (LANES // 2) < lines
    )
    inverse = 1.0 / total
    low_half = iota((4, LANES), 1) < LANES // 2

    def expand(scale):
        hi, lo = split2(jnp.where(low_half, scale * inverse, 0.0))
        both = jnp.where(low_half, hi.astype(f32), pltpu.roll(lo.astype(f32), LANES // 2, axis=1))
        rows = jnp.concatenate(
            [
                jnp.where(fits, jnp.broadcast_to(both[k : k + 1], (PROPS, LANES)), 0.0)
                for k in range(per)
            ],
            axis=0,
        )
        return matmul(rows.astype(bf16), spread)

    expanded = [expand(scale) for scale in scales]
    result = expanded[-1] * tree_picked + expanded[0] * parts_v[me].astype(f32)
    for d in range(n_kv - 1):
        landing[d][0].wait_recv()
        result = result + expanded[d + 1] * got_v[d].astype(f32)
    mine[...] = result.astype(bf16)

    target, early = lax.rem(me, n_tp), me // n_tp
    spreads = [
        pltpu.make_async_remote_copy(
            src_ref=mine,
            dst_ref=att.at[jnp.minimum(early, cpt - 1), tp],
            send_sem=ag_send.at[d],
            recv_sem=ag_recv.at[jnp.minimum(early, cpt - 1) * n_tp + tp],
            device_id={"kv": peer(d - 1) if d > 0 else me, "tp": target},
            device_id_type=MESH,
        )
        for d in range(n_kv)
    ]
    sends = early < cpt
    for d in range(1, n_kv):

        @pl.when(sends)
        def _(d=d):
            spreads[d].start()

    @pl.when(sends & (target != tp))
    def _():
        spreads[0].start()

    @pl.when(sends & (target == tp))
    def _():
        att[jnp.minimum(early, cpt - 1), tp] = mine[...]

    for copy in w_copies:
        copy.wait_recv()
    for at in range(cpt * n_tp):
        e, t = at // n_tp, at % n_tp

        @pl.when((me != e * n_tp + tp) | (tp != t))
        def _(at=at, e=e, t=t):
            pltpu.make_async_remote_copy(
                src_ref=mine,
                dst_ref=att.at[e, t],
                send_sem=ag_send.at[0],
                recv_sem=ag_recv.at[at],
                device_id={"kv": me, "tp": lax.rem(tp + 1, n_tp)},
                device_id_type=MESH,
            ).wait_recv()

    mixed = None
    for t in range(n_tp):
        rows = jnp.concatenate([att[e, t] for e in range(cpt)], axis=0)
        piece = matmul(rows, wall[t]).astype(bf16).astype(f32)
        mixed = piece if mixed is None else mixed + piece
    mixed_ref[...] = mixed.astype(bf16)
    if aligned:

        @pl.when(upper)
        def _():
            for copy in late:
                copy.wait_recv()
            for copy in late:
                copy.wait_send()

    newk_ref[...] = full[1]
    newv_ref[...] = full[2]
    for d in range(1, n_kv):

        @pl.when(sends)
        def _(d=d):
            spreads[d].wait_send()

    @pl.when(sends & (target != tp))
    def _():
        spreads[0].wait_send()

    for copy in started:
        copy.wait_send()
    for pair in landing:
        for copy in pair:
            copy.wait_send()


def write_kernel(
    prior_hbm,
    accepted_hbm,
    newk_ref,
    newv_ref,
    mixed_in,
    k_ref,
    v_ref,
    mixed_ref,
    ko_ref,
    vo_ref,
    prior_s,
    accepted_s,
    windows,
    scalar_sems,
    bulk_sems,
    window_sems,
    mixed_sem,
):
    seq_count, length, width = k_ref.shape
    window = 2 * PROPS
    offset = lax.axis_index("kv") * length
    scalars = [
        pltpu.make_async_copy(prior_hbm, prior_s, scalar_sems.at[0]),
        pltpu.make_async_copy(accepted_hbm, accepted_s, scalar_sems.at[1]),
    ]
    for copy in scalars:
        copy.start()
    bulk = []
    for b in range(seq_count):
        for at, (source, target) in enumerate(((k_ref, ko_ref), (v_ref, vo_ref))):
            copy = pltpu.make_async_copy(source.at[b], target.at[b], bulk_sems.at[at, b])
            copy.start()
            bulk.append(copy)
    mixed_copy = pltpu.make_async_copy(mixed_in, mixed_ref, mixed_sem)
    mixed_copy.start()
    for copy in scalars:
        copy.wait()
    placed = []
    for b in range(seq_count):
        limit = prior_s[b] + accepted_s[b] - offset
        start = pl.multiple_of(jnp.clip(limit, 0, length - window) // PROPS * PROPS, PROPS)
        select = start + iota((window, PROPS), 0) - limit == iota((window, PROPS), 1)
        select = ones_where(select, bf16)
        slot = start + iota((window, width), 0) - limit
        inside = (slot >= 0) & (slot < PROPS)
        for at, (source, fresh, target) in enumerate(
            ((k_ref, newk_ref, ko_ref), (v_ref, newv_ref, vo_ref))
        ):
            rows = matmul(select, fresh[b * PROPS : (b + 1) * PROPS])
            old = source[b, pl.ds(start, window), :].astype(f32)
            windows[at, b] = jnp.where(inside, rows, old).astype(bf16)
            placed.append(
                pltpu.make_async_copy(
                    windows.at[at, b],
                    target.at[b, pl.ds(start, window), :],
                    window_sems.at[at, b],
                )
            )
    for first, second in zip(bulk, placed):
        first.wait()
        second.start()
    mixed_copy.wait()
    for copy in placed:
        copy.wait()


def shards(
    n_kv,
    n_tp,
    tokens,
    norm_gain,
    w_query,
    w_key,
    w_value,
    w_gate,
    gate_bias,
    w_out,
    keys_cache,
    values_cache,
    cum_gates,
    prior_len,
    accepted,
    parents,
):
    row_count, depth = tokens.shape
    seq_count, length, width = keys_cache.shape
    heads = width // HEAD
    per = next(p for p in range(1, 5) if seq_count % p == 0 and seq_count // p <= n_kv)
    n_chunks = seq_count // per
    rc = per * PROPS
    cq = n_chunks // 4
    n_groups = n_kv // 4
    cpt = n_chunks // n_tp
    columns = w_out.shape[1]
    vmem = pl.BlockSpec(memory_space=pltpu.VMEM)
    hbm = pl.BlockSpec(memory_space=pltpu.HBM)
    dma = pltpu.SemaphoreType.DMA

    inputs = (
        tokens.reshape(n_chunks, rc, depth),
        norm_gain.reshape(1, depth),
        w_query,
        w_key,
        w_value,
        w_gate.T if depth % LANES == 0 else w_gate,
        gate_bias.reshape(1, -1),
        w_out,
        parents.T,
    )
    mixed, new_keys, new_values = pl.pallas_call(
        functools.partial(step_kernel, n_kv, n_tp, heads, per),
        out_shape=(
            jax.ShapeDtypeStruct((cpt * rc, columns), bf16),
            jax.ShapeDtypeStruct((n_chunks, rc, width), bf16),
            jax.ShapeDtypeStruct((n_chunks, rc, width), bf16),
        ),
        in_specs=[hbm] * 14,
        out_specs=[vmem] * 3,
        scratch_shapes=[pltpu.VMEM(value.shape, value.dtype) for value in inputs]
        + [pltpu.SMEM((seq_count,), i32)] * 2
        + [
            pltpu.VMEM((seq_count, length, width), bf16),
            pltpu.VMEM((seq_count, length, width), bf16),
            pltpu.VMEM((seq_count, heads, length), f32),
            pltpu.VMEM((3, n_chunks, rc, width), bf16),
            pltpu.VMEM((n_chunks, 8, LANES), f32),
            pltpu.VMEM((3, 3, cq, rc, width), bf16),
            pltpu.VMEM((3, cq, 8, LANES), f32),
            pltpu.VMEM((3, cq, rc, width), bf16),
            pltpu.VMEM((cq, 8, LANES), f32),
            pltpu.VMEM((3, n_groups - 1, cq, rc, width), bf16),
            pltpu.VMEM((n_groups - 1, cq, 8, LANES), f32),
            pltpu.VMEM((3, n_chunks, rc, width), bf16),
            pltpu.VMEM((n_chunks, 8, LANES), f32),
            pltpu.VMEM((n_tp, width, columns), bf16),
            pltpu.VMEM((n_kv, rc, width), bf16),
            pltpu.VMEM((n_kv, 8, LANES), f32),
            pltpu.VMEM((n_kv - 1, rc, width), bf16),
            pltpu.VMEM((n_kv - 1, 8, LANES), f32),
            pltpu.VMEM((rc, width), bf16),
            pltpu.VMEM((cpt, n_tp, rc, width), bf16),
            dma((len(inputs) + 2,)),
            dma((3, n_chunks)),
            dma((12 * cq,)),
            dma((12 * cq,)),
            dma((4 * (n_groups - 1) * cq,)),
            dma((4 * (n_groups - 1) * cq,)),
            dma((12 * cq,)),
            dma((12 * cq,)),
            dma((n_tp - 1,)),
            dma((n_tp - 1,)),
            dma((n_kv - 1,)),
            dma((n_kv - 1,)),
            dma((n_kv - 1,)),
            dma((n_kv - 1,)),
            dma((n_kv,)),
            dma((cpt * n_tp,)),
        ],
        compiler_params=pltpu.CompilerParams(
            collective_id=0, has_side_effects=True, vmem_limit_bytes=28 * 1024 * 1024
        ),
        name="step",
    )(
        *(
            pltpu.with_memory_space_constraint(value, pltpu.HBM)
            for value in (
                prior_len,
                accepted,
                *inputs,
                keys_cache,
                values_cache,
                cum_gates,
            )
        ),
    )

    return pl.pallas_call(
        write_kernel,
        out_shape=(
            jax.ShapeDtypeStruct((cpt * rc, columns), bf16),
            jax.ShapeDtypeStruct(keys_cache.shape, bf16),
            jax.ShapeDtypeStruct(values_cache.shape, bf16),
        ),
        in_specs=[hbm] * 2 + [vmem] * 5,
        out_specs=[hbm, hbm, hbm],
        scratch_shapes=[
            pltpu.SMEM((seq_count,), i32),
            pltpu.SMEM((seq_count,), i32),
            pltpu.VMEM((2, seq_count, 2 * PROPS, width), bf16),
            dma((2,)),
            dma((2, seq_count)),
            dma((2, seq_count)),
            dma(()),
        ],
        compiler_params=pltpu.CompilerParams(vmem_limit_bytes=8 * 1024 * 1024),
        name="write",
    )(
        pltpu.with_memory_space_constraint(prior_len, pltpu.HBM),
        pltpu.with_memory_space_constraint(accepted, pltpu.HBM),
        new_keys.reshape(row_count, width),
        new_values.reshape(row_count, width),
        mixed,
        keys_cache,
        values_cache,
    )


def solution(mesh):
    placed = (
        P(None, "kv"),
        P("kv"),
        P("kv", "tp"),
        P("kv", "tp"),
        P("kv", "tp"),
        P(),
        P(),
        P("tp", "kv"),
        P(None, "kv", "tp"),
        P(None, "kv", "tp"),
        P(None, "tp", "kv"),
        P(),
        P(),
        P(),
    )
    return jax.shard_map(
        functools.partial(shards, mesh.shape["kv"], mesh.shape["tp"]),
        mesh=mesh,
        in_specs=placed,
        out_specs=(P("tp", "kv"), P(None, "kv", "tp"), P(None, "kv", "tp")),
        check_vma=False,
    )
```

```python
import functools

import jax
import jax.numpy as jnp
from jax import lax
from jax.experimental import pallas as pl
from jax.experimental.pallas import tpu as pltpu
from jax.sharding import PartitionSpec as P

HEAD = 64
PROPS = 16
LANES = 128
SQUARE_ROW = 7
SUM_ROW = 4
masked_score = -1e30
norm_eps = 1e-06
MESH = pl.DeviceIdType.MESH
f32, bf16, i32 = jnp.float32, jnp.bfloat16, jnp.int32


def iota(shape, axis):
    return lax.broadcasted_iota(i32, shape, axis)


def ones_where(mask, dtype=f32):
    return jnp.where(mask, 1.0, 0.0).astype(dtype)


def split2(x):
    hi = x.astype(bf16)
    return hi, (x - hi.astype(f32)).astype(bf16)


def split3(x):
    hi = x.astype(bf16).astype(f32)
    mid = (x - hi).astype(bf16).astype(f32)
    return hi, mid, x - hi - mid


def contract_last(a, b):
    return lax.dot_general(a, b, (((1,), (1,)), ((), ())), preferred_element_type=f32)


def matmul(a, b):
    return jnp.dot(a, b, preferred_element_type=f32)


def step_kernel(
    n_kv,
    n_tp,
    heads,
    per,
    prior_hbm,
    accepted_hbm,
    tokens_hbm,
    gain_hbm,
    wq_hbm,
    wk_hbm,
    wv_hbm,
    wg_hbm,
    bias_hbm,
    wout_hbm,
    parents_hbm,
    k_hbm,
    v_hbm,
    cum_hbm,
    mixed_ref,
    newk_ref,
    newv_ref,
    tokens_ref,
    gain_ref,
    wq_ref,
    wk_ref,
    wv_ref,
    wg_ref,
    bias_ref,
    wout_ref,
    parents_ref,
    prior_s,
    accepted_s,
    kbuf,
    vbuf,
    cumbuf,
    part,
    gpart,
    arr1,
    garr1,
    half,
    ghalf,
    arr2,
    garr2,
    full,
    gfull,
    wall,
    parts_v,
    parts_s,
    got_v,
    got_s,
    mine,
    att,
    input_sems,
    load_sems,
    s1_send,
    s1_recv,
    s2_send,
    s2_recv,
    s3_send,
    s3_recv,
    w_send,
    w_recv,
    cv_send,
    cv_recv,
    cs_send,
    cs_recv,
    ag_send,
    ag_recv,
):
    me = lax.axis_index("kv")
    tp = lax.axis_index("tp")
    n_chunks, rc, depth = tokens_ref.shape
    length = kbuf.shape[1]
    width = heads * HEAD
    lines = heads * PROPS
    cq = n_chunks // 4
    n_groups = n_kv // 4
    cpt = n_chunks // n_tp
    corner, group = lax.rem(me, 4), me // 4
    quarter = pl.ds(corner * cq, cq)
    order = [lax.rem(group + i, cq) for i in range(cq)]

    aligned = n_tp == 4 and cpt == cq and n_kv == n_chunks
    inputs = []
    for at, (source, target) in enumerate(
        (
            (tokens_hbm, tokens_ref),
            (wq_hbm, wq_ref),
            (gain_hbm, gain_ref),
            (wg_hbm, wg_ref),
            (wk_hbm, wk_ref),
            (wv_hbm, wv_ref),
            (parents_hbm, parents_ref),
            (bias_hbm, bias_ref),
            (wout_hbm, wout_ref),
            (prior_hbm, prior_s),
            (accepted_hbm, accepted_s),
        )
    ):
        copy = pltpu.make_async_copy(source, target, input_sems.at[at])
        copy.start()
        inputs.append(copy)
    barrier = pltpu.get_barrier_semaphore()
    for d in range(1, n_kv * n_tp):
        other = lax.rem(me * n_tp + tp + d, n_kv * n_tp)
        pl.semaphore_signal(
            barrier,
            inc=1,
            device_id={"kv": other // n_tp, "tp": lax.rem(other, n_tp)},
            device_id_type=MESH,
        )

    def send(source, target, sems, at, kv=None, to_tp=None):
        where = {}
        if kv is not None:
            where["kv"] = kv
        if to_tp is not None:
            where["tp"] = to_tp
        copy = pltpu.make_async_remote_copy(
            src_ref=source,
            dst_ref=target,
            send_sem=sems[0].at[at],
            recv_sem=sems[1].at[at],
            device_id=where,
            device_id_type=MESH,
        )
        copy.start()
        return copy

    for copy in inputs[:3]:
        copy.wait()
    floats = tokens_ref[...].reshape(n_chunks * rc, depth).astype(f32)
    scaled = (floats * gain_ref[...]).astype(bf16)

    def product(piece, w_ref):
        value = matmul(scaled, w_ref[...]).astype(bf16)
        part[piece] = value.reshape(n_chunks, rc, width)

    product(0, wq_ref)
    pl.semaphore_wait(barrier, n_kv * n_tp - 1)
    started = []

    def flip(bits):
        low = lax.rem(corner + bits % 2, 2)
        return lax.rem(corner // 2 + bits // 2, 2) * 2 + low

    def corner_sends(sources, targets, sems, piece, j=0):
        out = [None] * 3
        for d in (3, 2, 1):
            there = flip(d)
            at = (piece * 3 + d - 1) * cq + j
            out[d - 1] = send(sources(there), targets(d), sems, at, kv=group * 4 + there)
        started.extend(out)
        return out

    def first_stage(piece, j, count):
        return corner_sends(
            lambda there: part.at[piece, pl.ds(there * cq + j, count)],
            lambda d: arr1.at[piece, d - 1, pl.ds(j, count)],
            (s1_send, s1_recv),
            piece,
            j,
        )

    def group_sends(source, target, piece, j=0):
        out = []
        for d in range(1, n_groups):
            there = lax.rem(group + d, n_groups) * 4 + corner
            at = (piece * (n_groups - 1) + d - 1) * cq + j
            out.append(send(source, target(d), (s2_send, s2_recv), at, kv=there))
        started.extend(out)
        return out

    def second_stage(piece, stage, j, count, sent=None):
        for copy in stage:
            copy.wait_recv()
        span = pl.ds(j, count)
        total = part[piece, pl.ds(corner * cq + j, count)].astype(f32)
        for d in range(3):
            total = total + arr1[piece, d, span].astype(f32)
        half[piece, span] = total.astype(bf16)
        if sent is not None:
            j, span = sent, pl.ds(sent, 1)
        return group_sends(
            half.at[piece, span], lambda d: arr2.at[piece, d - 1, span], piece, j
        )

    def finish(piece, stage, columns, spots):
        for copy in stage:
            copy.wait_recv()
        for j, scale in zip(spots, columns):
            total = half[piece, j].astype(f32)
            for d in range(n_groups - 1):
                total = total + arr2[piece, d, j].astype(f32)
            full[piece, corner * cq + j] = (total * scale).astype(bf16)

    def third_stage(piece, j, count):
        span = pl.ds(corner * cq + j, count)
        return corner_sends(
            lambda there: full.at[piece, span],
            lambda d: full.at[piece, span],
            (s3_send, s3_recv),
            piece,
            j,
        )

    q1 = [first_stage(0, order[0], 1)]
    inputs[3].wait()
    total_heads = bias_hbm.shape[1]
    pick = (iota((8, total_heads), 1) == tp * heads + iota((8, total_heads), 0)) & (
        iota((8, total_heads), 0) < heads
    )
    if depth % LANES == 0:
        gate_w = wg_ref[:, pl.ds(pl.multiple_of(me * depth, depth), depth)]
        gate_w = matmul(ones_where(pick, bf16), gate_w).astype(bf16)
    else:
        gate_w = wg_ref[pl.ds(pl.multiple_of(me * depth, depth), depth), :]
        gate_w = contract_last(ones_where(pick, bf16), gate_w).astype(bf16)
    square_w = ones_where(iota((8, depth), 0) == SQUARE_ROW, bf16)
    sq_hi, sq_lo = split2(floats * floats)
    gpart[...] = jnp.zeros_like(gpart)
    for c in range(n_chunks):
        rows = slice(c * rc, (c + 1) * rc)
        gpart[c, :, :rc] = (
            contract_last(gate_w, scaled[rows])
            + contract_last(square_w, sq_hi[rows])
            + contract_last(square_w, sq_lo[rows])
        )
    g1 = corner_sends(
        lambda there: gpart.at[pl.ds(there * cq, cq)],
        lambda d: garr1.at[d - 1],
        (s1_send, s1_recv),
        3,
    )
    q1 = q1 + [first_stage(0, j, 1) for j in order[1:]]
    loads = []
    for c in range(n_chunks):
        span = pl.ds(c * per, per)
        for at, (source, target) in enumerate(((k_hbm, kbuf), (v_hbm, vbuf), (cum_hbm, cumbuf))):
            copy = pltpu.make_async_copy(source.at[span], target.at[span], load_sems.at[at, c])
            copy.start()
            loads.append(copy)
    for copy in inputs[4:]:
        copy.wait()
    product(1, wk_ref)
    k1 = first_stage(1, 0, cq)
    product(2, wv_ref)

    slot = lax.rem(me, n_tp) * cpt + me // n_tp
    own = jnp.minimum(slot, n_chunks - 1)
    every = parents_ref[...]
    parent = jnp.concatenate(
        [
            jnp.sum(
                jnp.where(iota(every.shape, 1) == own * per + k, every, 0).astype(f32),
                axis=1,
                keepdims=True,
            ).astype(i32)
            for k in range(per)
        ],
        axis=0,
    )
    row, column = iota((rc, rc), 0), iota((rc, rc), 1)
    link = (parent + (row // PROPS) * PROPS == column) & (parent >= 0)
    reached = ones_where(link | (row == column))
    for squaring in range((PROPS - 1).bit_length()):
        reached = jnp.minimum(matmul(reached.astype(bf16), reached.astype(bf16)), 1.0)

    q2 = [second_stage(0, q1[0], order[0], 1)]
    for copy in g1:
        copy.wait_recv()
    ghalf[...] = gpart[quarter] + garr1[0] + garr1[1] + garr1[2]
    g2 = group_sends(ghalf, lambda d: garr2.at[d - 1], 3)
    for i in range(1, cq):
        q2.append(second_stage(0, q1[i], order[i], 1))
    v1 = first_stage(2, 0, cq)
    w_copies = []
    for d in range(1, n_tp):
        w_copies.append(
            send(
                wout_ref, wall.at[tp], (w_send, w_recv), d - 1, to_tp=lax.rem(tp + d, n_tp)
            )
        )
    started.extend(w_copies)
    wall[tp] = wout_ref[...]

    for copy in g2:
        copy.wait_recv()
    bias = jnp.sum(
        jnp.where(pick, jnp.broadcast_to(bias_ref[...], (8, total_heads)), 0.0),
        axis=1,
        keepdims=True,
    )
    inv_columns = []
    eye = iota((rc, LANES), 0) == iota((rc, LANES), 1)
    for j in order:
        gates = ghalf[j]
        for d in range(n_groups - 1):
            gates = gates + garr2[d, j]
        inv_row = lax.rsqrt(gates[SQUARE_ROW : SQUARE_ROW + 1, :] / (n_kv * depth) + norm_eps)
        pre = inv_row * gates + bias
        gfull[corner * cq + j] = jnp.minimum(pre, 0.0) - jnp.log1p(jnp.exp(-jnp.abs(pre)))
        inv_columns.append(
            jnp.sum(
                jnp.where(eye, jnp.broadcast_to(inv_row, (rc, LANES)), 0.0),
                axis=1,
                keepdims=True,
            )
        )
    scaled_columns = [c * HEAD ** (-0.5) for c in inv_columns]
    q3 = []
    first_only = order[1] if aligned else None
    upper = me >= n_kv // 2
    rise = [
        pltpu.make_async_remote_copy(
            src_ref=half.at[piece, 0],
            dst_ref=arr2.at[piece, 0, 0],
            send_sem=s2_send.at[piece * cq],
            recv_sem=s2_recv.at[piece * cq],
            device_id={"kv": lax.rem(me + 4, n_kv)},
            device_id_type=MESH,
        )
        for piece in (1, 2)
    ]

    def send_up(copy):
        @pl.when(jnp.logical_not(upper))
        def _():
            copy.start()

    k2 = None
    for i in list(range(1, cq)) + [0]:
        finish(0, q2[i], scaled_columns[i : i + 1], order[i : i + 1])
        q3.append(third_stage(0, order[i], 1))
        if k2 is None:
            k2 = second_stage(1, k1, 0, cq, first_only)
            if aligned:
                send_up(rise[0])
    g3 = []
    if not aligned:
        g3 = corner_sends(
            lambda there: gfull.at[quarter],
            lambda d: gfull.at[quarter],
            (s3_send, s3_recv),
            3,
        )
    lane_head = iota((PROPS, width), 1) // HEAD
    head_rows = [ones_where(lane_head == h) for h in range(heads)]
    head_mask = jnp.concatenate(head_rows, axis=0).astype(bf16)
    position = iota((lines, length), 1)
    short_position = iota((heads, length), 1)
    line_eye = iota((lines, LANES), 0) == iota((lines, LANES), 1)
    last_lane = iota((heads, LANES), 1) - LANES // 2
    last_mask = (last_lane >= 0) & (last_lane // PROPS == iota((heads, LANES), 0))
    tile_row = iota((8, LANES), 0)
    offset = me * length

    def as_row(value):
        return jnp.sum(jnp.where(line_eye, value, 0.0), axis=0, keepdims=True)

    def attend(owner):
        chunk = jnp.minimum(lax.rem(owner, n_tp) * cpt + owner // n_tp, n_chunks - 1)
        limits, scores = [], []
        for k in range(per):
            seq = chunk * per + k
            limits.append(prior_s[seq] + accepted_s[seq] - offset)
            query = full[0, chunk, k * PROPS : (k + 1) * PROPS, :]
            query = jnp.concatenate([query] * heads, axis=0) * head_mask
            scores.append(contract_last(query, kbuf[seq]))
        tile = jnp.zeros((8, LANES), f32)
        weights = []
        for k in range(per):
            seq = chunk * per + k
            cum = jnp.concatenate(
                [
                    jnp.broadcast_to(cumbuf[seq, h : h + 1, :], (PROPS, length))
                    for h in range(heads)
                ],
                axis=0,
            )
            value = jnp.where(position < limits[k], scores[k] - cum, masked_score)
            top = jnp.max(value, axis=1, keepdims=True)
            weight = jnp.exp(value - top)
            total = jnp.sum(weight, axis=1, keepdims=True)
            weights.append(weight.astype(bf16))
            last = jnp.sum(
                jnp.where(short_position == limits[k] - 1, cumbuf[seq], 0.0),
                axis=1,
                keepdims=True,
            )
            last_row = jnp.sum(jnp.where(last_mask, last, 0.0), axis=0, keepdims=True)
            tile = jnp.where(tile_row == k, as_row(top) + last_row, tile)
            tile = jnp.where(tile_row == SUM_ROW + k, as_row(total), tile)
        for k in range(per):
            values = matmul(weights[k], vbuf[chunk * per + k])
            picked = values[:PROPS] * head_rows[0]
            for h in range(1, heads):
                picked = picked + values[h * PROPS : (h + 1) * PROPS] * head_rows[h]
            parts_v[owner, k * PROPS : (k + 1) * PROPS, :] = picked.astype(bf16)
        parts_s[owner] = tile

    def peer(at):
        near = at >= n_kv - 4
        if isinstance(at, int):
            bits = 3 - at % 4 if near else at % 4
        else:
            bits = jnp.where(near, 3 - at % 4, at % 4)
        return lax.rem(group + at // 4 + 1, n_groups) * 4 + flip(bits)

    def part_copies(at):
        owner = peer(at)
        return [
            pltpu.make_async_remote_copy(
                src_ref=source.at[owner],
                dst_ref=target.at[at],
                send_sem=send_sem.at[at],
                recv_sem=recv_sem.at[at],
                device_id={"kv": owner},
                device_id_type=MESH,
            )
            for source, target, send_sem, recv_sem in (
                (parts_v, got_v, cv_send, cv_recv),
                (parts_s, got_s, cs_send, cs_recv),
            )
        ]

    def attend_and_send(at):
        attend(peer(at))
        for copy in part_copies(at):
            copy.start()

    for copy in loads:
        copy.wait()
    if aligned:
        def met(piece):
            return pltpu.make_async_remote_copy(
                src_ref=half.at[piece, order[0]],
                dst_ref=arr2.at[piece, 0, order[0]],
                send_sem=s2_send.at[piece * cq + order[0]],
                recv_sem=s2_recv.at[piece * cq + order[0]],
                device_id={"kv": lax.rem(me + 4, n_kv)},
                device_id_type=MESH,
            )

        late = [
            [
                pltpu.make_async_remote_copy(
                    src_ref=full.at[piece, corner * cq + j],
                    dst_ref=full.at[piece, corner * cq + j],
                    send_sem=s3_send.at[(piece * 3 + d - 1) * cq + j],
                    recv_sem=s3_recv.at[(piece * 3 + d - 1) * cq + j],
                    device_id={"kv": group * 4 + flip(d)},
                    device_id_type=MESH,
                )
                for piece in (1, 2)
                for d in (3, 2, 1)
            ]
            for j in range(cq)
        ]

        def lift(piece):
            rise[piece - 1].wait_recv()
            total = half[piece, 0].astype(f32) + arr2[piece, 0, 0].astype(f32)
            full[piece, corner * cq] = (total * inv_columns[1]).astype(bf16)

        attend_and_send(0)
        attend(me)
        v2 = second_stage(2, v1, 0, cq, first_only)
        for at in range(1, n_kv - 1):
            if at < 4:
                q3[0][at - 1].wait_recv()
            else:
                q3[1][2 - at % 4].wait_recv()
            attend_and_send(at)
            if at == 3:
                send_up(rise[1])
                finish(1, [met(1)], inv_columns[:1], order[:1])

                @pl.when(upper)
                def _():
                    lift(1)
                    for copy in late[1][:3] + late[0][:3]:
                        copy.start()

    else:
        v2 = second_stage(2, v1, 0, cq)
        for stage in q3:
            for copy in stage:
                copy.wait_recv()

        def one(at, carry):
            attend_and_send(at)
            return carry

        lax.fori_loop(0, n_kv - 1, one, 0)
        attend(me)
    k3 = v3 = []
    if aligned:

        finish(2, [met(2)], inv_columns[:1], order[:1])

        @pl.when(upper)
        def _():
            for copy in late[1][3:]:
                copy.start()

    else:
        finish(1, k2, inv_columns, order)
        finish(2, v2, inv_columns, order)
        k3 = third_stage(1, 0, cq)
        v3 = third_stage(2, 0, cq)
        for copy in g3 + k3 + v3:
            copy.wait_recv()
    gate_parts = jnp.concatenate(split3(gfull[own]), axis=0)[:, :rc].astype(bf16)
    tree_gates = contract_last(gate_parts, reached.astype(bf16))
    tree_gates = tree_gates[0:8] + tree_gates[8:16] + tree_gates[16:24]
    wide_rows = [ones_where(iota((rc, width), 1) // HEAD == h) for h in range(heads)]
    wide_mask = jnp.concatenate(wide_rows, axis=0).astype(bf16)
    tree_query = jnp.concatenate([full[0, own]] * heads, axis=0) * wide_mask
    tree = contract_last(tree_query, full[1, own])
    tree = tree - jnp.concatenate(
        [jnp.broadcast_to(tree_gates[h : h + 1, :], (rc, rc)) for h in range(heads)], axis=0
    )
    live = jnp.concatenate([reached] * heads, axis=0) > 0.5
    tree = jnp.where(live, tree, masked_score)
    tree_top = jnp.max(tree, axis=1, keepdims=True)
    tree_weights = jnp.where(live, jnp.exp(tree - tree_top), 0.0)
    tree_sum = jnp.sum(tree_weights, axis=1, keepdims=True)
    tree_values = matmul(tree_weights.astype(bf16), full[2, own])
    tree_picked = tree_values[:rc] * wide_rows[0]
    for h in range(1, heads):
        tree_picked = tree_picked + tree_values[h * rc : (h + 1) * rc] * wide_rows[h]
    def tile_of(value):
        rows = [
            as_row(
                jnp.concatenate(
                    [
                        value[h * rc + k * PROPS : h * rc + (k + 1) * PROPS]
                        for h in range(heads)
                    ],
                    axis=0,
                )
            )
            for k in range(per)
        ]
        rows = rows + [jnp.zeros((1, LANES), f32)] * (4 - per)
        return jnp.concatenate(rows, axis=0)

    tree_top_tile, tree_sum_tile = tile_of(tree_top), tile_of(tree_sum)

    landing = [part_copies(at) for at in range(n_kv - 1)]
    for pair in landing:
        pair[1].wait_recv()
    tiles = [parts_s[me]] + [got_s[d] for d in range(n_kv - 1)]
    last = tiles[0][:4]
    for tile in tiles[1:]:
        last = last + tile[:4]
    last = pltpu.roll(last, LANES // 2, axis=1)
    lane_ok = iota((4, LANES), 1) < lines
    tops = [jnp.where(lane_ok, tile[:4], 0.0) for tile in tiles]
    tops.append(jnp.where(lane_ok, tree_top_tile - last, 0.0))
    sums = [jnp.where(lane_ok, tile[4:], 1.0) for tile in tiles] + [
        jnp.where(lane_ok, tree_sum_tile, 1.0)
    ]
    top = functools.reduce(jnp.maximum, tops)
    scales = [jnp.exp(t - top) for t in tops]
    total = functools.reduce(lambda a, b: a + b, [a * b for a, b in zip(scales, sums)])
    half_lane = iota((LANES, width), 0) % (LANES // 2)
    spread = ones_where(
        (half_lane // PROPS == iota((LANES, width), 1) // HEAD) & (half_lane < lines), bf16
    )
    fits = (iota((PROPS, LANES), 1) % PROPS == iota((PROPS, LANES), 0)) & (
        iota((PROPS, LANES), 1) % (LANES // 2) < lines
    )
    inverse = 1.0 / total
    low_half = iota((4, LANES), 1) < LANES // 2

    def expand(scale):
        hi, lo = split2(jnp.where(low_half, scale * inverse, 0.0))
        both = jnp.where(low_half, hi.astype(f32), pltpu.roll(lo.astype(f32), LANES // 2, axis=1))
        rows = jnp.concatenate(
            [
                jnp.where(fits, jnp.broadcast_to(both[k : k + 1], (PROPS, LANES)), 0.0)
                for k in range(per)
            ],
            axis=0,
        )
        return matmul(rows.astype(bf16), spread)

    expanded = [expand(scale) for scale in scales]
    result = expanded[-1] * tree_picked + expanded[0] * parts_v[me].astype(f32)
    for d in range(n_kv - 1):
        landing[d][0].wait_recv()
        result = result + expanded[d + 1] * got_v[d].astype(f32)
    mine[...] = result.astype(bf16)

    target, early = lax.rem(me, n_tp), me // n_tp
    spreads = [
        pltpu.make_async_remote_copy(
            src_ref=mine,
            dst_ref=att.at[jnp.minimum(early, cpt - 1), tp],
            send_sem=ag_send.at[d],
            recv_sem=ag_recv.at[jnp.minimum(early, cpt - 1) * n_tp + tp],
            device_id={"kv": peer(d - 1) if d > 0 else me, "tp": target},
            device_id_type=MESH,
        )
        for d in range(n_kv)
    ]
    sends = early < cpt
    for d in range(1, n_kv):

        @pl.when(sends)
        def _(d=d):
            spreads[d].start()

    @pl.when(sends & (target != tp))
    def _():
        spreads[0].start()

    @pl.when(sends & (target == tp))
    def _():
        att[jnp.minimum(early, cpt - 1), tp] = mine[...]

    if aligned:

        @pl.when(upper)
        def _():
            lift(2)
            for copy in late[0][3:]:
                copy.start()

        @pl.when(jnp.logical_not(upper))
        def _():
            for copy in rise:
                copy.wait_send()

    for copy in w_copies:
        copy.wait_recv()
    for at in range(cpt * n_tp):
        e, t = at // n_tp, at % n_tp

        @pl.when((me != e * n_tp + tp) | (tp != t))
        def _(at=at, e=e, t=t):
            pltpu.make_async_remote_copy(
                src_ref=mine,
                dst_ref=att.at[e, t],
                send_sem=ag_send.at[0],
                recv_sem=ag_recv.at[at],
                device_id={"kv": me, "tp": lax.rem(tp + 1, n_tp)},
                device_id_type=MESH,
            ).wait_recv()

    mixed = None
    for t in range(n_tp):
        rows = jnp.concatenate([att[e, t] for e in range(cpt)], axis=0)
        piece = matmul(rows, wall[t]).astype(bf16).astype(f32)
        mixed = piece if mixed is None else mixed + piece
    mixed_ref[...] = mixed.astype(bf16)
    if aligned:

        @pl.when(upper)
        def _():
            for copy in late[1] + late[0]:
                copy.wait_recv()
            for copy in late[1] + late[0]:
                copy.wait_send()

    newk_ref[...] = full[1]
    newv_ref[...] = full[2]
    for d in range(1, n_kv):

        @pl.when(sends)
        def _(d=d):
            spreads[d].wait_send()

    @pl.when(sends & (target != tp))
    def _():
        spreads[0].wait_send()

    for copy in started:
        copy.wait_send()
    for pair in landing:
        for copy in pair:
            copy.wait_send()


def write_kernel(
    prior_hbm,
    accepted_hbm,
    newk_ref,
    newv_ref,
    mixed_in,
    k_ref,
    v_ref,
    mixed_ref,
    ko_ref,
    vo_ref,
    prior_s,
    accepted_s,
    windows,
    scalar_sems,
    bulk_sems,
    window_sems,
    mixed_sem,
):
    seq_count, length, width = k_ref.shape
    window = 2 * PROPS
    offset = lax.axis_index("kv") * length
    scalars = [
        pltpu.make_async_copy(prior_hbm, prior_s, scalar_sems.at[0]),
        pltpu.make_async_copy(accepted_hbm, accepted_s, scalar_sems.at[1]),
    ]
    for copy in scalars:
        copy.start()
    bulk = []
    for b in range(seq_count):
        for at, (source, target) in enumerate(((k_ref, ko_ref), (v_ref, vo_ref))):
            copy = pltpu.make_async_copy(source.at[b], target.at[b], bulk_sems.at[at, b])
            copy.start()
            bulk.append(copy)
    mixed_copy = pltpu.make_async_copy(mixed_in, mixed_ref, mixed_sem)
    mixed_copy.start()
    for copy in scalars:
        copy.wait()
    placed = []
    for b in range(seq_count):
        limit = prior_s[b] + accepted_s[b] - offset
        start = pl.multiple_of(jnp.clip(limit, 0, length - window) // PROPS * PROPS, PROPS)
        select = start + iota((window, PROPS), 0) - limit == iota((window, PROPS), 1)
        select = ones_where(select, bf16)
        slot = start + iota((window, width), 0) - limit
        inside = (slot >= 0) & (slot < PROPS)
        for at, (source, fresh, target) in enumerate(
            ((k_ref, newk_ref, ko_ref), (v_ref, newv_ref, vo_ref))
        ):
            rows = matmul(select, fresh[b * PROPS : (b + 1) * PROPS])
            old = source[b, pl.ds(start, window), :].astype(f32)
            windows[at, b] = jnp.where(inside, rows, old).astype(bf16)
            placed.append(
                pltpu.make_async_copy(
                    windows.at[at, b],
                    target.at[b, pl.ds(start, window), :],
                    window_sems.at[at, b],
                )
            )
    for first, second in zip(bulk, placed):
        first.wait()
        second.start()
    mixed_copy.wait()
    for copy in placed:
        copy.wait()


def shards(
    n_kv,
    n_tp,
    tokens,
    norm_gain,
    w_query,
    w_key,
    w_value,
    w_gate,
    gate_bias,
    w_out,
    keys_cache,
    values_cache,
    cum_gates,
    prior_len,
    accepted,
    parents,
):
    row_count, depth = tokens.shape
    seq_count, length, width = keys_cache.shape
    heads = width // HEAD
    per = next(p for p in range(1, 5) if seq_count % p == 0 and seq_count // p <= n_kv)
    n_chunks = seq_count // per
    rc = per * PROPS
    cq = n_chunks // 4
    n_groups = n_kv // 4
    cpt = n_chunks // n_tp
    columns = w_out.shape[1]
    vmem = pl.BlockSpec(memory_space=pltpu.VMEM)
    hbm = pl.BlockSpec(memory_space=pltpu.HBM)
    dma = pltpu.SemaphoreType.DMA

    inputs = (
        tokens.reshape(n_chunks, rc, depth),
        norm_gain.reshape(1, depth),
        w_query,
        w_key,
        w_value,
        w_gate.T if depth % LANES == 0 else w_gate,
        gate_bias.reshape(1, -1),
        w_out,
        parents.T,
    )
    mixed, new_keys, new_values = pl.pallas_call(
        functools.partial(step_kernel, n_kv, n_tp, heads, per),
        out_shape=(
            jax.ShapeDtypeStruct((cpt * rc, columns), bf16),
            jax.ShapeDtypeStruct((n_chunks, rc, width), bf16),
            jax.ShapeDtypeStruct((n_chunks, rc, width), bf16),
        ),
        in_specs=[hbm] * 14,
        out_specs=[vmem] * 3,
        scratch_shapes=[pltpu.VMEM(value.shape, value.dtype) for value in inputs]
        + [pltpu.SMEM((seq_count,), i32)] * 2
        + [
            pltpu.VMEM((seq_count, length, width), bf16),
            pltpu.VMEM((seq_count, length, width), bf16),
            pltpu.VMEM((seq_count, heads, length), f32),
            pltpu.VMEM((3, n_chunks, rc, width), bf16),
            pltpu.VMEM((n_chunks, 8, LANES), f32),
            pltpu.VMEM((3, 3, cq, rc, width), bf16),
            pltpu.VMEM((3, cq, 8, LANES), f32),
            pltpu.VMEM((3, cq, rc, width), bf16),
            pltpu.VMEM((cq, 8, LANES), f32),
            pltpu.VMEM((3, n_groups - 1, cq, rc, width), bf16),
            pltpu.VMEM((n_groups - 1, cq, 8, LANES), f32),
            pltpu.VMEM((3, n_chunks, rc, width), bf16),
            pltpu.VMEM((n_chunks, 8, LANES), f32),
            pltpu.VMEM((n_tp, width, columns), bf16),
            pltpu.VMEM((n_kv, rc, width), bf16),
            pltpu.VMEM((n_kv, 8, LANES), f32),
            pltpu.VMEM((n_kv - 1, rc, width), bf16),
            pltpu.VMEM((n_kv - 1, 8, LANES), f32),
            pltpu.VMEM((rc, width), bf16),
            pltpu.VMEM((cpt, n_tp, rc, width), bf16),
            dma((len(inputs) + 2,)),
            dma((3, n_chunks)),
            dma((12 * cq,)),
            dma((12 * cq,)),
            dma((4 * (n_groups - 1) * cq,)),
            dma((4 * (n_groups - 1) * cq,)),
            dma((12 * cq,)),
            dma((12 * cq,)),
            dma((n_tp - 1,)),
            dma((n_tp - 1,)),
            dma((n_kv - 1,)),
            dma((n_kv - 1,)),
            dma((n_kv - 1,)),
            dma((n_kv - 1,)),
            dma((n_kv,)),
            dma((cpt * n_tp,)),
        ],
        compiler_params=pltpu.CompilerParams(
            collective_id=0, has_side_effects=True, vmem_limit_bytes=28 * 1024 * 1024
        ),
        name="step",
    )(
        *(
            pltpu.with_memory_space_constraint(value, pltpu.HBM)
            for value in (
                prior_len,
                accepted,
                *inputs,
                keys_cache,
                values_cache,
                cum_gates,
            )
        ),
    )

    return pl.pallas_call(
        write_kernel,
        out_shape=(
            jax.ShapeDtypeStruct((cpt * rc, columns), bf16),
            jax.ShapeDtypeStruct(keys_cache.shape, bf16),
            jax.ShapeDtypeStruct(values_cache.shape, bf16),
        ),
        in_specs=[hbm] * 2 + [vmem] * 5,
        out_specs=[hbm, hbm, hbm],
        scratch_shapes=[
            pltpu.SMEM((seq_count,), i32),
            pltpu.SMEM((seq_count,), i32),
            pltpu.VMEM((2, seq_count, 2 * PROPS, width), bf16),
            dma((2,)),
            dma((2, seq_count)),
            dma((2, seq_count)),
            dma(()),
        ],
        compiler_params=pltpu.CompilerParams(vmem_limit_bytes=8 * 1024 * 1024),
        name="write",
    )(
        pltpu.with_memory_space_constraint(prior_len, pltpu.HBM),
        pltpu.with_memory_space_constraint(accepted, pltpu.HBM),
        new_keys.reshape(row_count, width),
        new_values.reshape(row_count, width),
        mixed,
        keys_cache,
        values_cache,
    )


def solution(mesh):
    placed = (
        P(None, "kv"),
        P("kv"),
        P("kv", "tp"),
        P("kv", "tp"),
        P("kv", "tp"),
        P(),
        P(),
        P("tp", "kv"),
        P(None, "kv", "tp"),
        P(None, "kv", "tp"),
        P(None, "tp", "kv"),
        P(),
        P(),
        P(),
    )
    return jax.shard_map(
        functools.partial(shards, mesh.shape["kv"], mesh.shape["tp"]),
        mesh=mesh,
        in_specs=placed,
        out_specs=(P("tp", "kv"), P(None, "kv", "tp"), P(None, "kv", "tp")),
        check_vma=False,
    )
```

```python
import functools

import jax
import jax.numpy as jnp
from jax import lax
from jax.experimental import pallas as pl
from jax.experimental.pallas import tpu as pltpu
from jax.sharding import PartitionSpec as P

HEAD = 64
PROPS = 16
LANES = 128
SQUARE_ROW = 7
SUM_ROW = 4
masked_score = -1e30
norm_eps = 1e-06
MESH = pl.DeviceIdType.MESH
f32, bf16, i32 = jnp.float32, jnp.bfloat16, jnp.int32


def iota(shape, axis):
    return lax.broadcasted_iota(i32, shape, axis)


def ones_where(mask, dtype=f32):
    return jnp.where(mask, 1.0, 0.0).astype(dtype)


def split2(x):
    hi = x.astype(bf16)
    return hi, (x - hi.astype(f32)).astype(bf16)


def split3(x):
    hi = x.astype(bf16).astype(f32)
    mid = (x - hi).astype(bf16).astype(f32)
    return hi, mid, x - hi - mid


def contract_last(a, b):
    return lax.dot_general(a, b, (((1,), (1,)), ((), ())), preferred_element_type=f32)


def matmul(a, b):
    return jnp.dot(a, b, preferred_element_type=f32)


def step_kernel(
    n_kv,
    n_tp,
    heads,
    per,
    prior_hbm,
    accepted_hbm,
    tokens_hbm,
    gain_hbm,
    wq_hbm,
    wk_hbm,
    wv_hbm,
    wg_hbm,
    bias_hbm,
    wout_hbm,
    parents_hbm,
    k_hbm,
    v_hbm,
    cum_hbm,
    mixed_ref,
    newk_ref,
    newv_ref,
    tokens_ref,
    gain_ref,
    wq_ref,
    wk_ref,
    wv_ref,
    wg_ref,
    bias_ref,
    wout_ref,
    parents_ref,
    prior_s,
    accepted_s,
    kbuf,
    vbuf,
    cumbuf,
    part,
    gpart,
    arr1,
    garr1,
    half,
    ghalf,
    arr2,
    garr2,
    full,
    gfull,
    wall,
    parts_v,
    parts_s,
    got_v,
    got_s,
    mine,
    att,
    input_sems,
    load_sems,
    s1_send,
    s1_recv,
    s2_send,
    s2_recv,
    s3_send,
    s3_recv,
    w_send,
    w_recv,
    cv_send,
    cv_recv,
    cs_send,
    cs_recv,
    ag_send,
    ag_recv,
):
    me = lax.axis_index("kv")
    tp = lax.axis_index("tp")
    n_chunks, rc, depth = tokens_ref.shape
    length = kbuf.shape[1]
    width = heads * HEAD
    lines = heads * PROPS
    cq = n_chunks // 4
    n_groups = n_kv // 4
    cpt = n_chunks // n_tp
    corner, group = lax.rem(me, 4), me // 4
    quarter = pl.ds(corner * cq, cq)
    order = [lax.rem(group + i, cq) for i in range(cq)]

    aligned = n_tp == 4 and cpt == cq and n_kv == n_chunks
    inputs = []
    for at, (source, target) in enumerate(
        (
            (tokens_hbm, tokens_ref),
            (wq_hbm, wq_ref),
            (gain_hbm, gain_ref),
            (wg_hbm, wg_ref),
            (wk_hbm, wk_ref),
            (wv_hbm, wv_ref),
            (parents_hbm, parents_ref),
            (bias_hbm, bias_ref),
            (wout_hbm, wout_ref),
            (prior_hbm, prior_s),
            (accepted_hbm, accepted_s),
        )
    ):
        copy = pltpu.make_async_copy(source, target, input_sems.at[at])
        copy.start()
        inputs.append(copy)
    barrier = pltpu.get_barrier_semaphore()
    for d in range(1, n_kv * n_tp):
        other = lax.rem(me * n_tp + tp + d, n_kv * n_tp)
        pl.semaphore_signal(
            barrier,
            inc=1,
            device_id={"kv": other // n_tp, "tp": lax.rem(other, n_tp)},
            device_id_type=MESH,
        )

    def send(source, target, sems, at, kv=None, to_tp=None, out=None):
        where = {}
        if kv is not None:
            where["kv"] = kv
        if to_tp is not None:
            where["tp"] = to_tp
        copy = pltpu.make_async_remote_copy(
            src_ref=source,
            dst_ref=target,
            send_sem=sems[0].at[at if out is None else out],
            recv_sem=sems[1].at[at],
            device_id=where,
            device_id_type=MESH,
        )
        copy.start()
        return copy

    for copy in inputs[:3]:
        copy.wait()
    floats = tokens_ref[...].reshape(n_chunks * rc, depth).astype(f32)
    scaled = (floats * gain_ref[...]).astype(bf16)

    def product(piece, w_ref):
        value = matmul(scaled, w_ref[...]).astype(bf16)
        part[piece] = value.reshape(n_chunks, rc, width)

    product(0, wq_ref)
    pl.semaphore_wait(barrier, n_kv * n_tp - 1)
    started = []

    def sent(like, sem):
        pltpu.make_async_remote_copy(
            src_ref=like,
            dst_ref=like,
            send_sem=sem,
            recv_sem=s1_recv.at[0],
            device_id={"kv": lax.rem(me + 1, n_kv)},
            device_id_type=MESH,
        ).wait_send()


    def flip(bits):
        low = lax.rem(corner + bits % 2, 2)
        return lax.rem(corner // 2 + bits // 2, 2) * 2 + low

    def corner_sends(sources, targets, sems, piece, j=0):
        out = [None] * 3
        for d in (3, 2, 1):
            there = flip(d)
            at = (piece * 3 + d - 1) * cq + j
            out[d - 1] = send(
                sources(there), targets(d), sems, at, kv=group * 4 + there, out=piece
            )
        return out

    def first_stage(piece, j, count):
        return corner_sends(
            lambda there: part.at[piece, pl.ds(there * cq + j, count)],
            lambda d: arr1.at[piece, d - 1, pl.ds(j, count)],
            (s1_send, s1_recv),
            piece,
            j,
        )

    def group_sends(source, target, piece, j=0):
        out = []
        for d in range(1, n_groups):
            there = lax.rem(group + d, n_groups) * 4 + corner
            at = (piece * (n_groups - 1) + d - 1) * cq + j
            out.append(send(source, target(d), (s2_send, s2_recv), at, kv=there))
        started.extend(out)
        return out

    def second_stage(piece, stage, j, count, sent=None):
        for copy in stage:
            copy.wait_recv()
        span = pl.ds(j, count)
        total = part[piece, pl.ds(corner * cq + j, count)].astype(f32)
        for d in range(3):
            total = total + arr1[piece, d, span].astype(f32)
        half[piece, span] = total.astype(bf16)
        if sent is not None:
            j, span = sent, pl.ds(sent, 1)
        return group_sends(
            half.at[piece, span], lambda d: arr2.at[piece, d - 1, span], piece, j
        )

    def finish(piece, stage, columns, spots):
        for copy in stage:
            copy.wait_recv()
        for j, scale in zip(spots, columns):
            total = half[piece, j].astype(f32)
            for d in range(n_groups - 1):
                total = total + arr2[piece, d, j].astype(f32)
            full[piece, corner * cq + j] = (total * scale).astype(bf16)

    def third_stage(piece, j, count):
        span = pl.ds(corner * cq + j, count)
        return corner_sends(
            lambda there: full.at[piece, span],
            lambda d: full.at[piece, span],
            (s3_send, s3_recv),
            piece,
            j,
        )

    q1 = [first_stage(0, order[0], 1)]
    inputs[3].wait()
    total_heads = bias_hbm.shape[1]
    pick = (iota((8, total_heads), 1) == tp * heads + iota((8, total_heads), 0)) & (
        iota((8, total_heads), 0) < heads
    )
    if depth % LANES == 0:
        gate_w = wg_ref[:, pl.ds(pl.multiple_of(me * depth, depth), depth)]
        gate_w = matmul(ones_where(pick, bf16), gate_w).astype(bf16)
    else:
        gate_w = wg_ref[pl.ds(pl.multiple_of(me * depth, depth), depth), :]
        gate_w = contract_last(ones_where(pick, bf16), gate_w).astype(bf16)
    square_w = ones_where(iota((8, depth), 0) == SQUARE_ROW, bf16)
    sq_hi, sq_lo = split2(floats * floats)
    gpart[...] = jnp.zeros_like(gpart)
    for c in range(n_chunks):
        rows = slice(c * rc, (c + 1) * rc)
        gpart[c, :, :rc] = (
            contract_last(gate_w, scaled[rows])
            + contract_last(square_w, sq_hi[rows])
            + contract_last(square_w, sq_lo[rows])
        )
    g1 = corner_sends(
        lambda there: gpart.at[pl.ds(there * cq, cq)],
        lambda d: garr1.at[d - 1],
        (s1_send, s1_recv),
        3,
    )
    q1 = q1 + [first_stage(0, j, 1) for j in order[1:]]
    loads = []
    for at, (source, target) in enumerate(((k_hbm, kbuf), (v_hbm, vbuf), (cum_hbm, cumbuf))):
        copy = pltpu.make_async_copy(source, target, load_sems.at[at])
        copy.start()
        loads.append(copy)
    for copy in inputs[4:]:
        copy.wait()
    product(1, wk_ref)
    k1 = first_stage(1, 0, cq)
    product(2, wv_ref)

    slot = lax.rem(me, n_tp) * cpt + me // n_tp
    own = jnp.minimum(slot, n_chunks - 1)
    every = parents_ref[...]
    parent = jnp.concatenate(
        [
            jnp.sum(
                jnp.where(iota(every.shape, 1) == own * per + k, every, 0).astype(f32),
                axis=1,
                keepdims=True,
            ).astype(i32)
            for k in range(per)
        ],
        axis=0,
    )
    row, column = iota((rc, rc), 0), iota((rc, rc), 1)
    link = (parent + (row // PROPS) * PROPS == column) & (parent >= 0)
    reached = ones_where(link | (row == column))
    for squaring in range((PROPS - 1).bit_length()):
        reached = jnp.minimum(matmul(reached.astype(bf16), reached.astype(bf16)), 1.0)

    q2 = [second_stage(0, q1[0], order[0], 1)]
    for copy in g1:
        copy.wait_recv()
    ghalf[...] = gpart[quarter] + garr1[0] + garr1[1] + garr1[2]
    g2 = group_sends(ghalf, lambda d: garr2.at[d - 1], 3)
    for i in range(1, cq):
        q2.append(second_stage(0, q1[i], order[i], 1))
    v1 = first_stage(2, 0, cq)
    w_copies = []
    for d in range(1, n_tp):
        w_copies.append(
            send(
                wout_ref, wall.at[tp], (w_send, w_recv), d - 1, to_tp=lax.rem(tp + d, n_tp)
            )
        )
    started.extend(w_copies)
    wall[tp] = wout_ref[...]

    for copy in g2:
        copy.wait_recv()
    bias = jnp.sum(
        jnp.where(pick, jnp.broadcast_to(bias_ref[...], (8, total_heads)), 0.0),
        axis=1,
        keepdims=True,
    )
    inv_columns = []
    eye = iota((rc, LANES), 0) == iota((rc, LANES), 1)
    for j in order:
        gates = ghalf[j]
        for d in range(n_groups - 1):
            gates = gates + garr2[d, j]
        inv_row = lax.rsqrt(gates[SQUARE_ROW : SQUARE_ROW + 1, :] / (n_kv * depth) + norm_eps)
        pre = inv_row * gates + bias
        gfull[corner * cq + j] = jnp.minimum(pre, 0.0) - jnp.log1p(jnp.exp(-jnp.abs(pre)))
        inv_columns.append(
            jnp.sum(
                jnp.where(eye, jnp.broadcast_to(inv_row, (rc, LANES)), 0.0),
                axis=1,
                keepdims=True,
            )
        )
    scaled_columns = [c * HEAD ** (-0.5) for c in inv_columns]
    q3 = []
    first_only = order[1] if aligned else None
    upper = me >= n_kv // 2
    rise = [
        pltpu.make_async_remote_copy(
            src_ref=half.at[piece, 0],
            dst_ref=arr2.at[piece, 0, 0],
            send_sem=s2_send.at[piece * cq],
            recv_sem=s2_recv.at[piece * cq],
            device_id={"kv": lax.rem(me + 4, n_kv)},
            device_id_type=MESH,
        )
        for piece in (1, 2)
    ]

    def send_up(copy):
        @pl.when(jnp.logical_not(upper))
        def _():
            copy.start()

    k2 = None
    for i in list(range(1, cq)) + [0]:
        finish(0, q2[i], scaled_columns[i : i + 1], order[i : i + 1])
        q3.append(third_stage(0, order[i], 1))
        if k2 is None:
            k2 = second_stage(1, k1, 0, cq, first_only)
            if aligned:
                send_up(rise[0])
    g3 = []
    if not aligned:
        g3 = corner_sends(
            lambda there: gfull.at[quarter],
            lambda d: gfull.at[quarter],
            (s3_send, s3_recv),
            3,
        )
    lane_head = iota((PROPS, width), 1) // HEAD
    head_rows = [ones_where(lane_head == h) for h in range(heads)]
    head_mask = jnp.concatenate(head_rows, axis=0).astype(bf16)
    position = iota((lines, length), 1)
    short_position = iota((heads, length), 1)
    line_eye = iota((lines, LANES), 0) == iota((lines, LANES), 1)
    last_lane = iota((heads, LANES), 1) - LANES // 2
    last_mask = (last_lane >= 0) & (last_lane // PROPS == iota((heads, LANES), 0))
    tile_row = iota((8, LANES), 0)
    offset = me * length

    def as_row(value):
        return jnp.sum(jnp.where(line_eye, value, 0.0), axis=0, keepdims=True)

    def attend(owner):
        chunk = jnp.minimum(lax.rem(owner, n_tp) * cpt + owner // n_tp, n_chunks - 1)
        limits, scores = [], []
        for k in range(per):
            seq = chunk * per + k
            limits.append(prior_s[seq] + accepted_s[seq] - offset)
            query = full[0, chunk, k * PROPS : (k + 1) * PROPS, :]
            query = jnp.concatenate([query] * heads, axis=0) * head_mask
            scores.append(contract_last(query, kbuf[seq]))
        tile = jnp.zeros((8, LANES), f32)
        weights = []
        for k in range(per):
            seq = chunk * per + k
            cum = jnp.concatenate(
                [
                    jnp.broadcast_to(cumbuf[seq, h : h + 1, :], (PROPS, length))
                    for h in range(heads)
                ],
                axis=0,
            )
            value = jnp.where(position < limits[k], scores[k] - cum, masked_score)
            top = jnp.max(value, axis=1, keepdims=True)
            weight = jnp.exp(value - top)
            total = jnp.sum(weight, axis=1, keepdims=True)
            weights.append(weight.astype(bf16))
            last = jnp.sum(
                jnp.where(short_position == limits[k] - 1, cumbuf[seq], 0.0),
                axis=1,
                keepdims=True,
            )
            last_row = jnp.sum(jnp.where(last_mask, last, 0.0), axis=0, keepdims=True)
            tile = jnp.where(tile_row == k, as_row(top) + last_row, tile)
            tile = jnp.where(tile_row == SUM_ROW + k, as_row(total), tile)
        for k in range(per):
            values = matmul(weights[k], vbuf[chunk * per + k])
            picked = values[:PROPS] * head_rows[0]
            for h in range(1, heads):
                picked = picked + values[h * PROPS : (h + 1) * PROPS] * head_rows[h]
            parts_v[owner, k * PROPS : (k + 1) * PROPS, :] = picked.astype(bf16)
        parts_s[owner] = tile

    def peer(at):
        near = at >= n_kv - 4
        if isinstance(at, int):
            bits = 3 - at % 4 if near else at % 4
        else:
            bits = jnp.where(near, 3 - at % 4, at % 4)
        return lax.rem(group + at // 4 + 1, n_groups) * 4 + flip(bits)

    def part_copies(at):
        owner = peer(at)
        return [
            pltpu.make_async_remote_copy(
                src_ref=source.at[owner],
                dst_ref=target.at[at],
                send_sem=send_sem,
                recv_sem=recv_sem.at[at],
                device_id={"kv": owner},
                device_id_type=MESH,
            )
            for source, target, send_sem, recv_sem in (
                (parts_v, got_v, cv_send, cv_recv),
                (parts_s, got_s, cs_send, cs_recv),
            )
        ]

    def attend_and_send(at):
        attend(peer(at))
        for copy in part_copies(at):
            copy.start()

    for copy in loads:
        copy.wait()
    if aligned:
        def met(piece):
            return pltpu.make_async_remote_copy(
                src_ref=half.at[piece, order[0]],
                dst_ref=arr2.at[piece, 0, order[0]],
                send_sem=s2_send.at[piece * cq + order[0]],
                recv_sem=s2_recv.at[piece * cq + order[0]],
                device_id={"kv": lax.rem(me + 4, n_kv)},
                device_id_type=MESH,
            )

        late = [
            [
                pltpu.make_async_remote_copy(
                    src_ref=full.at[piece, corner * cq + j],
                    dst_ref=full.at[piece, corner * cq + j],
                    send_sem=s3_send.at[piece],
                    recv_sem=s3_recv.at[(piece * 3 + d - 1) * cq + j],
                    device_id={"kv": group * 4 + flip(d)},
                    device_id_type=MESH,
                )
                for piece in (1, 2)
                for d in (3, 2, 1)
            ]
            for j in range(cq)
        ]

        def lift(piece):
            rise[piece - 1].wait_recv()
            total = half[piece, 0].astype(f32) + arr2[piece, 0, 0].astype(f32)
            full[piece, corner * cq] = (total * inv_columns[1]).astype(bf16)

        attend_and_send(0)
        attend(me)
        v2 = second_stage(2, v1, 0, cq, first_only)
        for at in range(1, n_kv - 1):
            if at < 4:
                q3[0][at - 1].wait_recv()
            else:
                q3[1][2 - at % 4].wait_recv()
            attend_and_send(at)
            if at == 3:
                send_up(rise[1])
                finish(1, [met(1)], inv_columns[:1], order[:1])

                @pl.when(upper)
                def _():
                    lift(1)
                    for copy in late[1][:3] + late[0][:3]:
                        copy.start()

    else:
        v2 = second_stage(2, v1, 0, cq)
        for stage in q3:
            for copy in stage:
                copy.wait_recv()

        def one(at, carry):
            attend_and_send(at)
            return carry

        lax.fori_loop(0, n_kv - 1, one, 0)
        attend(me)
    k3 = v3 = []
    if aligned:

        finish(2, [met(2)], inv_columns[:1], order[:1])

        @pl.when(upper)
        def _():
            for copy in late[1][3:]:
                copy.start()

    else:
        finish(1, k2, inv_columns, order)
        finish(2, v2, inv_columns, order)
        k3 = third_stage(1, 0, cq)
        v3 = third_stage(2, 0, cq)
        for copy in g3 + k3 + v3:
            copy.wait_recv()
    gate_parts = jnp.concatenate(split3(gfull[own]), axis=0)[:, :rc].astype(bf16)
    tree_gates = contract_last(gate_parts, reached.astype(bf16))
    tree_gates = tree_gates[0:8] + tree_gates[8:16] + tree_gates[16:24]
    wide_rows = [ones_where(iota((rc, width), 1) // HEAD == h) for h in range(heads)]
    wide_mask = jnp.concatenate(wide_rows, axis=0).astype(bf16)
    tree_query = jnp.concatenate([full[0, own]] * heads, axis=0) * wide_mask
    tree = contract_last(tree_query, full[1, own])
    tree = tree - jnp.concatenate(
        [jnp.broadcast_to(tree_gates[h : h + 1, :], (rc, rc)) for h in range(heads)], axis=0
    )
    live = jnp.concatenate([reached] * heads, axis=0) > 0.5
    tree = jnp.where(live, tree, masked_score)
    tree_top = jnp.max(tree, axis=1, keepdims=True)
    tree_weights = jnp.where(live, jnp.exp(tree - tree_top), 0.0)
    tree_sum = jnp.sum(tree_weights, axis=1, keepdims=True)
    tree_values = matmul(tree_weights.astype(bf16), full[2, own])
    tree_picked = tree_values[:rc] * wide_rows[0]
    for h in range(1, heads):
        tree_picked = tree_picked + tree_values[h * rc : (h + 1) * rc] * wide_rows[h]
    def tile_of(value):
        rows = [
            as_row(
                jnp.concatenate(
                    [
                        value[h * rc + k * PROPS : h * rc + (k + 1) * PROPS]
                        for h in range(heads)
                    ],
                    axis=0,
                )
            )
            for k in range(per)
        ]
        rows = rows + [jnp.zeros((1, LANES), f32)] * (4 - per)
        return jnp.concatenate(rows, axis=0)

    tree_top_tile, tree_sum_tile = tile_of(tree_top), tile_of(tree_sum)

    landing = [part_copies(at) for at in range(n_kv - 1)]
    for pair in landing:
        pair[1].wait_recv()
    tiles = [parts_s[me]] + [got_s[d] for d in range(n_kv - 1)]
    last = tiles[0][:4]
    for tile in tiles[1:]:
        last = last + tile[:4]
    last = pltpu.roll(last, LANES // 2, axis=1)
    lane_ok = iota((4, LANES), 1) < lines
    tops = [jnp.where(lane_ok, tile[:4], 0.0) for tile in tiles]
    tops.append(jnp.where(lane_ok, tree_top_tile - last, 0.0))
    sums = [jnp.where(lane_ok, tile[4:], 1.0) for tile in tiles] + [
        jnp.where(lane_ok, tree_sum_tile, 1.0)
    ]
    top = functools.reduce(jnp.maximum, tops)
    scales = [jnp.exp(t - top) for t in tops]
    total = functools.reduce(lambda a, b: a + b, [a * b for a, b in zip(scales, sums)])
    half_lane = iota((LANES, width), 0) % (LANES // 2)
    spread = ones_where(
        (half_lane // PROPS == iota((LANES, width), 1) // HEAD) & (half_lane < lines), bf16
    )
    fits = (iota((PROPS, LANES), 1) % PROPS == iota((PROPS, LANES), 0)) & (
        iota((PROPS, LANES), 1) % (LANES // 2) < lines
    )
    inverse = 1.0 / total
    low_half = iota((4, LANES), 1) < LANES // 2

    def expand(scale):
        hi, lo = split2(jnp.where(low_half, scale * inverse, 0.0))
        both = jnp.where(low_half, hi.astype(f32), pltpu.roll(lo.astype(f32), LANES // 2, axis=1))
        rows = jnp.concatenate(
            [
                jnp.where(fits, jnp.broadcast_to(both[k : k + 1], (PROPS, LANES)), 0.0)
                for k in range(per)
            ],
            axis=0,
        )
        return matmul(rows.astype(bf16), spread)

    expanded = [expand(scale) for scale in scales]
    result = expanded[-1] * tree_picked + expanded[0] * parts_v[me].astype(f32)
    for d in range(n_kv - 1):
        landing[d][0].wait_recv()
        result = result + expanded[d + 1] * got_v[d].astype(f32)
    mine[...] = result.astype(bf16)

    target, early = lax.rem(me, n_tp), me // n_tp
    spreads = [
        pltpu.make_async_remote_copy(
            src_ref=mine,
            dst_ref=att.at[jnp.minimum(early, cpt - 1), tp],
            send_sem=ag_send.at[d],
            recv_sem=ag_recv.at[jnp.minimum(early, cpt - 1) * n_tp + tp],
            device_id={"kv": peer(d - 1) if d > 0 else me, "tp": target},
            device_id_type=MESH,
        )
        for d in range(n_kv)
    ]
    sends = early < cpt
    for d in range(1, n_kv):

        @pl.when(sends)
        def _(d=d):
            spreads[d].start()

    @pl.when(sends & (target != tp))
    def _():
        spreads[0].start()

    @pl.when(sends & (target == tp))
    def _():
        att[jnp.minimum(early, cpt - 1), tp] = mine[...]

    if aligned:

        @pl.when(upper)
        def _():
            lift(2)
            for copy in late[0][3:]:
                copy.start()

        @pl.when(jnp.logical_not(upper))
        def _():
            for copy in rise:
                copy.wait_send()

    for copy in w_copies:
        copy.wait_recv()
    for at in range(cpt * n_tp):
        e, t = at // n_tp, at % n_tp

        @pl.when((me != e * n_tp + tp) | (tp != t))
        def _(at=at, e=e, t=t):
            pltpu.make_async_remote_copy(
                src_ref=mine,
                dst_ref=att.at[e, t],
                send_sem=ag_send.at[0],
                recv_sem=ag_recv.at[at],
                device_id={"kv": me, "tp": lax.rem(tp + 1, n_tp)},
                device_id_type=MESH,
            ).wait_recv()

    mixed = None
    for t in range(n_tp):
        rows = jnp.concatenate([att[e, t] for e in range(cpt)], axis=0)
        piece = matmul(rows, wall[t]).astype(bf16).astype(f32)
        mixed = piece if mixed is None else mixed + piece
    mixed_ref[...] = mixed.astype(bf16)
    if aligned:

        @pl.when(upper)
        def _():
            for copy in late[1] + late[0]:
                copy.wait_recv()
            for piece in (1, 2):
                sent(arr1.at[piece], s3_send.at[piece])

    newk_ref[...] = full[1]
    newv_ref[...] = full[2]
    for d in range(1, n_kv):

        @pl.when(sends)
        def _(d=d):
            spreads[d].wait_send()

    @pl.when(sends & (target != tp))
    def _():
        spreads[0].wait_send()

    for piece in range(3):
        sent(arr1.at[piece], s1_send.at[piece])
    sent(garr1, s1_send.at[3])
    sent(arr1.at[0], s3_send.at[0])
    if not aligned:
        sent(arr1.at[1], s3_send.at[1])
        sent(arr1.at[2], s3_send.at[2])
        sent(garr1, s3_send.at[3])
    for copy in started:
        copy.wait_send()
    sent(got_v, cv_send)
    sent(got_s, cs_send)


def write_kernel(
    prior_hbm,
    accepted_hbm,
    newk_ref,
    newv_ref,
    mixed_in,
    k_ref,
    v_ref,
    mixed_ref,
    ko_ref,
    vo_ref,
    prior_s,
    accepted_s,
    windows,
    scalar_sems,
    bulk_sems,
    window_sems,
    mixed_sem,
):
    seq_count, length, width = k_ref.shape
    window = 2 * PROPS
    offset = lax.axis_index("kv") * length
    scalars = [
        pltpu.make_async_copy(prior_hbm, prior_s, scalar_sems.at[0]),
        pltpu.make_async_copy(accepted_hbm, accepted_s, scalar_sems.at[1]),
    ]
    for copy in scalars:
        copy.start()
    bulk = []
    block = next(n for n in (3, 2, 1) if seq_count % n == 0)
    for b in range(seq_count):
        for at, (source, target) in enumerate(((k_ref, ko_ref), (v_ref, vo_ref))):
            copy = pltpu.make_async_copy(
                source.at[b], target.at[b], bulk_sems.at[at, b // block]
            )
            copy.start()
    for first in range(0, seq_count, block):
        span = pl.ds(first, block)
        for at, (source, target) in enumerate(((k_ref, ko_ref), (v_ref, vo_ref))):
            bulk.append(
                pltpu.make_async_copy(
                    source.at[span], target.at[span], bulk_sems.at[at, first // block]
                )
            )
    mixed_copy = pltpu.make_async_copy(mixed_in, mixed_ref, mixed_sem)
    mixed_copy.start()
    for copy in scalars:
        copy.wait()
    placed = []
    for b in range(seq_count):
        limit = prior_s[b] + accepted_s[b] - offset
        start = pl.multiple_of(jnp.clip(limit, 0, length - window) // PROPS * PROPS, PROPS)
        select = start + iota((window, PROPS), 0) - limit == iota((window, PROPS), 1)
        select = ones_where(select, bf16)
        slot = start + iota((window, width), 0) - limit
        inside = (slot >= 0) & (slot < PROPS)
        for at, (source, fresh, target) in enumerate(
            ((k_ref, newk_ref, ko_ref), (v_ref, newv_ref, vo_ref))
        ):
            rows = matmul(select, fresh[b * PROPS : (b + 1) * PROPS])
            old = source[b, pl.ds(start, window), :].astype(f32)
            windows[at, b] = jnp.where(inside, rows, old).astype(bf16)
            placed.append(
                pltpu.make_async_copy(
                    windows.at[at, b],
                    target.at[b, pl.ds(start, window), :],
                    window_sems.at[at],
                )
            )
    for at, copy in enumerate(bulk):
        copy.wait()
        base = at // 2 * 2 * block + at % 2
        for second in placed[base : base + 2 * block : 2]:
            second.start()
    mixed_copy.wait()
    for at in range(2):
        pltpu.make_async_copy(windows.at[at], windows.at[at], window_sems.at[at]).wait()


def shards(
    n_kv,
    n_tp,
    tokens,
    norm_gain,
    w_query,
    w_key,
    w_value,
    w_gate,
    gate_bias,
    w_out,
    keys_cache,
    values_cache,
    cum_gates,
    prior_len,
    accepted,
    parents,
):
    row_count, depth = tokens.shape
    seq_count, length, width = keys_cache.shape
    heads = width // HEAD
    per = next(p for p in range(1, 5) if seq_count % p == 0 and seq_count // p <= n_kv)
    n_chunks = seq_count // per
    rc = per * PROPS
    cq = n_chunks // 4
    n_groups = n_kv // 4
    cpt = n_chunks // n_tp
    columns = w_out.shape[1]
    vmem = pl.BlockSpec(memory_space=pltpu.VMEM)
    hbm = pl.BlockSpec(memory_space=pltpu.HBM)
    dma = pltpu.SemaphoreType.DMA

    inputs = (
        tokens.reshape(n_chunks, rc, depth),
        norm_gain.reshape(1, depth),
        w_query,
        w_key,
        w_value,
        w_gate.T if depth % LANES == 0 else w_gate,
        gate_bias.reshape(1, -1),
        w_out,
        parents.T,
    )
    mixed, new_keys, new_values = pl.pallas_call(
        functools.partial(step_kernel, n_kv, n_tp, heads, per),
        out_shape=(
            jax.ShapeDtypeStruct((cpt * rc, columns), bf16),
            jax.ShapeDtypeStruct((n_chunks, rc, width), bf16),
            jax.ShapeDtypeStruct((n_chunks, rc, width), bf16),
        ),
        in_specs=[hbm] * 14,
        out_specs=[vmem] * 3,
        scratch_shapes=[pltpu.VMEM(value.shape, value.dtype) for value in inputs]
        + [pltpu.SMEM((seq_count,), i32)] * 2
        + [
            pltpu.VMEM((seq_count, length, width), bf16),
            pltpu.VMEM((seq_count, length, width), bf16),
            pltpu.VMEM((seq_count, heads, length), f32),
            pltpu.VMEM((3, n_chunks, rc, width), bf16),
            pltpu.VMEM((n_chunks, 8, LANES), f32),
            pltpu.VMEM((3, 3, cq, rc, width), bf16),
            pltpu.VMEM((3, cq, 8, LANES), f32),
            pltpu.VMEM((3, cq, rc, width), bf16),
            pltpu.VMEM((cq, 8, LANES), f32),
            pltpu.VMEM((3, n_groups - 1, cq, rc, width), bf16),
            pltpu.VMEM((n_groups - 1, cq, 8, LANES), f32),
            pltpu.VMEM((3, n_chunks, rc, width), bf16),
            pltpu.VMEM((n_chunks, 8, LANES), f32),
            pltpu.VMEM((n_tp, width, columns), bf16),
            pltpu.VMEM((n_kv, rc, width), bf16),
            pltpu.VMEM((n_kv, 8, LANES), f32),
            pltpu.VMEM((n_kv - 1, rc, width), bf16),
            pltpu.VMEM((n_kv - 1, 8, LANES), f32),
            pltpu.VMEM((rc, width), bf16),
            pltpu.VMEM((cpt, n_tp, rc, width), bf16),
            dma((len(inputs) + 2,)),
            dma((3,)),
            dma((4,)),
            dma((12 * cq,)),
            dma((4 * (n_groups - 1) * cq,)),
            dma((4 * (n_groups - 1) * cq,)),
            dma((4,)),
            dma((12 * cq,)),
            dma((n_tp - 1,)),
            dma((n_tp - 1,)),
            dma(()),
            dma((n_kv - 1,)),
            dma(()),
            dma((n_kv - 1,)),
            dma((n_kv,)),
            dma((cpt * n_tp,)),
        ],
        compiler_params=pltpu.CompilerParams(
            collective_id=0, has_side_effects=True, vmem_limit_bytes=28 * 1024 * 1024
        ),
        name="step",
    )(
        *(
            pltpu.with_memory_space_constraint(value, pltpu.HBM)
            for value in (
                prior_len,
                accepted,
                *inputs,
                keys_cache,
                values_cache,
                cum_gates,
            )
        ),
    )

    return pl.pallas_call(
        write_kernel,
        out_shape=(
            jax.ShapeDtypeStruct((cpt * rc, columns), bf16),
            jax.ShapeDtypeStruct(keys_cache.shape, bf16),
            jax.ShapeDtypeStruct(values_cache.shape, bf16),
        ),
        in_specs=[hbm] * 2 + [vmem] * 5,
        out_specs=[hbm, hbm, hbm],
        scratch_shapes=[
            pltpu.SMEM((seq_count,), i32),
            pltpu.SMEM((seq_count,), i32),
            pltpu.VMEM((2, seq_count, 2 * PROPS, width), bf16),
            dma((2,)),
            dma((2, seq_count // next(n for n in (3, 2, 1) if seq_count % n == 0))),
            dma((2,)),
            dma(()),
        ],
        compiler_params=pltpu.CompilerParams(vmem_limit_bytes=8 * 1024 * 1024),
        name="write",
    )(
        pltpu.with_memory_space_constraint(prior_len, pltpu.HBM),
        pltpu.with_memory_space_constraint(accepted, pltpu.HBM),
        new_keys.reshape(row_count, width),
        new_values.reshape(row_count, width),
        mixed,
        keys_cache,
        values_cache,
    )


def solution(mesh):
    placed = (
        P(None, "kv"),
        P("kv"),
        P("kv", "tp"),
        P("kv", "tp"),
        P("kv", "tp"),
        P(),
        P(),
        P("tp", "kv"),
        P(None, "kv", "tp"),
        P(None, "kv", "tp"),
        P(None, "tp", "kv"),
        P(),
        P(),
        P(),
    )
    return jax.shard_map(
        functools.partial(shards, mesh.shape["kv"], mesh.shape["tp"]),
        mesh=mesh,
        in_specs=placed,
        out_specs=(P("tp", "kv"), P(None, "kv", "tp"), P(None, "kv", "tp")),
        check_vma=False,
    )
```
